32 devices in a mesh: ep: 8 (over z, y), tp: 4 (over x, core).
Axes of the slice: x: 2, y: 2, z: 4, core: 2. Of those that a mesh axis runs over, the one named last changes fastest.
Arguments:
- tokens: bfloat16 [64, 1024], P('ep'), may hold values from -6 to 6
- mix_gain: float32 [1024], replicated, may hold values from 0.1 to 1.9
- w_query: bfloat16 [1024, 512], P(None, 'tp'), may hold values from -0.1875 to 0.1875
- w_key: bfloat16 [1024, 512], P(None, 'tp'), may hold values from -0.1875 to 0.1875
- w_value: bfloat16 [1024, 1024], P(None, 'tp'), may hold values from -0.1875 to 0.1875
- w_ogate: bfloat16 [1024, 1024], P(None, 'tp'), may hold values from -0.1875 to 0.1875
- w_igate: bfloat16 [1024, 4], replicated, may hold values from -0.1875 to 0.1875
- w_fgate: bfloat16 [1024, 4], replicated, may hold values from -0.1875 to 0.1875
- forget_bias: float32 [4], replicated, may hold values from -1 to 3
- head_gain: float32 [1024], P('tp'), may hold values from 0.1 to 1.9
- w_out: bfloat16 [1024, 1024], P('tp'), may hold values from -0.1875 to 0.1875
- memory: float32 [64, 4, 128, 256], P('ep', 'tp'), may hold values from -0.4 to 0.4
- normalizer: float32 [64, 4, 128], P('ep', 'tp'), may hold values from -0.4 to 0.4
- running_max: float32 [64, 4], P('ep', 'tp'), may hold values from -4 to 4
- ffn_gain: float32 [1024], replicated, may hold values from 0.1 to 1.9
- route: int32 [64, 2], replicated, may hold values from 0 to 7, all different within a row; in each aligned block of 64 rows (0 to 63, 64 to 127, ...) at most 32 rows name the same one
- route_weight: float32 [64, 2], replicated, may hold values from 0.05 to 1
- w_gate: bfloat16 [8, 1024, 512], P('ep', None, 'tp'), may hold values from -0.1875 to 0.1875
- w_up: bfloat16 [8, 1024, 512], P('ep', None, 'tp'), may hold values from -0.1875 to 0.1875
- w_down: bfloat16 [8, 512, 1024], P('ep', 'tp'), may hold values from -0.25 to 0.25
Outputs:
- mixed: bfloat16 [64, 1024], P(None, 'ep')
- new_memory: float32 [64, 4, 128, 256], P('ep', 'tp')
- new_normalizer: float32 [64, 4, 128], P('ep', 'tp')
- new_max: float32 [64, 4], P('ep', 'tp')
The draws below stay inside these ranges and needn't reach their ends.
Inputs may be any that keep to these rules, and one draw needn't show every extreme that they name: `route`: each expert is named by at most 32 routes in all, a bound that some block reaches; the two choices of a token differ.
All inputs are finite; a program needn't handle non-finite values.
Results may differ from the reference program's by a relative error of at most 0.014.
Values may be sent and summed in bfloat16 or wider, within the bound.
No kernel may reach another device: no remote copies, remote signals or barrier semaphores. Data moves between devices by JAX's collectives and lax.ppermute only.
A program may use at most 64 MiB of HBM per device.

```python
import math
import jax
import jax.numpy as jnp
import numpy as np
from jax import lax

MODEL_WIDTH = 1024
HEADS = 4
QK = 128
DV = 256
EXPERT_HIDDEN = 512
TOPK = 2
TOKENS = 64
EXPERTS = 8
EXPERT_CAPACITY = 32
N_TP = 4


def shard_levels(key, shape, split, low, largest):
    def one(dim, blocks):
        steps = jax.random.uniform(jax.random.fold_in(jax.random.fold_in(key, 6), dim), (blocks,), jnp.float32, low / len(split), largest / len(split))
        return jnp.repeat(jnp.exp(steps), shape[dim] // blocks).reshape((-1,) + (1,) * (len(shape) - dim - 1))

    level = one(*split[0])
    for cut in split[1:]:
        level = level * one(*cut)
    return level


def shared_out(key, own, number, rows, number_of, top, reach, lean):
    ranking = jax.random.permutation(key, number_of)
    packed, common = load_shares(number_of, rows * top, reach, lean, True), load_shares(number_of, rows * top, reach, lean, False)
    places = jnp.arange(number_of)

    def named(sizes, turn):
        used = int((sizes > 0).sum())
        fixed = max(1, used // 4)
        shifted = fixed + (places - fixed + turn * (used - fixed)) % max(1, number_of - fixed)
        return jnp.zeros((number_of,), jnp.int32).at[ranking[jnp.where(places < fixed, places, shifted)]].set(jnp.asarray(sizes, jnp.int32))

    sizes = jnp.where(number % 4 == 0, named(packed, number // 4), named(common, number - number // 4 - 1))
    mixed = jax.random.permutation(jax.random.fold_in(own, 3), number_of)
    source_of, taker = mixed[0:number_of // 2 * 2:2], mixed[1:number_of // 2 * 2:2]
    room = jnp.minimum(sizes[source_of] - 1, reach - sizes[taker]) // 2
    room = jnp.where((source_of == ranking[0]) | (taker == ranking[0]) | (sizes[taker] == 0), 0, jnp.maximum(room, 0))
    shifted = jax.random.randint(jax.random.fold_in(own, 4), (number_of // 2,), 0, 1 << 20) % (room + 1)
    sizes = sizes.at[source_of].add(-shifted).at[taker].add(shifted)
    items = jnp.searchsorted(jnp.cumsum(sizes), jnp.arange(rows * top), side="right").astype(jnp.int32)
    table = items.reshape(top, rows).T
    table = table[jax.random.permutation(jax.random.fold_in(own, 1), rows)]
    turn = jax.random.randint(jax.random.fold_in(own, 2), (rows, 1), 0, top)
    return jnp.take_along_axis(table, (jnp.arange(top)[None, :] + turn) % top, axis=1)


def load_shares(amount, total, most, skew, full):
    portions = [(1 << 20) // math.isqrt(rank ** skew) + 1 for rank in range(1, amount + 1)]
    largest = most if full else min(most, max(-(-total // amount), total * portions[0] // sum(portions)))
    least = 1 if total - largest >= amount - 1 else 0
    holding, spare = [largest] + [least] * (amount - 1), total - largest - least * (amount - 1)
    while spare > 0:
        free = [i for i in range(1, amount) if holding[i] < largest] or [i for i in range(1, amount) if holding[i] < most]
        whole, remaining = sum([portions[i] for i in free]), spare
        for i in free:
            addition = min(most - holding[i], max(1, remaining * portions[i] // whole), spare)
            holding[i] = holding[i] + addition
            spare = spare - addition
    return np.array(holding)


def scatter_about(key, dims, scale, most, split=(), kind=jnp.bfloat16):
    entries = scale * jax.random.normal(key, dims, jnp.float32)
    if split:
        entries = entries * shard_levels(key, dims, split, -0.22, 0.18)
    return jnp.clip(entries, -most, most).astype(kind)


def setup_inputs(seed: int = 0) -> dict:
    arg_keys = jax.random.split(jax.random.key(seed), 21)
    tokens = scatter_about(arg_keys[0], (TOKENS, MODEL_WIDTH), 1.0, 6.0, ((0, 8),))
    mix_gain = jnp.clip(1.0 + 0.18 * jax.random.normal(arg_keys[1], (MODEL_WIDTH,), jnp.float32), 0.1, 1.9)
    w_query = scatter_about(arg_keys[2], (MODEL_WIDTH, HEADS * QK), MODEL_WIDTH ** -0.5, 0.1875, ((1, 4),))
    w_key = scatter_about(arg_keys[3], (MODEL_WIDTH, HEADS * QK), MODEL_WIDTH ** -0.5, 0.1875, ((1, 4),))
    w_value = scatter_about(arg_keys[4], (MODEL_WIDTH, HEADS * DV), MODEL_WIDTH ** -0.5, 0.1875, ((1, 4),))
    w_ogate = scatter_about(arg_keys[5], (MODEL_WIDTH, HEADS * DV), MODEL_WIDTH ** -0.5, 0.1875, ((1, 4),))
    w_igate = scatter_about(arg_keys[6], (MODEL_WIDTH, HEADS), MODEL_WIDTH ** -0.5, 0.1875)
    w_fgate = scatter_about(arg_keys[7], (MODEL_WIDTH, HEADS), MODEL_WIDTH ** -0.5, 0.1875)
    forget_bias = jnp.clip(jax.random.uniform(arg_keys[8], (HEADS,), jnp.float32, -1.0, 3.0), -1.0, 3.0)
    head_gain = jnp.clip(1.0 + 0.18 * jax.random.normal(arg_keys[9], (HEADS * DV,), jnp.float32), 0.1, 1.9)
    w_out = scatter_about(arg_keys[10], (HEADS * DV, MODEL_WIDTH), (HEADS * DV) ** -0.5, 0.1875, ((0, 4),))
    memory = scatter_about(arg_keys[11], (TOKENS, HEADS, QK, DV), 0.06, 0.4, ((0, 8), (1, 4)), jnp.float32)
    normalizer = scatter_about(arg_keys[12], (TOKENS, HEADS, QK), 0.06, 0.4, ((0, 8), (1, 4)), jnp.float32)
    running_max = scatter_about(arg_keys[13], (TOKENS, HEADS), 1.0, 4.0, ((0, 8), (1, 4)), jnp.float32)
    ffn_gain = jnp.clip(1.0 + 0.18 * jax.random.normal(arg_keys[14], (MODEL_WIDTH,), jnp.float32), 0.1, 1.9)
    route_keys = jax.random.split(jax.random.fold_in(arg_keys[15], 1), TOKENS // TOKENS)
    route_turns = jax.random.permutation(jax.random.fold_in(arg_keys[15], 3), TOKENS // TOKENS)
    route = jax.vmap(lambda own, number: shared_out(jax.random.fold_in(arg_keys[15], 2), own, number, TOKENS, EXPERTS, TOPK, EXPERT_CAPACITY, 2))(route_keys, route_turns).reshape((TOKENS, TOPK))
    route_weight = jnp.clip(jnp.exp(jax.random.uniform(arg_keys[16], (TOKENS, TOPK), jnp.float32, math.log(0.05), math.log(1.0))), 0.05, 1.0)
    w_gate = scatter_about(arg_keys[17], (EXPERTS, MODEL_WIDTH, EXPERT_HIDDEN), MODEL_WIDTH ** -0.5, 0.1875, ((0, 8), (2, 4)))
    w_up = scatter_about(arg_keys[18], (EXPERTS, MODEL_WIDTH, EXPERT_HIDDEN), MODEL_WIDTH ** -0.5, 0.1875, ((0, 8), (2, 4)))
    w_down = scatter_about(arg_keys[19], (EXPERTS, EXPERT_HIDDEN, MODEL_WIDTH), EXPERT_HIDDEN ** -0.5, 0.25, ((0, 8), (1, 4)))
    return dict(tokens=tokens, mix_gain=mix_gain, w_query=w_query, w_key=w_key, w_value=w_value, w_ogate=w_ogate, w_igate=w_igate, w_fgate=w_fgate, forget_bias=forget_bias, head_gain=head_gain, w_out=w_out, memory=memory, normalizer=normalizer, running_max=running_max, ffn_gain=ffn_gain, route=route, route_weight=route_weight, w_gate=w_gate, w_up=w_up, w_down=w_down)


EPS = 1e-06

def round_trip(values):
    rounded = lax.optimization_barrier(values.astype(jnp.bfloat16))
    return rounded.astype(jnp.float32)

def norm_rows(values, gain):
    floats = values.astype(jnp.float32)
    scale = lax.rsqrt(lax.optimization_barrier(jnp.mean(floats * floats, axis=-1, keepdims=True)) + EPS)
    return (floats * scale * gain.astype(jnp.float32)).astype(jnp.bfloat16)

def slot_targets(route):
    flat = route.reshape(-1).astype(jnp.int32)
    onehot = (flat[:, None] == jnp.arange(EXPERTS, dtype=jnp.int32)[None, :]).astype(jnp.int32)
    before = jnp.cumsum(onehot, axis=0) - onehot
    slot = lax.optimization_barrier(jnp.sum(before * onehot, axis=1))
    return (flat * EXPERT_CAPACITY + slot).astype(jnp.int32)

def reference(tokens, mix_gain, w_query, w_key, w_value, w_ogate, w_igate, w_fgate, forget_bias, head_gain, w_out, memory, normalizer, running_max, ffn_gain, route, route_weight, w_gate, w_up, w_down):
    count = tokens.shape[0]
    normed = norm_rows(tokens, mix_gain)

    def project(weight, size):
        result = jnp.dot(normed, weight, preferred_element_type=jnp.float32)
        return round_trip(result).reshape(count, HEADS, size)
    query = project(w_query, QK)
    scaled_key = project(w_key, QK) * QK ** (-0.5)
    value = project(w_value, DV)
    ogate = project(w_ogate, DV)
    log_in = jnp.dot(normed, w_igate, preferred_element_type=jnp.float32)
    log_forget = jax.nn.log_sigmoid(jnp.dot(normed, w_fgate, preferred_element_type=jnp.float32) + forget_bias.astype(jnp.float32))
    new_max = jnp.maximum(log_forget + running_max, log_in)
    keep = jnp.exp(log_forget + running_max - new_max)
    admit = jnp.exp(log_in - new_max)
    floor = jnp.exp(-new_max)

    def per_head(items):
        state, norm_state, q_head, k_head, v_head, keep_head, admit_head, floor_head = items
        state = keep_head[:, None, None] * state + admit_head[:, None, None] * k_head[:, :, None] * v_head[:, None, :]
        norm_state = keep_head[:, None] * norm_state + admit_head[:, None] * k_head
        numer = jnp.einsum('tk,tkv->tv', q_head, state, precision=lax.Precision.HIGHEST)
        denom = lax.optimization_barrier(jnp.sum(q_head * norm_state, axis=1))
        read = numer / jnp.maximum(jnp.abs(denom), floor_head)[:, None]
        return (state, norm_state, read)
    heads_first = lambda a: jnp.moveaxis(a, 1, 0)
    states, norms, reads = lax.map(per_head, (heads_first(memory), heads_first(normalizer), heads_first(query), heads_first(scaled_key), heads_first(value), keep.T, admit.T, floor.T))
    new_memory = jnp.moveaxis(states, 0, 1)
    new_normalizer = jnp.moveaxis(norms, 0, 1)
    read = jnp.moveaxis(reads, 0, 1)
    scale = lax.rsqrt(lax.optimization_barrier(jnp.mean(read * read, axis=-1, keepdims=True)) + EPS)
    gated = (jax.nn.sigmoid(ogate) * read * scale * head_gain.reshape(HEADS, DV)).astype(jnp.bfloat16)
    partials = jnp.einsum('thv,hvd->htd', gated.astype(jnp.float32), w_out.reshape(HEADS, DV, MODEL_WIDTH).astype(jnp.float32))
    cell_out = lax.optimization_barrier(jnp.sum(round_trip(partials), axis=0))
    middle = (tokens.astype(jnp.float32) + cell_out).astype(jnp.bfloat16)
    routed_in = norm_rows(middle, ffn_gain)
    targets = slot_targets(route)
    slots = jnp.zeros((EXPERTS * EXPERT_CAPACITY, MODEL_WIDTH), jnp.bfloat16).at[targets].set(jnp.repeat(routed_in, TOPK, axis=0)).reshape(EXPERTS, EXPERT_CAPACITY, MODEL_WIDTH)

    def expert(items):
        rows, gate_m, up_m, down_matrix = items
        gate_v = jnp.dot(rows, gate_m, preferred_element_type=jnp.float32)
        up_v = jnp.dot(rows, up_m, preferred_element_type=jnp.float32)
        activation = (jax.nn.silu(gate_v) * up_v).astype(jnp.bfloat16)
        partial_pieces = jnp.einsum('pxt,xtl->xpl', activation.reshape(EXPERT_CAPACITY, N_TP, EXPERT_HIDDEN // N_TP).astype(jnp.float32), down_matrix.reshape(N_TP, EXPERT_HIDDEN // N_TP, MODEL_WIDTH).astype(jnp.float32))
        return lax.optimization_barrier(jnp.sum(round_trip(partial_pieces), axis=0)).astype(jnp.bfloat16)
    results = lax.map(expert, (slots, w_gate, w_up, w_down))
    picked = results.reshape(EXPERTS * EXPERT_CAPACITY, MODEL_WIDTH)[targets].reshape(count, TOPK, MODEL_WIDTH).astype(jnp.float32)
    weights = route_weight / lax.optimization_barrier(jnp.sum(route_weight, axis=1, keepdims=True))
    mixed = (middle.astype(jnp.float32) + lax.optimization_barrier(jnp.sum(picked * weights[:, :, None], axis=1))).astype(jnp.bfloat16)
    return (mixed, new_memory, new_normalizer, new_max)
```

```python
import functools

import jax
import jax.numpy as jnp
from jax import lax
from jax.experimental import pallas as pl
from jax.experimental.pallas import tpu as pltpu
from jax.sharding import PartitionSpec as P

EXPERT_CAPACITY = 32
EPS = 1e-06
LANES = 128
CHUNK_ROWS = 512

F32 = jnp.float32
BF16 = jnp.bfloat16


def iota(shape, dim):
    return lax.broadcasted_iota(jnp.int32, shape, dim)


def dot(a, b):
    return jnp.dot(a, b, preferred_element_type=F32)


def rounded(a, b):
    return dot(a, b).astype(BF16).astype(F32)


def norm_rows(floats, gain):
    scale = lax.rsqrt(jnp.mean(floats * floats, axis=-1, keepdims=True) + EPS)
    return (floats * scale * gain).astype(BF16)


def column_of(row, eye):
    return jnp.sum(jnp.where(eye, row, 0.0), axis=1, keepdims=True)


def row_of(column, eye):
    return jnp.sum(jnp.where(eye, column, 0.0), axis=0, keepdims=True)


def cell_kernel(
    head_ref, bias_ref, tokens_ref, mix_ref, wi_ref, wf_ref, hgain_ref, norm_ref, max_ref,
    wq_hbm, wk_hbm, wv_hbm, wo_hbm, mem_hbm, wout_hbm,
    part_ref, nstate_ref, nmax_ref, keep_ref, adk_ref, value_ref,
    wq, wk, wv, wo, mem, wout, sems,
):
    pairs = ((wq_hbm, wq), (wk_hbm, wk), (wv_hbm, wv), (wo_hbm, wo), (mem_hbm, mem), (wout_hbm, wout))
    copies = [pltpu.make_async_copy(src, dst, sems.at[i]) for i, (src, dst) in enumerate(pairs)]
    for copy in copies:
        copy.start()
    head = head_ref[0]
    rows = tokens_ref.shape[0]
    qk_dim = wq.shape[1]
    normed = norm_rows(tokens_ref[...].astype(F32), mix_ref[...])
    contract_last = (((1,), (1,)), ((), ()))
    pick = iota((rows, wi_ref.shape[0]), 1) == head
    gate_in = lax.dot_general(normed, wi_ref[...], contract_last, preferred_element_type=F32)
    gate_forget = lax.dot_general(normed, wf_ref[...], contract_last, preferred_element_type=F32)
    log_in = jnp.sum(jnp.where(pick, gate_in, 0.0), axis=1, keepdims=True)
    forget_pre = jnp.sum(jnp.where(pick, gate_forget, 0.0), axis=1, keepdims=True) + bias_ref[head]
    log_forget = jnp.minimum(forget_pre, 0.0) - jnp.log1p(jnp.exp(-jnp.abs(forget_pre)))
    eye = iota((rows, rows), 0) == iota((rows, rows), 1)
    carried = log_forget + column_of(max_ref[...], eye)
    new_max = jnp.maximum(carried, log_in)
    keep = jnp.exp(carried - new_max)
    admit = jnp.exp(log_in - new_max)
    nmax_ref[...] = row_of(new_max, eye)
    copies[0].wait()
    query = rounded(normed, wq[...])
    copies[1].wait()
    scaled_key = rounded(normed, wk[...]) * qk_dim ** (-0.5)
    admitted = admit * scaled_key
    norm_state = keep * norm_ref[...] + admitted
    nstate_ref[...] = norm_state
    adk_ref[...] = admitted
    keep_ref[...] = jnp.broadcast_to(keep, keep_ref.shape)
    denom = jnp.sum(query * norm_state, axis=1, keepdims=True)
    overlap = jnp.sum(query * admitted, axis=1, keepdims=True)
    query_cols = jnp.transpose(query)
    copies[2].wait()
    value = rounded(normed, wv[...])
    value_ref[...] = value
    copies[3].wait()
    ogate = rounded(normed, wo[...])
    copies[4].wait()
    reads = [
        jnp.sum(query_cols[:, t : t + 1] * mem[t], axis=0, keepdims=True) for t in range(rows)
    ]
    numer = keep * jnp.concatenate(reads, axis=0) + overlap * value
    read = numer / jnp.maximum(jnp.abs(denom), jnp.exp(-new_max))
    scale = lax.rsqrt(jnp.mean(read * read, axis=-1, keepdims=True) + EPS)
    gated = (jax.nn.sigmoid(ogate) * read * scale * hgain_ref[...]).astype(BF16)
    copies[5].wait()
    part_ref[...] = dot(gated, wout[...]).astype(BF16)


def state_kernel(keep_ref, adk_ref, value_ref, mem_ref, out_ref):
    block = mem_ref.shape[0]
    first = pl.program_id(0) * block
    rows = adk_ref.shape[0]
    adk_cols = jnp.transpose(adk_ref[...])
    for t in range(block):
        lane = iota(adk_cols.shape, 1) == first + t
        column = jnp.sum(jnp.where(lane, adk_cols, 0.0), axis=1, keepdims=True)
        keep = keep_ref[pl.ds(first + t, 1), :][:, 0:1]
        out_ref[t] = keep * mem_ref[t] + column * value_ref[pl.ds(first + t, 1), :]


def middle_kernel(*refs):
    tokens_ref, *parts, out_ref = refs
    total = parts[0][...].astype(F32)
    for part in parts[1:]:
        total = total + part[...].astype(F32)
    middle = (tokens_ref[...].astype(F32) + total).astype(BF16)
    for copy in range(out_ref.shape[0]):
        out_ref[copy] = middle


def earlier_matrix(count):
    return (iota((count, count), 0) < iota((count, count), 1)).astype(BF16)


def expert_kernel(
    place_ref, middle_ref, gain_ref, route_ref, weight_ref, wg_ref, wu_ref, wd_ref, own_ref, send_ref
):
    expert, half = place_ref[0], place_ref[1]
    count = middle_ref.shape[0]
    normed = norm_rows(middle_ref[...].astype(F32), gain_ref[...])
    route = route_ref[...]
    weight = weight_ref[...]
    named = route == expert
    share = jnp.where(named, weight, 0.0) / jnp.sum(weight, axis=0, keepdims=True)
    share = jnp.sum(share, axis=0, keepdims=True)
    member = jnp.sum(named.astype(F32), axis=0, keepdims=True)
    slot = dot(jnp.broadcast_to(member, (8, count)).astype(BF16), earlier_matrix(count))[0:1]
    shape = (EXPERT_CAPACITY, count)
    chosen = (iota(shape, 0).astype(F32) == slot) & (member > 0.5)
    rows = dot(chosen.astype(BF16), normed).astype(BF16)
    slot_share = jnp.sum(jnp.where(chosen, share, 0.0), axis=1, keepdims=True)
    gate = dot(rows, wg_ref[...])
    up = dot(rows, wu_ref[...])
    act = (jax.nn.silu(gate) * up).astype(BF16)
    result = (dot(act, wd_ref[...]) * slot_share).astype(BF16)
    part = own_ref.shape[0]
    low, high = result[:part], result[EXPERT_CAPACITY - part :]
    own_ref[...] = jnp.where(half == 0, low, high)
    send_ref[...] = jnp.where(half == 0, high, low)


def spread_kernel(own_ref, got_ref, out_ref):
    total = (own_ref[...].astype(F32) + got_ref[...].astype(F32)).astype(BF16)
    owners, copies, _, cols = out_ref.shape
    for owner in range(owners):
        piece = total[:, owner * cols : (owner + 1) * cols]
        for copy in range(copies):
            out_ref[owner, copy] = piece


def mix_kernel(middle_ref, route_ref, got_ref, out_ref, *, experts, sources, part):
    route = route_ref[...]
    count = route.shape[1]
    shape = (experts, count)
    member = jnp.zeros(shape, jnp.bool_)
    for choice in range(route.shape[0]):
        member = member | (iota(shape, 0) == route[choice : choice + 1])
    slots = dot(member.astype(BF16), earlier_matrix(count))
    slots = jnp.where(member, slots, -1.0).astype(BF16)
    total_rows = got_ref.shape[0]
    chunk = min(CHUNK_ROWS, total_rows)
    per_expert = sources * part

    def picked(start):
        column = iota((experts, chunk), 1) + start
        expand = (column // per_expert == iota((experts, chunk), 0)).astype(BF16)
        expanded = lax.dot_general(
            slots, expand, (((0,), (0,)), ((), ())), preferred_element_type=F32
        )
        column = iota((1, chunk), 1) + start
        source = (column // part) % sources
        groups = EXPERT_CAPACITY // part
        slot = (source % groups) * part + column % part
        pick = (expanded == slot.astype(F32)).astype(BF16)
        return dot(pick, got_ref[pl.ds(start, chunk), :])

    total = middle_ref[...].astype(F32)
    if total_rows == chunk:
        total = total + picked(0)
    else:
        total = lax.fori_loop(
            0, total_rows // chunk, lambda i, acc: acc + picked(i * chunk), total
        )
    out_ref[...] = total.astype(BF16)


def exchanged(values, axis):
    count = lax.axis_size(axis)
    if count & (count - 1) == 0:
        pairings = [[(i, i ^ k) for i in range(count)] for k in range(1, count)]
    else:
        pairings = [[(i, (i + k) % count) for i in range(count)] for k in range(1, count)]
    return [lax.ppermute(values, axis, pairing) for pairing in pairings]


def call(kernel, out_shape, in_specs, name, out_specs=None, **kw):
    vmem = pl.BlockSpec(memory_space=pltpu.VMEM)
    if out_specs is None:
        out_specs = jax.tree.map(lambda _: vmem, out_shape)
    return pl.pallas_call(
        kernel, out_shape=out_shape, in_specs=in_specs, out_specs=out_specs, name=name, **kw
    )


def shards(
    tokens, mix_gain, w_query, w_key, w_value, w_ogate, w_igate, w_fgate, forget_bias, head_gain,
    w_out, memory, normalizer, running_max, ffn_gain, route, route_weight, w_gate, w_up, w_down,
):
    vmem = pl.BlockSpec(memory_space=pltpu.VMEM)
    smem = pl.BlockSpec(memory_space=pltpu.SMEM)
    hbm = pl.BlockSpec(memory_space=pl.ANY)
    owners, heads = lax.axis_size("ep"), lax.axis_size("tp")
    rows, width = tokens.shape
    cols = width // owners
    count = route.shape[0]
    qk_dim, dv = w_query.shape[1], w_value.shape[1]
    head = lax.axis_index("tp")
    spec = jax.ShapeDtypeStruct

    partial, norm_state, new_max, keep, admitted, value = call(
        cell_kernel,
        (
            spec((rows, width), BF16),
            spec((rows, qk_dim), F32),
            spec((1, rows), F32),
            spec((rows, LANES), F32),
            spec((rows, qk_dim), F32),
            spec((rows, dv), F32),
        ),
        [smem, smem] + [vmem] * 7 + [hbm] * 6,
        "cell",
        scratch_shapes=[
            pltpu.VMEM(w_query.shape, BF16),
            pltpu.VMEM(w_key.shape, BF16),
            pltpu.VMEM(w_value.shape, BF16),
            pltpu.VMEM(w_ogate.shape, BF16),
            pltpu.VMEM((rows, qk_dim, dv), F32),
            pltpu.VMEM(w_out.shape, BF16),
            pltpu.SemaphoreType.DMA((6,)),
        ],
    )(
        head.reshape(1),
        forget_bias,
        tokens,
        mix_gain.reshape(1, -1),
        w_igate.T,
        w_fgate.T,
        head_gain.reshape(1, -1),
        normalizer.reshape(rows, qk_dim),
        running_max.T,
        w_query,
        w_key,
        w_value,
        w_ogate,
        memory.reshape(rows, qk_dim, dv),
        w_out,
    )

    block = 2 if rows % 2 == 0 else 1
    mem_spec = pl.BlockSpec((block, qk_dim, dv), lambda i: (i, 0, 0))
    whole = lambda shape: pl.BlockSpec(shape, lambda i: (0, 0))
    state = call(
        state_kernel,
        spec((rows, qk_dim, dv), F32),
        [whole(keep.shape), whole(admitted.shape), whole(value.shape), mem_spec],
        "state",
        out_specs=mem_spec,
        grid=(rows // block,),
        cost_estimate=pl.CostEstimate(flops=1 << 23, bytes_accessed=1 << 21, transcendentals=0),
    )(keep, admitted, value, memory.reshape(rows, qk_dim, dv))

    parts = exchanged(partial, "tp")
    spread = call(
        middle_kernel, spec((owners, rows, width), BF16), [vmem] * (2 + len(parts)), "middle"
    )(tokens, partial, *parts)
    middle = lax.all_to_all(spread, "ep", split_axis=0, concat_axis=0, tiled=True)
    middle = middle.reshape(count, width)
    place = lax.axis_index("ep")
    own_middle = lax.dynamic_slice_in_dim(middle, place * cols, cols, axis=1)

    groups = 2 if heads % 2 == 0 else 1
    part = EXPERT_CAPACITY // groups
    half = head % groups
    own, send = call(
        expert_kernel,
        (spec((part, width), BF16), spec((part, width), BF16)),
        [smem] + [vmem] * 7,
        "expert",
    )(
        jnp.stack([place, half]).astype(jnp.int32),
        middle,
        ffn_gain.reshape(1, -1),
        route.T,
        route_weight.T,
        w_gate[0],
        w_up[0],
        w_down[0],
    )
    if groups == 2:
        got = lax.ppermute(send, "tp", [(i, i ^ 1) for i in range(heads)])
    else:
        got = jnp.zeros_like(send)
    if cols % LANES == 0:
        pieces = call(
            spread_kernel, spec((owners, heads, part, cols), BF16), [vmem, vmem], "spread"
        )(own, got)
    else:
        total = (own.astype(F32) + got.astype(F32)).astype(BF16)
        total = total.reshape(part, owners, cols).transpose(1, 0, 2)
        pieces = jnp.broadcast_to(total[:, None], (owners, heads, part, cols))
    pieces = pieces.reshape(owners * heads, part, cols)
    results = lax.all_to_all(pieces, ("ep", "tp"), split_axis=0, concat_axis=0, tiled=True)
    mixed = call(
        functools.partial(mix_kernel, experts=owners, sources=heads, part=part),
        spec((count, cols), BF16),
        [vmem] * 3,
        "mix",
    )(own_middle, route.T, results.reshape(owners * heads * part, cols))
    return (
        mixed,
        state.reshape(memory.shape),
        norm_state.reshape(normalizer.shape),
        new_max.T,
    )


def solution(mesh):
    return jax.shard_map(
        shards,
        mesh=mesh,
        in_specs=(
            P("ep", None),
            P(),
            P(None, "tp"),
            P(None, "tp"),
            P(None, "tp"),
            P(None, "tp"),
            P(),
            P(),
            P(),
            P("tp"),
            P("tp", None),
            P("ep", "tp", None, None),
            P("ep", "tp", None),
            P("ep", "tp"),
            P(),
            P(),
            P(),
            P("ep", None, "tp"),
            P("ep", None, "tp"),
            P("ep", "tp", None),
        ),
        out_specs=(P(None, "ep"), P("ep", "tp", None, None), P("ep", "tp", None), P("ep", "tp")),
        check_vma=False,
    )
```

```python
import functools

import jax
import jax.numpy as jnp
from jax import lax
from jax.experimental import pallas as pl
from jax.experimental.pallas import tpu as pltpu
from jax.sharding import PartitionSpec as P

EXPERT_CAPACITY = 32
EPS = 1e-06
LANES = 128
CHUNK_ROWS = 512
VMEM_LIMIT = 32 << 20

F32 = jnp.float32
BF16 = jnp.bfloat16


def iota(shape, dim):
    return lax.broadcasted_iota(jnp.int32, shape, dim)


def dot(a, b):
    return jnp.dot(a, b, preferred_element_type=F32)


def rounded(a, b):
    return dot(a, b).astype(BF16).astype(F32)


def norm_rows(floats, gain):
    scale = lax.rsqrt(jnp.mean(floats * floats, axis=-1, keepdims=True) + EPS)
    return (floats * scale * gain).astype(BF16)


def column_of(row, eye):
    return jnp.sum(jnp.where(eye, row, 0.0), axis=1, keepdims=True)


def row_of(column, eye):
    return jnp.sum(jnp.where(eye, column, 0.0), axis=0, keepdims=True)


def cell_kernel(
    head_ref, bias_ref, tokens_ref, mix_ref, wi_ref, wf_ref, hgain_ref, norm_ref, max_ref,
    wq_hbm, wk_hbm, wv_hbm, wo_hbm, mem_hbm, wout_hbm,
    part_ref, nstate_ref, nmax_ref, keep_ref, adk_ref, value_ref,
    wq, wk, wv, wo, mem, wout, sems,
):
    pairs = ((wq_hbm, wq), (wk_hbm, wk), (wv_hbm, wv), (wo_hbm, wo), (mem_hbm, mem), (wout_hbm, wout))
    copies = [pltpu.make_async_copy(src, dst, sems.at[i]) for i, (src, dst) in enumerate(pairs)]
    for copy in copies:
        copy.start()
    head = head_ref[0]
    rows = tokens_ref.shape[0]
    qk_dim = wq.shape[1]
    normed = norm_rows(tokens_ref[...].astype(F32), mix_ref[...])
    contract_last = (((1,), (1,)), ((), ()))
    pick = iota((rows, wi_ref.shape[0]), 1) == head
    gate_in = lax.dot_general(normed, wi_ref[...], contract_last, preferred_element_type=F32)
    gate_forget = lax.dot_general(normed, wf_ref[...], contract_last, preferred_element_type=F32)
    log_in = jnp.sum(jnp.where(pick, gate_in, 0.0), axis=1, keepdims=True)
    forget_pre = jnp.sum(jnp.where(pick, gate_forget, 0.0), axis=1, keepdims=True) + bias_ref[head]
    log_forget = jnp.minimum(forget_pre, 0.0) - jnp.log1p(jnp.exp(-jnp.abs(forget_pre)))
    eye = iota((rows, rows), 0) == iota((rows, rows), 1)
    carried = log_forget + column_of(max_ref[...], eye)
    new_max = jnp.maximum(carried, log_in)
    keep = jnp.exp(carried - new_max)
    admit = jnp.exp(log_in - new_max)
    nmax_ref[...] = row_of(new_max, eye)
    copies[0].wait()
    query = rounded(normed, wq[...])
    copies[1].wait()
    scaled_key = rounded(normed, wk[...]) * qk_dim ** (-0.5)
    admitted = admit * scaled_key
    norm_state = keep * norm_ref[...] + admitted
    nstate_ref[...] = norm_state
    adk_ref[...] = admitted
    keep_ref[...] = jnp.broadcast_to(keep, keep_ref.shape)
    denom = jnp.sum(query * norm_state, axis=1, keepdims=True)
    overlap = jnp.sum(query * admitted, axis=1, keepdims=True)
    query_cols = jnp.transpose(query)
    copies[2].wait()
    value = rounded(normed, wv[...])
    value_ref[...] = value
    copies[3].wait()
    ogate = rounded(normed, wo[...])
    copies[4].wait()
    reads = [
        jnp.sum(query_cols[:, t : t + 1] * mem[t], axis=0, keepdims=True) for t in range(rows)
    ]
    numer = keep * jnp.concatenate(reads, axis=0) + overlap * value
    read = numer / jnp.maximum(jnp.abs(denom), jnp.exp(-new_max))
    scale = lax.rsqrt(jnp.mean(read * read, axis=-1, keepdims=True) + EPS)
    gated = (jax.nn.sigmoid(ogate) * read * scale * hgain_ref[...]).astype(BF16)
    copies[5].wait()
    part_ref[...] = dot(gated, wout[...]).astype(BF16)


def state_kernel(keep_ref, adk_ref, value_ref, mem_ref, out_ref):
    block = mem_ref.shape[0]
    first = pl.program_id(0) * block
    rows = adk_ref.shape[0]
    adk_cols = jnp.transpose(adk_ref[...])
    for t in range(block):
        lane = iota(adk_cols.shape, 1) == first + t
        column = jnp.sum(jnp.where(lane, adk_cols, 0.0), axis=1, keepdims=True)
        keep = keep_ref[pl.ds(first + t, 1), :][:, 0:1]
        out_ref[t] = keep * mem_ref[t] + column * value_ref[pl.ds(first + t, 1), :]


def middle_kernel(*refs):
    tokens_ref, *parts, out_ref = refs
    total = parts[0][...].astype(F32)
    for part in parts[1:]:
        total = total + part[...].astype(F32)
    middle = (tokens_ref[...].astype(F32) + total).astype(BF16)
    for copy in range(out_ref.shape[0]):
        out_ref[copy] = middle


def earlier_matrix(count):
    return (iota((count, count), 0) < iota((count, count), 1)).astype(BF16)


def plan_kernel(
    place_ref, gain_ref, route_ref, weight_ref, chosen_ref, share_ref, gain_out_ref, *pick_refs,
    experts, sources, part,
):
    route = route_ref[...]
    weight = weight_ref[...]
    count = route.shape[1]
    earlier = earlier_matrix(count)
    named = route == place_ref[0]
    share = jnp.where(named, weight, 0.0) / jnp.sum(weight, axis=0, keepdims=True)
    share = jnp.sum(share, axis=0, keepdims=True)
    member = jnp.sum(named.astype(F32), axis=0, keepdims=True)
    slot = dot(jnp.broadcast_to(member, (8, count)).astype(BF16), earlier)[0:1]
    shape = (EXPERT_CAPACITY, count)
    chosen = (iota(shape, 0).astype(F32) == slot) & (member > 0.5)
    chosen_ref[...] = chosen.astype(BF16)
    slot_share = jnp.sum(jnp.where(chosen, share, 0.0), axis=1, keepdims=True)
    share_ref[...] = jnp.broadcast_to(slot_share, share_ref.shape)
    gain_out_ref[...] = gain_ref[...]
    for pick_ref in pick_refs:
        slots = slot_table(route, experts)
        pick_ref[...] = pick_matrix(slots, 0, pick_ref.shape[1], sources, part)


def slot_table(route, experts):
    count = route.shape[1]
    shape = (experts, count)
    member = jnp.zeros(shape, jnp.bool_)
    for choice in range(route.shape[0]):
        member = member | (iota(shape, 0) == route[choice : choice + 1])
    slots = dot(member.astype(BF16), earlier_matrix(count))
    return jnp.where(member, slots, -1.0).astype(BF16)


def pick_matrix(slots, start, size, sources, part):
    experts = slots.shape[0]
    column = iota((experts, size), 1) + start
    expand = (column // (sources * part) == iota((experts, size), 0)).astype(BF16)
    expanded = lax.dot_general(
        slots, expand, (((0,), (0,)), ((), ())), preferred_element_type=F32
    )
    column = iota((1, size), 1) + start
    source = (column // part) % sources
    slot = (source % (EXPERT_CAPACITY // part)) * part + column % part
    return (expanded == slot.astype(F32)).astype(BF16)


def expert_kernel(
    place_ref, middle_ref, gain_ref, chosen_ref, share_ref, wg_ref, wu_ref, wd_ref,
    own_ref, send_ref, *block_refs,
):
    expert, half = place_ref[0], place_ref[1]
    for block_ref in block_refs:
        cols = block_ref.shape[1]
        block_ref[...] = middle_ref[:, pl.ds(pl.multiple_of(expert * cols, cols), cols)]
    normed = norm_rows(middle_ref[...].astype(F32), gain_ref[...])
    rows = dot(chosen_ref[...], normed).astype(BF16)
    gate = dot(rows, wg_ref[...])
    up = dot(rows, wu_ref[...])
    act = (jax.nn.silu(gate) * up).astype(BF16)
    result = (dot(act, wd_ref[...]) * share_ref[:, 0:1]).astype(BF16)
    part = own_ref.shape[0]
    low, high = result[:part], result[EXPERT_CAPACITY - part :]
    own_ref[...] = jnp.where(half == 0, low, high)
    send_ref[...] = jnp.where(half == 0, high, low)


def spread_kernel(own_ref, got_ref, out_ref):
    total = (own_ref[...].astype(F32) + got_ref[...].astype(F32)).astype(BF16)
    owners, copies, _, cols = out_ref.shape
    for owner in range(owners):
        piece = total[:, owner * cols : (owner + 1) * cols]
        for copy in range(copies):
            out_ref[owner, copy] = piece


def mix_kernel(middle_ref, pick_ref, got_ref, out_ref):
    total = middle_ref[...].astype(F32) + dot(pick_ref[...], got_ref[...])
    out_ref[...] = total.astype(BF16)


def long_mix_kernel(middle_ref, route_ref, got_ref, out_ref, *, experts, sources, part):
    slots = slot_table(route_ref[...], experts)

    def add(step, total):
        start = step * CHUNK_ROWS
        pick = pick_matrix(slots, start, CHUNK_ROWS, sources, part)
        return total + dot(pick, got_ref[pl.ds(start, CHUNK_ROWS), :])

    steps = got_ref.shape[0] // CHUNK_ROWS
    total = lax.fori_loop(0, steps, add, middle_ref[...].astype(F32))
    out_ref[...] = total.astype(BF16)


def exchanged(values, axis):
    count = lax.axis_size(axis)
    if count & (count - 1) == 0:
        pairings = [[(i, i ^ k) for i in range(count)] for k in range(1, count)]
    else:
        pairings = [[(i, (i + k) % count) for i in range(count)] for k in range(1, count)]
    return [lax.ppermute(values, axis, pairing) for pairing in pairings]


def near(values):
    return pltpu.with_memory_space_constraint(values, pltpu.VMEM)


def far(values):
    return pltpu.with_memory_space_constraint(values, pltpu.HBM)


def call(kernel, out_shape, in_specs, name, out_specs=None, **kw):
    if out_specs is None:
        vmem = pl.BlockSpec(memory_space=pltpu.VMEM)
        out_specs = [vmem] * len(out_shape) if isinstance(out_shape, tuple) else vmem
    return pl.pallas_call(
        kernel,
        out_shape=out_shape,
        in_specs=in_specs,
        out_specs=out_specs,
        name=name,
        compiler_params=pltpu.CompilerParams(vmem_limit_bytes=VMEM_LIMIT),
        **kw,
    )


def shards(
    tokens, mix_gain, w_query, w_key, w_value, w_ogate, w_igate, w_fgate, forget_bias, head_gain,
    w_out, memory, normalizer, running_max, ffn_gain, route, route_weight, w_gate, w_up, w_down,
):
    vmem = pl.BlockSpec(memory_space=pltpu.VMEM)
    smem = pl.BlockSpec(memory_space=pltpu.SMEM)
    hbm = pl.BlockSpec(memory_space=pl.ANY)
    owners, heads = lax.axis_size("ep"), lax.axis_size("tp")
    rows, width = tokens.shape
    cols = width // owners
    count = route.shape[0]
    qk_dim, dv = w_query.shape[1], w_value.shape[1]
    head = lax.axis_index("tp")
    spec = jax.ShapeDtypeStruct

    partial, norm_state, new_max, keep, admitted, value = call(
        cell_kernel,
        (
            pltpu.VMEM((rows, width), BF16),
            spec((rows, qk_dim), F32),
            spec((1, rows), F32),
            pltpu.VMEM((rows, LANES), F32),
            pltpu.VMEM((rows, qk_dim), F32),
            pltpu.VMEM((rows, dv), F32),
        ),
        [smem, smem] + [vmem] * 7 + [hbm] * 6,
        "cell",
        scratch_shapes=[
            pltpu.VMEM(w_query.shape, BF16),
            pltpu.VMEM(w_key.shape, BF16),
            pltpu.VMEM(w_value.shape, BF16),
            pltpu.VMEM(w_ogate.shape, BF16),
            pltpu.VMEM((rows, qk_dim, dv), F32),
            pltpu.VMEM(w_out.shape, BF16),
            pltpu.SemaphoreType.DMA((6,)),
        ],
    )(
        head.reshape(1),
        forget_bias,
        far(tokens),
        far(mix_gain.reshape(1, -1)),
        far(w_igate.T),
        far(w_fgate.T),
        far(head_gain.reshape(1, -1)),
        far(normalizer.reshape(rows, qk_dim)),
        far(running_max.T),
        far(w_query),
        far(w_key),
        far(w_value),
        far(w_ogate),
        far(memory.reshape(rows, qk_dim, dv)),
        far(w_out),
    )

    block = 2 if rows % 2 == 0 else 1
    mem_spec = pl.BlockSpec((block, qk_dim, dv), lambda i: (i, 0, 0))
    whole = lambda shape: pl.BlockSpec(shape, lambda i: (0, 0))
    state = call(
        state_kernel,
        spec((rows, qk_dim, dv), F32),
        [whole(keep.shape), whole(admitted.shape), whole(value.shape), mem_spec],
        "state",
        out_specs=mem_spec,
        grid=(rows // block,),
        cost_estimate=pl.CostEstimate(flops=1 << 23, bytes_accessed=1 << 21, transcendentals=0),
    )(near(keep), near(admitted), near(value), far(memory.reshape(rows, qk_dim, dv)))

    parts = exchanged(partial, "tp")
    spread = call(
        middle_kernel, pltpu.VMEM((owners, rows, width), BF16), [vmem] * (2 + len(parts)), "middle"
    )(near(tokens), near(partial), *map(near, parts))
    middle = lax.all_to_all(spread, "ep", split_axis=0, concat_axis=0, tiled=True)
    middle = middle.reshape(count, width)
    place = lax.axis_index("ep")
    groups = 2 if heads % 2 == 0 else 1
    part = EXPERT_CAPACITY // groups
    half = lax.bitwise_and(head, groups - 1)
    places = jnp.stack([place, half]).astype(jnp.int32)
    got_rows = owners * heads * part
    short = got_rows <= CHUNK_ROWS
    aligned = cols % LANES == 0
    sizes = dict(experts=owners, sources=heads, part=part)
    chosen, share, gain, *pick = call(
        functools.partial(plan_kernel, **sizes),
        (
            pltpu.VMEM((EXPERT_CAPACITY, count), BF16),
            pltpu.VMEM((EXPERT_CAPACITY, LANES), F32),
            pltpu.VMEM((1, width), F32),
        )
        + ((pltpu.VMEM((count, got_rows), BF16),) if short else ()),
        [smem] + [vmem] * 3,
        "plan",
        cost_estimate=pl.CostEstimate(flops=1 << 22, bytes_accessed=1 << 16, transcendentals=0),
    )(places, far(ffn_gain.reshape(1, -1)), far(route.T), far(route_weight.T))
    own, send, *own_middle = call(
        expert_kernel,
        (pltpu.VMEM((part, width), BF16), pltpu.VMEM((part, width), BF16))
        + ((pltpu.VMEM((count, cols), BF16),) if aligned else ()),
        [smem] + [vmem] * 7,
        "expert",
    )(
        places,
        near(middle),
        near(gain),
        near(chosen),
        near(share),
        near(w_gate[0]),
        near(w_up[0]),
        near(w_down[0]),
    )
    if not aligned:
        own_middle = [lax.dynamic_slice_in_dim(middle, place * cols, cols, axis=1)]
    if groups == 2:
        got = lax.ppermute(send, "tp", [(i, i ^ 1) for i in range(heads)])
    else:
        got = jnp.zeros_like(send)
    if aligned:
        pieces = call(
            spread_kernel, pltpu.VMEM((owners, heads, part, cols), BF16), [vmem, vmem], "spread"
        )(near(own), near(got))
    else:
        total = (own.astype(F32) + got.astype(F32)).astype(BF16)
        total = total.reshape(part, owners, cols).transpose(1, 0, 2)
        pieces = jnp.broadcast_to(total[:, None], (owners, heads, part, cols))
    pieces = pieces.reshape(owners * heads, part, cols)
    results = lax.all_to_all(pieces, ("ep", "tp"), split_axis=0, concat_axis=0, tiled=True)
    results = near(results.reshape(got_rows, cols))
    if short:
        mixed = call(mix_kernel, spec((count, cols), BF16), [vmem] * 3, "mix")(
            near(own_middle[0]), near(pick[0]), results
        )
    else:
        mixed = call(
            functools.partial(long_mix_kernel, **sizes),
            spec((count, cols), BF16),
            [vmem] * 3,
            "mix",
        )(own_middle[0], route.T, results)
    return (
        mixed,
        state.reshape(memory.shape),
        norm_state.reshape(normalizer.shape),
        new_max.T,
    )


def solution(mesh):
    return jax.shard_map(
        shards,
        mesh=mesh,
        in_specs=(
            P("ep", None),
            P(),
            P(None, "tp"),
            P(None, "tp"),
            P(None, "tp"),
            P(None, "tp"),
            P(),
            P(),
            P(),
            P("tp"),
            P("tp", None),
            P("ep", "tp", None, None),
            P("ep", "tp", None),
            P("ep", "tp"),
            P(),
            P(),
            P(),
            P("ep", None, "tp"),
            P("ep", None, "tp"),
            P("ep", "tp", None),
        ),
        out_specs=(P(None, "ep"), P("ep", "tp", None, None), P("ep", "tp", None), P("ep", "tp")),
        check_vma=False,
    )
```

```python
import functools

import jax
import jax.numpy as jnp
from jax import lax
from jax.experimental import pallas as pl
from jax.experimental.pallas import tpu as pltpu
from jax.sharding import PartitionSpec as P

EXPERT_CAPACITY = 32
EPS = 1e-06
LANES = 128
CHUNK_ROWS = 512
VMEM_LIMIT = 32 << 20
CELL_INPUTS = (
    "tokens", "mix", "wi", "wf", "bias", "max", "wq", "wk", "norm", "mem", "wv", "wo", "hgain", "wout"
)

F32 = jnp.float32
BF16 = jnp.bfloat16


def iota(shape, dim):
    return lax.broadcasted_iota(jnp.int32, shape, dim)


def dot(a, b):
    return jnp.dot(a, b, preferred_element_type=F32)


def rounded(a, b):
    return dot(a, b).astype(BF16).astype(F32)


def norm_rows(floats, gain):
    scale = lax.rsqrt(jnp.mean(floats * floats, axis=-1, keepdims=True) + EPS)
    return (floats * scale * gain).astype(BF16)


def column_of(row, eye):
    return jnp.sum(jnp.where(eye, row, 0.0), axis=1, keepdims=True)


def row_of(column, eye):
    return jnp.sum(jnp.where(eye, column, 0.0), axis=0, keepdims=True)


def cell_kernel(*refs):
    count = len(CELL_INPUTS)
    far_refs, outs, near_refs, sems = refs[:count], refs[count:-count - 1], refs[-count - 1 : -1], refs[-1]
    part_ref, nstate_ref, nmax_ref, keep_ref, adk_ref, value_ref, mem_ref = outs
    copies, local = {}, {}
    for i, name in enumerate(CELL_INPUTS):
        local[name] = mem_ref if name == "mem" else near_refs[i]
        copies[name] = pltpu.make_async_copy(far_refs[i], local[name], sems.at[i])
        copies[name].start()

    def ready(name):
        copies[name].wait()
        return local[name]

    head = lax.axis_index("tp")
    tokens = ready("tokens")[...].astype(F32)
    rows = tokens.shape[0]
    normed = norm_rows(tokens, ready("mix")[...])
    contract_last = (((1,), (1,)), ((), ()))
    wi_ref, wf_ref = ready("wi"), ready("wf")
    bias, old_max = ready("bias")[...], ready("max")[...]
    heads = bias.shape[1]
    pick = iota((rows, heads), 1) == head
    gate_in = lax.dot_general(normed, wi_ref[...], contract_last, preferred_element_type=F32)
    gate_forget = lax.dot_general(normed, wf_ref[...], contract_last, preferred_element_type=F32)
    log_in = jnp.sum(jnp.where(pick, gate_in, 0.0), axis=1, keepdims=True)
    forget_pre = jnp.sum(jnp.where(pick, gate_forget + bias, 0.0), axis=1, keepdims=True)
    log_forget = jnp.minimum(forget_pre, 0.0) - jnp.log1p(jnp.exp(-jnp.abs(forget_pre)))
    eye = iota((rows, rows), 0) == iota((rows, rows), 1)
    carried = log_forget + column_of(old_max, eye)
    new_max = jnp.maximum(carried, log_in)
    keep = jnp.exp(carried - new_max)
    admit = jnp.exp(log_in - new_max)
    nmax_ref[...] = row_of(new_max, eye)
    query = rounded(normed, ready("wq")[...])
    scaled_key = rounded(normed, ready("wk")[...]) * query.shape[1] ** (-0.5)
    admitted = admit * scaled_key
    norm_state = keep * ready("norm")[...] + admitted
    nstate_ref[...] = norm_state
    adk_ref[...] = admitted
    keep_ref[...] = jnp.broadcast_to(keep, keep_ref.shape)
    denom = jnp.sum(query * norm_state, axis=1, keepdims=True)
    overlap = jnp.sum(query * admitted, axis=1, keepdims=True)
    query_cols = jnp.transpose(query)
    mem = ready("mem")
    reads = [
        jnp.sum(query_cols[:, t : t + 1] * mem[t], axis=0, keepdims=True) for t in range(rows)
    ]
    value = rounded(normed, ready("wv")[...])
    value_ref[...] = value
    numer = keep * jnp.concatenate(reads, axis=0) + overlap * value
    read = numer / jnp.maximum(jnp.abs(denom), jnp.exp(-new_max))
    scale = lax.rsqrt(jnp.mean(read * read, axis=-1, keepdims=True) + EPS)
    ogate = rounded(normed, ready("wo")[...])
    gated = (jax.nn.sigmoid(ogate) * read * scale * ready("hgain")[...]).astype(BF16)
    part_ref[...] = dot(gated, ready("wout")[...]).astype(BF16)


def middle_kernel(*refs):
    tokens_ref, *parts, out_ref = refs
    total = parts[0][...].astype(F32)
    for part in parts[1:]:
        total = total + part[...].astype(F32)
    middle = (tokens_ref[...].astype(F32) + total).astype(BF16)
    for copy in range(out_ref.shape[0]):
        out_ref[copy] = middle


def earlier_matrix(count):
    return (iota((count, count), 0) < iota((count, count), 1)).astype(BF16)


def plan_kernel(
    place_ref, nstate_ref, nmax_ref, gain_ref, route_ref, weight_ref,
    nstate_out_ref, nmax_out_ref, chosen_ref, share_ref, gain_out_ref, *pick_refs,
    experts, sources, part,
):
    nstate_out_ref[...] = nstate_ref[...]
    nmax_out_ref[...] = nmax_ref[...]
    route = route_ref[...]
    weight = weight_ref[...]
    count = route.shape[1]
    earlier = earlier_matrix(count)
    named = route == place_ref[0]
    share = jnp.where(named, weight, 0.0) / jnp.sum(weight, axis=0, keepdims=True)
    share = jnp.sum(share, axis=0, keepdims=True)
    member = jnp.sum(named.astype(F32), axis=0, keepdims=True)
    slot = dot(jnp.broadcast_to(member, (8, count)).astype(BF16), earlier)[0:1]
    shape = (EXPERT_CAPACITY, count)
    chosen = (iota(shape, 0).astype(F32) == slot) & (member > 0.5)
    chosen_ref[...] = chosen.astype(BF16)
    slot_share = jnp.sum(jnp.where(chosen, share, 0.0), axis=1, keepdims=True)
    share_ref[...] = jnp.broadcast_to(slot_share, share_ref.shape)
    gain_out_ref[...] = gain_ref[...]
    for pick_ref in pick_refs:
        slots = slot_table(route, experts)
        pick_ref[...] = pick_matrix(slots, 0, pick_ref.shape[1], sources, part)


def slot_table(route, experts):
    count = route.shape[1]
    shape = (experts, count)
    member = jnp.zeros(shape, jnp.bool_)
    for choice in range(route.shape[0]):
        member = member | (iota(shape, 0) == route[choice : choice + 1])
    slots = dot(member.astype(BF16), earlier_matrix(count))
    return jnp.where(member, slots, -1.0).astype(BF16)


def pick_matrix(slots, start, size, sources, part):
    experts = slots.shape[0]
    column = iota((experts, size), 1) + start
    expand = (column // (sources * part) == iota((experts, size), 0)).astype(BF16)
    expanded = lax.dot_general(
        slots, expand, (((0,), (0,)), ((), ())), preferred_element_type=F32
    )
    column = iota((1, size), 1) + start
    source = (column // part) % sources
    slot = (source % (EXPERT_CAPACITY // part)) * part + column % part
    return (expanded == slot.astype(F32)).astype(BF16)


def expert_kernel(
    place_ref, middle_ref, gain_ref, chosen_ref, share_ref, wg_ref, wu_ref, wd_ref,
    own_ref, send_ref, *block_refs,
):
    expert, half = place_ref[0], place_ref[1]
    for block_ref in block_refs:
        cols = block_ref.shape[1]
        block_ref[...] = middle_ref[:, pl.ds(pl.multiple_of(expert * cols, cols), cols)]
    normed = norm_rows(middle_ref[...].astype(F32), gain_ref[...])
    rows = dot(chosen_ref[...], normed).astype(BF16)
    gate = dot(rows, wg_ref[...])
    up = dot(rows, wu_ref[...])
    act = (jax.nn.silu(gate) * up).astype(BF16)
    result = (dot(act, wd_ref[...]) * share_ref[:, 0:1]).astype(BF16)
    part = own_ref.shape[0]
    low, high = result[:part], result[EXPERT_CAPACITY - part :]
    own_ref[...] = jnp.where(half == 0, low, high)
    send_ref[...] = jnp.where(half == 0, high, low)


def spread_kernel(own_ref, got_ref, out_ref):
    total = (own_ref[...].astype(F32) + got_ref[...].astype(F32)).astype(BF16)
    owners, copies, _, cols = out_ref.shape
    for owner in range(owners):
        piece = total[:, owner * cols : (owner + 1) * cols]
        for copy in range(copies):
            out_ref[owner, copy] = piece


def mix_kernel(middle_ref, pick_ref, got_ref, out_ref):
    total = middle_ref[...].astype(F32) + dot(pick_ref[...], got_ref[...])
    out_ref[...] = total.astype(BF16)


def long_mix_kernel(middle_ref, route_ref, got_ref, out_ref, *, experts, sources, part):
    slots = slot_table(route_ref[...], experts)

    def add(step, total):
        start = step * CHUNK_ROWS
        pick = pick_matrix(slots, start, CHUNK_ROWS, sources, part)
        return total + dot(pick, got_ref[pl.ds(start, CHUNK_ROWS), :])

    steps = got_ref.shape[0] // CHUNK_ROWS
    total = lax.fori_loop(0, steps, add, middle_ref[...].astype(F32))
    out_ref[...] = total.astype(BF16)


def exchanged(values, axis):
    count = lax.axis_size(axis)
    if count & (count - 1) == 0:
        pairings = [[(i, i ^ k) for i in range(count)] for k in range(1, count)]
    else:
        pairings = [[(i, (i + k) % count) for i in range(count)] for k in range(1, count)]
    return [lax.ppermute(values, axis, pairing) for pairing in pairings]


def near(values):
    return pltpu.with_memory_space_constraint(values, pltpu.VMEM)


def far(values):
    return pltpu.with_memory_space_constraint(values, pltpu.HBM)


def call(kernel, out_shape, in_specs, name, out_specs=None, **kw):
    if out_specs is None:
        vmem = pl.BlockSpec(memory_space=pltpu.VMEM)
        out_specs = [vmem] * len(out_shape) if isinstance(out_shape, tuple) else vmem
    return pl.pallas_call(
        kernel,
        out_shape=out_shape,
        in_specs=in_specs,
        out_specs=out_specs,
        name=name,
        compiler_params=pltpu.CompilerParams(vmem_limit_bytes=VMEM_LIMIT),
        **kw,
    )


def shards(
    tokens, mix_gain, w_query, w_key, w_value, w_ogate, w_igate, w_fgate, forget_bias, head_gain,
    w_out, memory, normalizer, running_max, ffn_gain, route, route_weight, w_gate, w_up, w_down,
):
    vmem = pl.BlockSpec(memory_space=pltpu.VMEM)
    smem = pl.BlockSpec(memory_space=pltpu.SMEM)
    hbm = pl.BlockSpec(memory_space=pl.ANY)
    owners, heads = lax.axis_size("ep"), lax.axis_size("tp")
    rows, width = tokens.shape
    cols = width // owners
    count = route.shape[0]
    qk_dim, dv = w_query.shape[1], w_value.shape[1]
    head = lax.axis_index("tp")
    spec = jax.ShapeDtypeStruct
    memory_rows = memory.reshape(rows, qk_dim, dv)
    cell_inputs = dict(
        tokens=tokens,
        mix=mix_gain.reshape(1, -1),
        wi=w_igate.T,
        wf=w_fgate.T,
        bias=forget_bias.reshape(1, -1),
        max=running_max.T,
        wq=w_query,
        wk=w_key,
        norm=normalizer.reshape(rows, qk_dim),
        mem=memory_rows,
        wv=w_value,
        wo=w_ogate,
        hgain=head_gain.reshape(1, -1),
        wout=w_out,
    )
    cell_inputs = [cell_inputs[name] for name in CELL_INPUTS]
    partial, norm_state, new_max, keep, admitted, value, near_memory = call(
        cell_kernel,
        (
            pltpu.VMEM((rows, width), BF16),
            pltpu.VMEM((rows, qk_dim), F32),
            pltpu.VMEM((1, rows), F32),
            pltpu.VMEM((rows, LANES), F32),
            pltpu.VMEM((rows, qk_dim), F32),
            pltpu.VMEM((rows, dv), F32),
            pltpu.VMEM((rows, qk_dim, dv), F32),
        ),
        [hbm] * len(cell_inputs),
        "cell",
        scratch_shapes=[
            pltpu.VMEM((8, LANES) if name == "mem" else x.shape, x.dtype)
            for name, x in zip(CELL_INPUTS, cell_inputs)
        ]
        + [pltpu.SemaphoreType.DMA((len(cell_inputs),))],
    )(*map(far, cell_inputs))

    state = keep[:, 0:1, None] * near_memory + admitted[:, :, None] * value[:, None, :]

    parts = exchanged(partial, "tp")
    place = lax.axis_index("ep")
    groups = 2 if heads % 2 == 0 else 1
    part = EXPERT_CAPACITY // groups
    half = lax.bitwise_and(head, groups - 1)
    places = jnp.stack([place, half]).astype(jnp.int32)
    got_rows = owners * heads * part
    short = got_rows <= CHUNK_ROWS
    aligned = cols % LANES == 0
    sizes = dict(experts=owners, sources=heads, part=part)
    norm_state, new_max, chosen, share, gain, *pick = call(
        functools.partial(plan_kernel, **sizes),
        (
            spec(norm_state.shape, F32),
            spec(new_max.shape, F32),
            pltpu.VMEM((EXPERT_CAPACITY, count), BF16),
            pltpu.VMEM((EXPERT_CAPACITY, LANES), F32),
            pltpu.VMEM((1, width), F32),
        )
        + ((pltpu.VMEM((count, got_rows), BF16),) if short else ()),
        [smem] + [vmem] * 5,
        "plan",
        cost_estimate=pl.CostEstimate(flops=1 << 22, bytes_accessed=1 << 16, transcendentals=0),
    )(places, near(norm_state), near(new_max), far(ffn_gain.reshape(1, -1)), far(route.T), far(route_weight.T))
    parts, state, norm_state, new_max, chosen, share, gain, pick = lax.optimization_barrier(
        (parts, state, norm_state, new_max, chosen, share, gain, pick)
    )
    spread = call(
        middle_kernel, pltpu.VMEM((owners, rows, width), BF16), [vmem] * (2 + len(parts)), "middle"
    )(near(tokens), near(partial), *map(near, parts))
    middle = lax.all_to_all(spread, "ep", split_axis=0, concat_axis=0, tiled=True)
    middle = middle.reshape(count, width)
    own, send, *own_middle = call(
        expert_kernel,
        (pltpu.VMEM((part, width), BF16), pltpu.VMEM((part, width), BF16))
        + ((pltpu.VMEM((count, cols), BF16),) if aligned else ()),
        [smem] + [vmem] * 7,
        "expert",
    )(
        places,
        near(middle),
        near(gain),
        near(chosen),
        near(share),
        near(w_gate[0]),
        near(w_up[0]),
        near(w_down[0]),
    )
    if not aligned:
        own_middle = [lax.dynamic_slice_in_dim(middle, place * cols, cols, axis=1)]
    if groups == 2:
        got = lax.ppermute(send, "tp", [(i, i ^ 1) for i in range(heads)])
    else:
        got = jnp.zeros_like(send)
    if aligned:
        pieces = call(
            spread_kernel, pltpu.VMEM((owners, heads, part, cols), BF16), [vmem, vmem], "spread"
        )(near(own), near(got))
    else:
        total = (own.astype(F32) + got.astype(F32)).astype(BF16)
        total = total.reshape(part, owners, cols).transpose(1, 0, 2)
        pieces = jnp.broadcast_to(total[:, None], (owners, heads, part, cols))
    pieces = pieces.reshape(owners * heads, part, cols)
    results = lax.all_to_all(pieces, ("ep", "tp"), split_axis=0, concat_axis=0, tiled=True)
    results = near(results.reshape(got_rows, cols))
    if short:
        mixed = call(mix_kernel, spec((count, cols), BF16), [vmem] * 3, "mix")(
            near(own_middle[0]), near(pick[0]), results
        )
    else:
        mixed = call(
            functools.partial(long_mix_kernel, **sizes),
            spec((count, cols), BF16),
            [vmem] * 3,
            "mix",
        )(own_middle[0], route.T, results)
    return (
        mixed,
        state.reshape(memory.shape),
        norm_state.reshape(normalizer.shape),
        new_max.T,
    )


def solution(mesh):
    return jax.shard_map(
        shards,
        mesh=mesh,
        in_specs=(
            P("ep", None),
            P(),
            P(None, "tp"),
            P(None, "tp"),
            P(None, "tp"),
            P(None, "tp"),
            P(),
            P(),
            P(),
            P("tp"),
            P("tp", None),
            P("ep", "tp", None, None),
            P("ep", "tp", None),
            P("ep", "tp"),
            P(),
            P(),
            P(),
            P("ep", None, "tp"),
            P("ep", None, "tp"),
            P("ep", "tp", None),
        ),
        out_specs=(P(None, "ep"), P("ep", "tp", None, None), P("ep", "tp", None), P("ep", "tp")),
        check_vma=False,
    )
```

```python
import functools

import jax
import jax.numpy as jnp
from jax import lax
from jax.experimental import pallas as pl
from jax.experimental.pallas import tpu as pltpu
from jax.sharding import PartitionSpec as P

EXPERT_CAPACITY = 32
EPS = 1e-06
LANES = 128
CHUNK_ROWS = 512
VMEM_LIMIT = 32 << 20
CELL_INPUTS = (
    "tokens", "mix", "wi", "wf", "bias", "max", "route", "share", "wq", "wk", "norm", "mem", "wv",
    "wo", "hgain", "wout", "fgain",
)

F32 = jnp.float32
BF16 = jnp.bfloat16


def iota(shape, dim):
    return lax.broadcasted_iota(jnp.int32, shape, dim)


def dot(a, b):
    return jnp.dot(a, b, preferred_element_type=F32)


def rounded(a, b):
    return dot(a, b).astype(BF16).astype(F32)


def norm_rows(floats, gain):
    scale = lax.rsqrt(jnp.mean(floats * floats, axis=-1, keepdims=True) + EPS)
    return (floats * scale * gain).astype(BF16)


def column_of(row, eye):
    return jnp.sum(jnp.where(eye, row, 0.0), axis=1, keepdims=True)


def row_of(column, eye):
    return jnp.sum(jnp.where(eye, column, 0.0), axis=0, keepdims=True)


def cell_kernel(*refs, experts, sources, part):
    count = len(CELL_INPUTS)
    far_refs, outs, scratch = refs[:count], refs[count : -count - 4], refs[-count - 4 :]
    near_refs, (nstate_near, nmax_near), (sems, out_sems) = scratch[:count], scratch[count:-2], scratch[-2:]
    (
        own_ref, send_ref, nstate_ref, nmax_ref, keep_ref, adk_ref, value_ref, mem_ref, gain_ref,
        chosen_ref, share_ref, *pick_refs,
    ) = outs
    direct = {"mem": mem_ref, "fgain": gain_ref}
    copies, local = {}, {}
    for i, name in enumerate(CELL_INPUTS):
        local[name] = direct.get(name, near_refs[i])
        copies[name] = pltpu.make_async_copy(far_refs[i], local[name], sems.at[i])
        copies[name].start()

    def ready(name):
        copies[name].wait()
        return local[name]

    head = lax.axis_index("tp")
    tokens = ready("tokens")[...].astype(F32)
    rows = tokens.shape[0]
    normed = norm_rows(tokens, ready("mix")[...])
    contract_last = (((1,), (1,)), ((), ()))
    wi_ref, wf_ref = ready("wi"), ready("wf")
    bias, old_max = ready("bias")[...], ready("max")[...]
    heads = bias.shape[1]
    pick = iota((rows, heads), 1) == head
    gate_in = lax.dot_general(normed, wi_ref[...], contract_last, preferred_element_type=F32)
    gate_forget = lax.dot_general(normed, wf_ref[...], contract_last, preferred_element_type=F32)
    log_in = jnp.sum(jnp.where(pick, gate_in, 0.0), axis=1, keepdims=True)
    forget_pre = jnp.sum(jnp.where(pick, gate_forget + bias, 0.0), axis=1, keepdims=True)
    log_forget = jnp.minimum(forget_pre, 0.0) - jnp.log1p(jnp.exp(-jnp.abs(forget_pre)))
    eye = iota((rows, rows), 0) == iota((rows, rows), 1)
    carried = log_forget + column_of(old_max, eye)
    new_max = jnp.maximum(carried, log_in)
    keep = jnp.exp(carried - new_max)
    admit = jnp.exp(log_in - new_max)
    nmax_near[...] = row_of(new_max, eye)
    nmax_copy = pltpu.make_async_copy(nmax_near, nmax_ref, out_sems.at[0])
    nmax_copy.start()
    route, weight = ready("route")[...], ready("share")[...]
    plan(route, weight, chosen_ref, share_ref)
    for pick_ref in pick_refs:
        slots = slot_table(route, experts)
        pick_ref[...] = pick_matrix(slots, 0, pick_ref.shape[1], sources, part)
    query = rounded(normed, ready("wq")[...])
    scaled_key = rounded(normed, ready("wk")[...]) * query.shape[1] ** (-0.5)
    admitted = admit * scaled_key
    norm_state = keep * ready("norm")[...] + admitted
    nstate_near[...] = norm_state
    nstate_copy = pltpu.make_async_copy(nstate_near, nstate_ref, out_sems.at[1])
    nstate_copy.start()
    adk_ref[...] = admitted
    keep_ref[...] = jnp.broadcast_to(keep, keep_ref.shape)
    denom = jnp.sum(query * norm_state, axis=1, keepdims=True)
    overlap = jnp.sum(query * admitted, axis=1, keepdims=True)
    query_cols = jnp.transpose(query)
    mem = ready("mem")
    reads = [
        jnp.sum(query_cols[:, t : t + 1] * mem[t], axis=0, keepdims=True) for t in range(rows)
    ]
    value = rounded(normed, ready("wv")[...])
    value_ref[...] = value
    numer = keep * jnp.concatenate(reads, axis=0) + overlap * value
    read = numer / jnp.maximum(jnp.abs(denom), jnp.exp(-new_max))
    scale = lax.rsqrt(jnp.mean(read * read, axis=-1, keepdims=True) + EPS)
    ogate = rounded(normed, ready("wo")[...])
    gated = (jax.nn.sigmoid(ogate) * read * scale * ready("hgain")[...]).astype(BF16)
    partial = dot(gated, ready("wout")[...])
    span = own_ref.shape[1]
    low, high = partial[:, :span], partial[:, span:]
    first = head % 2 == 0
    residual = jnp.where(first, tokens[:, :span], tokens[:, span:]) * 0.5
    own_ref[...] = jnp.where(first, low, high) + residual
    send_ref[...] = jnp.where(first, high, low).astype(BF16)
    ready("fgain")
    nmax_copy.wait()
    nstate_copy.wait()


def pair_kernel(own_ref, got_ref, out_ref):
    total = (own_ref[...] + got_ref[...].astype(F32)).astype(BF16)
    for copy in range(out_ref.shape[0]):
        out_ref[copy] = total


def join_kernel(got_ref, out_ref):
    owners, chips, rows, span = got_ref.shape
    total = got_ref[:, 0].astype(F32)
    for chip in range(1, chips):
        total = total + got_ref[:, chip].astype(F32)
    out_ref[...] = total.astype(BF16).reshape(owners * rows, span)


def earlier_matrix(count):
    return (iota((count, count), 0) < iota((count, count), 1)).astype(BF16)


def plan(route, weight, chosen_ref, share_ref):
    count = route.shape[1]
    named = route == lax.axis_index("ep")
    share = jnp.where(named, weight, 0.0) / jnp.sum(weight, axis=0, keepdims=True)
    share = jnp.sum(share, axis=0, keepdims=True)
    member = jnp.sum(named.astype(F32), axis=0, keepdims=True)
    slot = dot(jnp.broadcast_to(member, (8, count)).astype(BF16), earlier_matrix(count))[0:1]
    shape = (EXPERT_CAPACITY, count)
    chosen = (iota(shape, 0).astype(F32) == slot) & (member > 0.5)
    chosen_ref[...] = chosen.astype(BF16)
    slot_share = jnp.sum(jnp.where(chosen, share, 0.0), axis=1, keepdims=True)
    share_ref[...] = jnp.broadcast_to(slot_share, share_ref.shape)


def slot_table(route, experts):
    count = route.shape[1]
    shape = (experts, count)
    member = jnp.zeros(shape, jnp.bool_)
    for choice in range(route.shape[0]):
        member = member | (iota(shape, 0) == route[choice : choice + 1])
    slots = dot(member.astype(BF16), earlier_matrix(count))
    return jnp.where(member, slots, -1.0).astype(BF16)


def pick_matrix(slots, start, size, sources, part):
    experts = slots.shape[0]
    column = iota((experts, size), 1) + start
    expand = (column // (sources * part) == iota((experts, size), 0)).astype(BF16)
    expanded = lax.dot_general(
        slots, expand, (((0,), (0,)), ((), ())), preferred_element_type=F32
    )
    column = iota((1, size), 1) + start
    source = (column // part) % sources
    slot = (source % (EXPERT_CAPACITY // part)) * part + column % part
    return (expanded == slot.astype(F32)).astype(BF16)


def expert_kernel(
    own_ref, got_ref, gain_ref, chosen_ref, share_ref, wg_ref, wu_ref, wd_ref,
    keep_ref, send_ref, *block_refs,
):
    expert, half = lax.axis_index("ep"), lax.axis_index("tp") % 2
    span = own_ref.shape[1]
    width = 2 * span
    for block_ref in block_refs:
        cols = block_ref.shape[1]
        start = expert * cols
        inner = pl.ds(pl.multiple_of(start % span, cols), cols)
        mine = start // span == half
        block_ref[...] = jnp.where(mine, own_ref[:, inner], got_ref[:, inner])
    gate = up = 0.0
    chosen = chosen_ref[...]
    sides = []
    for side, ref in ((half, own_ref), (1 - half, got_ref)):
        rows = dot(chosen, ref[...])
        sides.append((rows, pl.multiple_of(side * span, span)))
    square = sum(jnp.sum(rows * rows, axis=-1, keepdims=True) for rows, _ in sides)
    scale = lax.rsqrt(square / width + EPS)
    for rows, start in sides:
        normed = (rows * scale * gain_ref[:, pl.ds(start, span)]).astype(BF16)
        gate = gate + dot(normed, wg_ref[pl.ds(start, span), :])
        up = up + dot(normed, wu_ref[pl.ds(start, span), :])
    act = (jax.nn.silu(gate) * up).astype(BF16)
    result = (dot(act, wd_ref[...]) * share_ref[:, 0:1]).astype(BF16)
    part = keep_ref.shape[0]
    low, high = result[:part], result[part:]
    keep_ref[...] = jnp.where(half == 0, low, high)
    send_ref[...] = jnp.where(half == 0, high, low)


def spread_kernel(own_ref, got_ref, out_ref):
    total = (own_ref[...].astype(F32) + got_ref[...].astype(F32)).astype(BF16)
    owners, copies, _, cols = out_ref.shape
    for owner in range(owners):
        piece = total[:, owner * cols : (owner + 1) * cols]
        for copy in range(copies):
            out_ref[owner, copy] = piece


def mix_kernel(middle_ref, pick_ref, got_ref, out_ref):
    total = middle_ref[...].astype(F32) + dot(pick_ref[...], got_ref[...])
    out_ref[...] = total.astype(BF16)


def long_mix_kernel(middle_ref, route_ref, got_ref, out_ref, *, experts, sources, part):
    slots = slot_table(route_ref[...], experts)

    def add(step, total):
        start = step * CHUNK_ROWS
        pick = pick_matrix(slots, start, CHUNK_ROWS, sources, part)
        return total + dot(pick, got_ref[pl.ds(start, CHUNK_ROWS), :])

    steps = got_ref.shape[0] // CHUNK_ROWS
    total = lax.fori_loop(0, steps, add, middle_ref[...].astype(F32))
    out_ref[...] = total.astype(BF16)


def paired(values):
    heads = lax.axis_size("tp")
    return lax.ppermute(values, "tp", [(i, i ^ 1) for i in range(heads)])


def near(values):
    return pltpu.with_memory_space_constraint(values, pltpu.VMEM)


def far(values):
    return pltpu.with_memory_space_constraint(values, pltpu.HBM)


def call(kernel, out_shape, in_specs, name, out_specs=None, **kw):
    if out_specs is None:
        vmem = pl.BlockSpec(memory_space=pltpu.VMEM)
        out_specs = [vmem] * len(out_shape) if isinstance(out_shape, tuple) else vmem
    return pl.pallas_call(
        kernel,
        out_shape=out_shape,
        in_specs=in_specs,
        out_specs=out_specs,
        name=name,
        compiler_params=pltpu.CompilerParams(vmem_limit_bytes=VMEM_LIMIT),
        **kw,
    )


def shards(
    tokens, mix_gain, w_query, w_key, w_value, w_ogate, w_igate, w_fgate, forget_bias, head_gain,
    w_out, memory, normalizer, running_max, ffn_gain, route, route_weight, w_gate, w_up, w_down,
):
    vmem = pl.BlockSpec(memory_space=pltpu.VMEM)
    hbm = pl.BlockSpec(memory_space=pl.ANY)
    owners, heads = lax.axis_size("ep"), lax.axis_size("tp")
    chips = heads // 2
    rows, width = tokens.shape
    span = width // 2
    cols = width // owners
    count = route.shape[0]
    qk_dim, dv = w_query.shape[1], w_value.shape[1]
    part = EXPERT_CAPACITY // 2
    got_rows = owners * heads * part
    short = got_rows <= CHUNK_ROWS
    aligned = cols % LANES == 0
    sizes = dict(experts=owners, sources=heads, part=part)
    spec = jax.ShapeDtypeStruct
    memory_rows = memory.reshape(rows, qk_dim, dv)
    cell_inputs = dict(
        tokens=tokens,
        mix=mix_gain.reshape(1, -1),
        wi=w_igate.T,
        wf=w_fgate.T,
        bias=forget_bias.reshape(1, -1),
        max=running_max.T,
        route=route.T,
        share=route_weight.T,
        fgain=ffn_gain.reshape(1, -1),
        wq=w_query,
        wk=w_key,
        norm=normalizer.reshape(rows, qk_dim),
        mem=memory_rows,
        wv=w_value,
        wo=w_ogate,
        hgain=head_gain.reshape(1, -1),
        wout=w_out,
    )
    cell_inputs = [cell_inputs[name] for name in CELL_INPUTS]
    scratch = [(8, LANES) if name in ("mem", "fgain") else x.shape for name, x in zip(CELL_INPUTS, cell_inputs)]
    own, send, norm_state, new_max, keep, admitted, value, near_memory, gain, chosen, share, *pick = call(
        functools.partial(cell_kernel, **sizes),
        (
            pltpu.VMEM((rows, span), F32),
            pltpu.VMEM((rows, span), BF16),
            pltpu.HBM((rows, qk_dim), F32),
            pltpu.HBM((1, rows), F32),
            pltpu.VMEM((rows, LANES), F32),
            pltpu.VMEM((rows, qk_dim), F32),
            pltpu.VMEM((rows, dv), F32),
            pltpu.VMEM((rows, qk_dim, dv), F32),
            pltpu.VMEM((1, width), F32),
            pltpu.VMEM((EXPERT_CAPACITY, count), BF16),
            pltpu.VMEM((EXPERT_CAPACITY, LANES), F32),
        )
        + ((pltpu.VMEM((count, got_rows), BF16),) if short else ()),
        [hbm] * len(cell_inputs),
        "cell",
        out_specs=[vmem, vmem, hbm, hbm] + [vmem] * (8 if short else 7),
        scratch_shapes=[pltpu.VMEM(shape, x.dtype) for shape, x in zip(scratch, cell_inputs)]
        + [
            pltpu.VMEM((rows, qk_dim), F32),
            pltpu.VMEM((1, rows), F32),
            pltpu.SemaphoreType.DMA((len(cell_inputs),)),
            pltpu.SemaphoreType.DMA((2,)),
        ],
    )(*map(far, cell_inputs))

    chunks = call(pair_kernel, pltpu.VMEM((owners * chips, rows, span), BF16), [vmem] * 2, "pair")(
        near(own), near(paired(send))
    )
    same = [[e * heads + t for e in range(owners) for t in range(c, heads, 2)] for c in range(2)]
    chunks = lax.all_to_all(
        chunks, ("ep", "tp"), split_axis=0, concat_axis=0, tiled=True, axis_index_groups=same
    )
    own = call(join_kernel, pltpu.VMEM((count, span), BF16), [vmem], "join")(
        near(chunks.reshape(owners, chips, rows, span))
    )
    own, near_memory, keep, admitted, value = lax.optimization_barrier(
        (own, near_memory, keep, admitted, value)
    )
    got = paired(own)
    state = keep[:, 0:1, None] * near_memory + admitted[:, :, None] * value[:, None, :]
    got, state = lax.optimization_barrier((got, state))
    kept, send, *own_middle = call(
        expert_kernel,
        (pltpu.VMEM((part, width), BF16), pltpu.VMEM((part, width), BF16))
        + ((pltpu.VMEM((count, cols), BF16),) if aligned else ()),
        [vmem] * 8,
        "expert",
    )(
        near(own),
        near(got),
        near(gain),
        near(chosen),
        near(share),
        near(w_gate[0]),
        near(w_up[0]),
        near(w_down[0]),
    )
    handed = paired(send)
    if aligned:
        pieces = call(
            spread_kernel, pltpu.VMEM((owners, heads, part, cols), BF16), [vmem, vmem], "spread"
        )(near(kept), near(handed))
    else:
        first = lax.axis_index("tp") % 2 == 0
        middle = jnp.concatenate([jnp.where(first, own, got), jnp.where(first, got, own)], axis=1)
        start = lax.axis_index("ep") * cols
        own_middle = [lax.dynamic_slice_in_dim(middle, start, cols, axis=1)]
        total = (kept.astype(F32) + handed.astype(F32)).astype(BF16)
        total = total.reshape(part, owners, cols).transpose(1, 0, 2)
        pieces = jnp.broadcast_to(total[:, None], (owners, heads, part, cols))
    pieces = pieces.reshape(owners * heads, part, cols)
    results = lax.all_to_all(pieces, ("ep", "tp"), split_axis=0, concat_axis=0, tiled=True)
    results = near(results.reshape(got_rows, cols))
    if short:
        mixed = call(mix_kernel, spec((count, cols), BF16), [vmem] * 3, "mix")(
            near(own_middle[0]), near(pick[0]), results
        )
    else:
        mixed = call(
            functools.partial(long_mix_kernel, **sizes),
            spec((count, cols), BF16),
            [vmem] * 3,
            "mix",
        )(own_middle[0], route.T, results)
    return (
        mixed,
        state.reshape(memory.shape),
        norm_state.reshape(normalizer.shape),
        new_max.T,
    )


def solution(mesh):
    return jax.shard_map(
        shards,
        mesh=mesh,
        in_specs=(
            P("ep", None),
            P(),
            P(None, "tp"),
            P(None, "tp"),
            P(None, "tp"),
            P(None, "tp"),
            P(),
            P(),
            P(),
            P("tp"),
            P("tp", None),
            P("ep", "tp", None, None),
            P("ep", "tp", None),
            P("ep", "tp"),
            P(),
            P(),
            P(),
            P("ep", None, "tp"),
            P("ep", None, "tp"),
            P("ep", "tp", None),
        ),
        out_specs=(P(None, "ep"), P("ep", "tp", None, None), P("ep", "tp", None), P("ep", "tp")),
        check_vma=False,
    )
```

```python
import functools

import jax
import jax.numpy as jnp
from jax import lax
from jax.experimental import pallas as pl
from jax.experimental.pallas import tpu as pltpu
from jax.sharding import PartitionSpec as P

EXPERT_CAPACITY = 32
EPS = 1e-06
LANES = 128
CHUNK_ROWS = 512
VMEM_LIMIT = 32 << 20
CELL_INPUTS = (
    "tokens", "mix", "wi", "wf", "bias", "max", "wq", "wk", "norm", "mem", "wv", "wo", "hgain",
    "wout", "fgain", "route", "share",
)
CELL_PASSED = ("mem", "fgain", "route", "share")

F32 = jnp.float32
BF16 = jnp.bfloat16


def iota(shape, dim):
    return lax.broadcasted_iota(jnp.int32, shape, dim)


def dot(a, b):
    return jnp.dot(a, b, preferred_element_type=F32)


def rounded(a, b):
    return dot(a, b).astype(BF16).astype(F32)


def norm_rows(floats, gain):
    scale = lax.rsqrt(jnp.mean(floats * floats, axis=-1, keepdims=True) + EPS)
    return (floats * scale * gain).astype(BF16)


def column_of(row, eye):
    return jnp.sum(jnp.where(eye, row, 0.0), axis=1, keepdims=True)


def row_of(column, eye):
    return jnp.sum(jnp.where(eye, column, 0.0), axis=0, keepdims=True)


def cell_kernel(*refs):
    count = len(CELL_INPUTS)
    far_refs, outs, scratch = refs[:count], refs[count : -count - 4], refs[-count - 4 :]
    near_refs, (nstate_near, nmax_near), (sems, out_sems) = scratch[:count], scratch[count:-2], scratch[-2:]
    (
        own_ref, send_ref, nstate_ref, nmax_ref, keep_ref, adk_ref, value_ref, mem_ref, gain_ref,
        route_ref, share_ref,
    ) = outs
    direct = dict(zip(CELL_PASSED, (mem_ref, gain_ref, route_ref, share_ref)))
    copies, local = {}, {}
    for i, name in enumerate(CELL_INPUTS):
        local[name] = direct.get(name, near_refs[i])
        copies[name] = pltpu.make_async_copy(far_refs[i], local[name], sems.at[i])
        copies[name].start()

    def ready(name):
        copies[name].wait()
        return local[name]

    head = lax.axis_index("tp")
    tokens = ready("tokens")[...].astype(F32)
    rows = tokens.shape[0]
    normed = norm_rows(tokens, ready("mix")[...])
    contract_last = (((1,), (1,)), ((), ()))
    wi_ref, wf_ref = ready("wi"), ready("wf")
    bias, old_max = ready("bias")[...], ready("max")[...]
    heads = bias.shape[1]
    pick = iota((rows, heads), 1) == head
    gate_in = lax.dot_general(normed, wi_ref[...], contract_last, preferred_element_type=F32)
    gate_forget = lax.dot_general(normed, wf_ref[...], contract_last, preferred_element_type=F32)
    log_in = jnp.sum(jnp.where(pick, gate_in, 0.0), axis=1, keepdims=True)
    forget_pre = jnp.sum(jnp.where(pick, gate_forget + bias, 0.0), axis=1, keepdims=True)
    log_forget = jnp.minimum(forget_pre, 0.0) - jnp.log1p(jnp.exp(-jnp.abs(forget_pre)))
    eye = iota((rows, rows), 0) == iota((rows, rows), 1)
    carried = log_forget + column_of(old_max, eye)
    new_max = jnp.maximum(carried, log_in)
    keep = jnp.exp(carried - new_max)
    admit = jnp.exp(log_in - new_max)
    nmax_near[...] = row_of(new_max, eye)
    nmax_copy = pltpu.make_async_copy(nmax_near, nmax_ref, out_sems.at[0])
    nmax_copy.start()
    query = rounded(normed, ready("wq")[...])
    scaled_key = rounded(normed, ready("wk")[...]) * query.shape[1] ** (-0.5)
    admitted = admit * scaled_key
    norm_state = keep * ready("norm")[...] + admitted
    nstate_near[...] = norm_state
    nstate_copy = pltpu.make_async_copy(nstate_near, nstate_ref, out_sems.at[1])
    nstate_copy.start()
    adk_ref[...] = admitted
    keep_ref[...] = jnp.broadcast_to(keep, keep_ref.shape)
    denom = jnp.sum(query * norm_state, axis=1, keepdims=True)
    overlap = jnp.sum(query * admitted, axis=1, keepdims=True)
    query_cols = jnp.transpose(query)
    mem = ready("mem")
    reads = [
        jnp.sum(query_cols[:, t : t + 1] * mem[t], axis=0, keepdims=True) for t in range(rows)
    ]
    value = rounded(normed, ready("wv")[...])
    value_ref[...] = value
    numer = keep * jnp.concatenate(reads, axis=0) + overlap * value
    read = numer / jnp.maximum(jnp.abs(denom), jnp.exp(-new_max))
    scale = lax.rsqrt(jnp.mean(read * read, axis=-1, keepdims=True) + EPS)
    ogate = rounded(normed, ready("wo")[...])
    gated = (jax.nn.sigmoid(ogate) * read * scale * ready("hgain")[...]).astype(BF16)
    partial = dot(gated, ready("wout")[...])
    span = own_ref.shape[1]
    low, high = partial[:, :span], partial[:, span:]
    first = head % 2 == 0
    residual = jnp.where(first, tokens[:, :span], tokens[:, span:]) * 0.5
    own_ref[...] = jnp.where(first, low, high) + residual
    send_ref[...] = jnp.where(first, high, low).astype(BF16)
    for name in ("fgain", "route", "share"):
        ready(name)
    nmax_copy.wait()
    nstate_copy.wait()


def pair_kernel(own_ref, got_ref, out_ref):
    total = (own_ref[...] + got_ref[...].astype(F32)).astype(BF16)
    for copy in range(out_ref.shape[0]):
        out_ref[copy] = total


def join_kernel(got_ref, out_ref):
    owners, chips, rows, span = got_ref.shape
    total = got_ref[:, 0].astype(F32)
    for chip in range(1, chips):
        total = total + got_ref[:, chip].astype(F32)
    out_ref[...] = total.astype(BF16).reshape(owners * rows, span)


def earlier_matrix(count):
    return (iota((count, count), 0) < iota((count, count), 1)).astype(BF16)


def plan_kernel(
    route_ref, weight_ref, chosen_ref, share_ref, *pick_refs, experts, sources, part
):
    route, weight = route_ref[...], weight_ref[...]
    count = route.shape[1]
    named = route == lax.axis_index("ep")
    share = jnp.where(named, weight, 0.0) / jnp.sum(weight, axis=0, keepdims=True)
    share = jnp.sum(share, axis=0, keepdims=True)
    member = jnp.sum(named.astype(F32), axis=0, keepdims=True)
    slot = dot(jnp.broadcast_to(member, (8, count)).astype(BF16), earlier_matrix(count))[0:1]
    shape = (EXPERT_CAPACITY, count)
    chosen = (iota(shape, 0).astype(F32) == slot) & (member > 0.5)
    chosen_ref[...] = chosen.astype(BF16)
    slot_share = jnp.sum(jnp.where(chosen, share, 0.0), axis=1, keepdims=True)
    share_ref[...] = jnp.broadcast_to(slot_share, share_ref.shape)
    for pick_ref in pick_refs:
        slots = slot_table(route, experts)
        pick_ref[...] = pick_matrix(slots, 0, pick_ref.shape[1], sources, part)


def slot_table(route, experts):
    count = route.shape[1]
    shape = (experts, count)
    member = jnp.zeros(shape, jnp.bool_)
    for choice in range(route.shape[0]):
        member = member | (iota(shape, 0) == route[choice : choice + 1])
    slots = dot(member.astype(BF16), earlier_matrix(count))
    return jnp.where(member, slots, -1.0).astype(BF16)


def pick_matrix(slots, start, size, sources, part):
    experts = slots.shape[0]
    column = iota((experts, size), 1) + start
    expand = (column // (sources * part) == iota((experts, size), 0)).astype(BF16)
    expanded = lax.dot_general(
        slots, expand, (((0,), (0,)), ((), ())), preferred_element_type=F32
    )
    column = iota((1, size), 1) + start
    source = (column // part) % sources
    slot = (source % (EXPERT_CAPACITY // part)) * part + column % part
    return (expanded == slot.astype(F32)).astype(BF16)


def expert_kernel(
    own_ref, got_ref, gain_ref, chosen_ref, share_ref, wg_ref, wu_ref, wd_ref,
    keep_ref, send_ref, *block_refs,
):
    expert, half = lax.axis_index("ep"), lax.axis_index("tp") % 2
    span = own_ref.shape[1]
    width = 2 * span
    for block_ref in block_refs:
        cols = block_ref.shape[1]
        start = expert * cols
        inner = pl.ds(pl.multiple_of(start % span, cols), cols)
        mine = start // span == half
        block_ref[...] = jnp.where(mine, own_ref[:, inner], got_ref[:, inner])
    gate = up = 0.0
    chosen = chosen_ref[...]
    sides = []
    for side, ref in ((half, own_ref), (1 - half, got_ref)):
        rows = dot(chosen, ref[...])
        sides.append((rows, pl.multiple_of(side * span, span)))
    square = sum(jnp.sum(rows * rows, axis=-1, keepdims=True) for rows, _ in sides)
    scale = lax.rsqrt(square / width + EPS)
    for rows, start in sides:
        normed = (rows * scale * gain_ref[:, pl.ds(start, span)]).astype(BF16)
        gate = gate + dot(normed, wg_ref[pl.ds(start, span), :])
        up = up + dot(normed, wu_ref[pl.ds(start, span), :])
    act = (jax.nn.silu(gate) * up).astype(BF16)
    result = (dot(act, wd_ref[...]) * share_ref[:, 0:1]).astype(BF16)
    part = keep_ref.shape[0]
    low, high = result[:part], result[part:]
    keep_ref[...] = jnp.where(half == 0, low, high)
    send_ref[...] = jnp.where(half == 0, high, low)


def spread_kernel(own_ref, got_ref, out_ref):
    total = (own_ref[...].astype(F32) + got_ref[...].astype(F32)).astype(BF16)
    owners, copies, _, cols = out_ref.shape
    for owner in range(owners):
        piece = total[:, owner * cols : (owner + 1) * cols]
        for copy in range(copies):
            out_ref[owner, copy] = piece


def mix_kernel(middle_ref, pick_ref, got_ref, out_ref):
    total = middle_ref[...].astype(F32) + dot(pick_ref[...], got_ref[...])
    out_ref[...] = total.astype(BF16)


def long_mix_kernel(middle_ref, route_ref, got_ref, out_ref, *, experts, sources, part):
    slots = slot_table(route_ref[...], experts)

    def add(step, total):
        start = step * CHUNK_ROWS
        pick = pick_matrix(slots, start, CHUNK_ROWS, sources, part)
        return total + dot(pick, got_ref[pl.ds(start, CHUNK_ROWS), :])

    steps = got_ref.shape[0] // CHUNK_ROWS
    total = lax.fori_loop(0, steps, add, middle_ref[...].astype(F32))
    out_ref[...] = total.astype(BF16)


def paired(values):
    heads = lax.axis_size("tp")
    return lax.ppermute(values, "tp", [(i, i ^ 1) for i in range(heads)])


def near(values):
    return pltpu.with_memory_space_constraint(values, pltpu.VMEM)


def far(values):
    return pltpu.with_memory_space_constraint(values, pltpu.HBM)


def call(kernel, out_shape, in_specs, name, out_specs=None, **kw):
    if out_specs is None:
        vmem = pl.BlockSpec(memory_space=pltpu.VMEM)
        out_specs = [vmem] * len(out_shape) if isinstance(out_shape, tuple) else vmem
    return pl.pallas_call(
        kernel,
        out_shape=out_shape,
        in_specs=in_specs,
        out_specs=out_specs,
        name=name,
        compiler_params=pltpu.CompilerParams(vmem_limit_bytes=VMEM_LIMIT),
        **kw,
    )


def shards(
    tokens, mix_gain, w_query, w_key, w_value, w_ogate, w_igate, w_fgate, forget_bias, head_gain,
    w_out, memory, normalizer, running_max, ffn_gain, route, route_weight, w_gate, w_up, w_down,
):
    vmem = pl.BlockSpec(memory_space=pltpu.VMEM)
    hbm = pl.BlockSpec(memory_space=pl.ANY)
    owners, heads = lax.axis_size("ep"), lax.axis_size("tp")
    chips = heads // 2
    rows, width = tokens.shape
    span = width // 2
    cols = width // owners
    count = route.shape[0]
    qk_dim, dv = w_query.shape[1], w_value.shape[1]
    part = EXPERT_CAPACITY // 2
    got_rows = owners * heads * part
    short = got_rows <= CHUNK_ROWS
    aligned = cols % LANES == 0
    sizes = dict(experts=owners, sources=heads, part=part)
    spec = jax.ShapeDtypeStruct
    memory_rows = memory.reshape(rows, qk_dim, dv)
    cell_inputs = dict(
        tokens=tokens,
        mix=mix_gain.reshape(1, -1),
        wi=w_igate.T,
        wf=w_fgate.T,
        bias=forget_bias.reshape(1, -1),
        max=running_max.T,
        route=route.T,
        share=route_weight.T,
        fgain=ffn_gain.reshape(1, -1),
        wq=w_query,
        wk=w_key,
        norm=normalizer.reshape(rows, qk_dim),
        mem=memory_rows,
        wv=w_value,
        wo=w_ogate,
        hgain=head_gain.reshape(1, -1),
        wout=w_out,
    )
    cell_inputs = [cell_inputs[name] for name in CELL_INPUTS]
    scratch = [
        (8, LANES) if name in CELL_PASSED else x.shape for name, x in zip(CELL_INPUTS, cell_inputs)
    ]
    own, send, norm_state, new_max, *state_parts, gain, near_route, near_weight = call(
        cell_kernel,
        (
            pltpu.VMEM((rows, span), F32),
            pltpu.VMEM((rows, span), BF16),
            pltpu.HBM((rows, qk_dim), F32),
            pltpu.HBM((1, rows), F32),
            pltpu.VMEM((rows, dv), F32),
            pltpu.VMEM((rows, qk_dim), F32),
            pltpu.VMEM((rows, dv), F32),
            pltpu.VMEM((rows, qk_dim, dv), F32),
            pltpu.VMEM((1, width), F32),
            pltpu.VMEM((route.shape[1], count), jnp.int32),
            pltpu.VMEM((route.shape[1], count), F32),
        ),
        [hbm] * len(cell_inputs),
        "cell",
        out_specs=[vmem, vmem, hbm, hbm] + [vmem] * 7,
        scratch_shapes=[pltpu.VMEM(shape, x.dtype) for shape, x in zip(scratch, cell_inputs)]
        + [
            pltpu.VMEM((rows, qk_dim), F32),
            pltpu.VMEM((1, rows), F32),
            pltpu.SemaphoreType.DMA((len(cell_inputs),)),
            pltpu.SemaphoreType.DMA((2,)),
        ],
    )(*map(far, cell_inputs))

    chosen, share, *pick = call(
        functools.partial(plan_kernel, **sizes),
        (
            pltpu.VMEM((EXPERT_CAPACITY, count), BF16),
            pltpu.VMEM((EXPERT_CAPACITY, LANES), F32),
        )
        + ((pltpu.VMEM((count, got_rows), BF16),) if short else ()),
        [vmem] * 2,
        "plan",
        cost_estimate=pl.CostEstimate(flops=1 << 22, bytes_accessed=1 << 16, transcendentals=0),
    )(near(near_route), near(near_weight))
    got, chosen, share, pick = lax.optimization_barrier((paired(send), chosen, share, pick))
    chunks = call(pair_kernel, pltpu.VMEM((owners * chips, rows, span), BF16), [vmem] * 2, "pair")(
        near(own), near(got)
    )
    same = [[e * heads + t for e in range(owners) for t in range(c, heads, 2)] for c in range(2)]
    chunks = lax.all_to_all(
        chunks, ("ep", "tp"), split_axis=0, concat_axis=0, tiled=True, axis_index_groups=same
    )
    own = call(join_kernel, pltpu.VMEM((count, span), BF16), [vmem], "join")(
        near(chunks.reshape(owners, chips, rows, span))
    )
    got = paired(own)
    kept, send, *own_middle = call(
        expert_kernel,
        (pltpu.VMEM((part, width), BF16), pltpu.VMEM((part, width), BF16))
        + ((pltpu.VMEM((count, cols), BF16),) if aligned else ()),
        [vmem] * 8,
        "expert",
    )(
        near(own),
        near(got),
        near(gain),
        near(chosen),
        near(share),
        near(w_gate[0]),
        near(w_up[0]),
        near(w_down[0]),
    )
    send, state_parts = lax.optimization_barrier((send, state_parts))
    handed = paired(send)
    keep, admitted, value, near_memory = state_parts
    state = keep[:, None, :] * near_memory + admitted[:, :, None] * value[:, None, :]
    handed, state = lax.optimization_barrier((handed, state))
    if aligned:
        pieces = call(
            spread_kernel, pltpu.VMEM((owners, heads, part, cols), BF16), [vmem, vmem], "spread"
        )(near(kept), near(handed))
    else:
        first = lax.axis_index("tp") % 2 == 0
        middle = jnp.concatenate([jnp.where(first, own, got), jnp.where(first, got, own)], axis=1)
        start = lax.axis_index("ep") * cols
        own_middle = [lax.dynamic_slice_in_dim(middle, start, cols, axis=1)]
        total = (kept.astype(F32) + handed.astype(F32)).astype(BF16)
        total = total.reshape(part, owners, cols).transpose(1, 0, 2)
        pieces = jnp.broadcast_to(total[:, None], (owners, heads, part, cols))
    pieces = pieces.reshape(owners * heads, part, cols)
    results = lax.all_to_all(pieces, ("ep", "tp"), split_axis=0, concat_axis=0, tiled=True)
    results = near(results.reshape(got_rows, cols))
    if short:
        mixed = call(mix_kernel, spec((count, cols), BF16), [vmem] * 3, "mix")(
            near(own_middle[0]), near(pick[0]), results
        )
    else:
        mixed = call(
            functools.partial(long_mix_kernel, **sizes),
            spec((count, cols), BF16),
            [vmem] * 3,
            "mix",
        )(own_middle[0], route.T, results)
    return (
        mixed,
        state.reshape(memory.shape),
        norm_state.reshape(normalizer.shape),
        new_max.T,
    )


def solution(mesh):
    return jax.shard_map(
        shards,
        mesh=mesh,
        in_specs=(
            P("ep", None),
            P(),
            P(None, "tp"),
            P(None, "tp"),
            P(None, "tp"),
            P(None, "tp"),
            P(),
            P(),
            P(),
            P("tp"),
            P("tp", None),
            P("ep", "tp", None, None),
            P("ep", "tp", None),
            P("ep", "tp"),
            P(),
            P(),
            P(),
            P("ep", None, "tp"),
            P("ep", None, "tp"),
            P("ep", "tp", None),
        ),
        out_specs=(P(None, "ep"), P("ep", "tp", None, None), P("ep", "tp", None), P("ep", "tp")),
        check_vma=False,
    )
```

```python
import functools

import jax
import jax.numpy as jnp
from jax import lax
from jax.experimental import pallas as pl
from jax.experimental.pallas import tpu as pltpu
from jax.sharding import PartitionSpec as P

EXPERT_CAPACITY = 32
EPS = 1e-06
LANES = 128
CHUNK_ROWS = 512
VMEM_LIMIT = 32 << 20
CELL_INPUTS = (
    "tokens", "mix", "wq", "wi", "wf", "bias", "max", "wk", "norm", "mem", "hgain", "fgain", "route",
    "share", "wv", "wo", "wout",
)
CELL_PASSED = ("mem", "fgain", "route", "share")

F32 = jnp.float32
BF16 = jnp.bfloat16


def iota(shape, dim):
    return lax.broadcasted_iota(jnp.int32, shape, dim)


def dot(a, b):
    return jnp.dot(a, b, preferred_element_type=F32)


def rounded(a, b):
    return dot(a, b).astype(BF16).astype(F32)


def norm_rows(floats, gain):
    scale = lax.rsqrt(jnp.mean(floats * floats, axis=-1, keepdims=True) + EPS)
    return (floats * scale * gain).astype(BF16)


def column_of(row, eye):
    return jnp.sum(jnp.where(eye, row, 0.0), axis=1, keepdims=True)


def row_of(column, eye):
    return jnp.sum(jnp.where(eye, column, 0.0), axis=0, keepdims=True)


def cell_kernel(*refs):
    count = len(CELL_INPUTS)
    far_refs, outs, scratch = refs[:count], refs[count : -count - 4], refs[-count - 4 :]
    near_refs, (nstate_near, nmax_near), (sems, out_sems) = scratch[:count], scratch[count:-2], scratch[-2:]
    (
        own_ref, send_ref, nstate_ref, nmax_ref, keep_ref, adk_ref, value_ref, mem_ref, gain_ref,
        route_ref, share_ref,
    ) = outs
    direct = dict(zip(CELL_PASSED, (mem_ref, gain_ref, route_ref, share_ref)))
    copies, local = {}, {}
    for i, name in enumerate(CELL_INPUTS):
        local[name] = direct.get(name, near_refs[i])
        copies[name] = pltpu.make_async_copy(far_refs[i], local[name], sems.at[i])
        copies[name].start()

    def ready(*names):
        for name in names:
            copies[name].wait()
        return local[names[-1]]

    head = lax.axis_index("tp")
    tokens = ready("tokens")[...].astype(F32)
    rows = tokens.shape[0]
    normed = norm_rows(tokens, ready("mix")[...])
    contract_last = (((1,), (1,)), ((), ()))
    wi_ref, wf_ref = ready("wi"), ready("wf")
    bias, old_max = ready("bias")[...], ready("max")[...]
    heads = bias.shape[1]
    pick = iota((rows, heads), 1) == head
    gate_in = lax.dot_general(normed, wi_ref[...], contract_last, preferred_element_type=F32)
    gate_forget = lax.dot_general(normed, wf_ref[...], contract_last, preferred_element_type=F32)
    log_in = jnp.sum(jnp.where(pick, gate_in, 0.0), axis=1, keepdims=True)
    forget_pre = jnp.sum(jnp.where(pick, gate_forget + bias, 0.0), axis=1, keepdims=True)
    log_forget = jnp.minimum(forget_pre, 0.0) - jnp.log1p(jnp.exp(-jnp.abs(forget_pre)))
    eye = iota((rows, rows), 0) == iota((rows, rows), 1)
    carried = log_forget + column_of(old_max, eye)
    new_max = jnp.maximum(carried, log_in)
    keep = jnp.exp(carried - new_max)
    admit = jnp.exp(log_in - new_max)
    nmax_near[...] = row_of(new_max, eye)
    nmax_copy = pltpu.make_async_copy(nmax_near, nmax_ref, out_sems.at[0])
    nmax_copy.start()
    ready("norm", "hgain", "fgain", "route", "share", "wq", "wk")
    query = rounded(normed, local["wq"][...])
    scaled_key = rounded(normed, local["wk"][...]) * query.shape[1] ** (-0.5)
    admitted = admit * scaled_key
    norm_state = keep * local["norm"][...] + admitted
    nstate_near[...] = norm_state
    nstate_copy = pltpu.make_async_copy(nstate_near, nstate_ref, out_sems.at[1])
    nstate_copy.start()
    adk_ref[...] = admitted
    keep_ref[...] = jnp.broadcast_to(keep, keep_ref.shape)
    denom = jnp.sum(query * norm_state, axis=1, keepdims=True)
    overlap = jnp.sum(query * admitted, axis=1, keepdims=True)
    query_cols = jnp.transpose(query)
    mem = ready("mem")
    reads = [
        jnp.sum(query_cols[:, t : t + 1] * mem[t], axis=0, keepdims=True) for t in range(rows)
    ]
    ready("wv", "wo")
    value = rounded(normed, local["wv"][...])
    ogate = rounded(normed, local["wo"][...])
    value_ref[...] = value
    numer = keep * jnp.concatenate(reads, axis=0) + overlap * value
    read = numer / jnp.maximum(jnp.abs(denom), jnp.exp(-new_max))
    scale = lax.rsqrt(jnp.mean(read * read, axis=-1, keepdims=True) + EPS)
    gated = (jax.nn.sigmoid(ogate) * read * scale * local["hgain"][...]).astype(BF16)
    partial = dot(gated, ready("wout")[...])
    span = own_ref.shape[1]
    low, high = partial[:, :span], partial[:, span:]
    first = head % 2 == 0
    residual = jnp.where(first, tokens[:, :span], tokens[:, span:]) * 0.5
    own_ref[...] = jnp.where(first, low, high) + residual
    send_ref[...] = jnp.where(first, high, low).astype(BF16)
    nmax_copy.wait()
    nstate_copy.wait()


def state_kernel(keep_ref, adk_ref, value_ref, mem_ref, out_ref, made, sems):
    adk_cols = jnp.transpose(adk_ref[...])
    copies = []
    for t in range(mem_ref.shape[0]):
        old = keep_ref[t : t + 1, :] * mem_ref[t]
        made[t] = old + adk_cols[:, t : t + 1] * value_ref[t : t + 1, :]
        copies.append(pltpu.make_async_copy(made.at[t], out_ref.at[t], sems.at[t]))
        copies[-1].start()
    for copy in copies:
        copy.wait()


def pair_kernel(own_ref, got_ref, out_ref):
    total = (own_ref[...] + got_ref[...].astype(F32)).astype(BF16)
    places, cores, _, span = out_ref.shape
    for core in range(cores):
        piece = total[:, core * span : (core + 1) * span]
        for place in range(places):
            out_ref[place, core] = piece


def join_kernel(got_ref, out_ref):
    owners, chips, cores, rows, span = got_ref.shape
    for core in range(cores):
        total = got_ref[:, 0, core].astype(F32)
        for chip in range(1, chips):
            total = total + got_ref[:, chip, core].astype(F32)
        total = total.astype(BF16).reshape(owners * rows, span)
        out_ref[:, core * span : (core + 1) * span] = total


def earlier_matrix(count):
    return (iota((count, count), 0) < iota((count, count), 1)).astype(BF16)


def plan_kernel(
    route_ref, weight_ref, chosen_ref, share_ref, *pick_refs, experts, sources, part
):
    route, weight = route_ref[...], weight_ref[...]
    count = route.shape[1]
    named = route == lax.axis_index("ep")
    share = jnp.where(named, weight, 0.0) / jnp.sum(weight, axis=0, keepdims=True)
    share = jnp.sum(share, axis=0, keepdims=True)
    member = jnp.sum(named.astype(F32), axis=0, keepdims=True)
    slot = dot(jnp.broadcast_to(member, (8, count)).astype(BF16), earlier_matrix(count))[0:1]
    shape = (EXPERT_CAPACITY, count)
    chosen = (iota(shape, 0).astype(F32) == slot) & (member > 0.5)
    chosen_ref[...] = chosen.astype(BF16)
    slot_share = jnp.sum(jnp.where(chosen, share, 0.0), axis=1, keepdims=True)
    share_ref[...] = jnp.broadcast_to(slot_share, share_ref.shape)
    for pick_ref in pick_refs:
        slots = slot_table(route, experts)
        pick_ref[...] = pick_matrix(slots, 0, pick_ref.shape[1], sources, part)


def slot_table(route, experts):
    count = route.shape[1]
    shape = (experts, count)
    member = jnp.zeros(shape, jnp.bool_)
    for choice in range(route.shape[0]):
        member = member | (iota(shape, 0) == route[choice : choice + 1])
    slots = dot(member.astype(BF16), earlier_matrix(count))
    return jnp.where(member, slots, -1.0).astype(BF16)


def pick_matrix(slots, start, size, sources, part):
    experts = slots.shape[0]
    column = iota((experts, size), 1) + start
    expand = (column // (sources * part) == iota((experts, size), 0)).astype(BF16)
    expanded = lax.dot_general(
        slots, expand, (((0,), (0,)), ((), ())), preferred_element_type=F32
    )
    column = iota((1, size), 1) + start
    source = (column // part) % sources
    slot = (source % (EXPERT_CAPACITY // part)) * part + column % part
    return (expanded == slot.astype(F32)).astype(BF16)


def expert_kernel(
    own_ref, got_ref, gain_ref, chosen_ref, share_ref, wg_ref, wu_ref, wd_ref,
    keep_ref, send_ref, *block_refs,
):
    expert, half = lax.axis_index("ep"), lax.axis_index("tp") % 2
    span = own_ref.shape[1]
    width = 2 * span
    quarter = span // 2
    for block_ref in block_refs:
        cols = block_ref.shape[1]
        start = expert * cols
        inner = pl.ds(pl.multiple_of(start // span * quarter + start % quarter, cols), cols)
        mine = start % span // quarter == half
        block_ref[...] = jnp.where(mine, own_ref[:, inner], got_ref[:, inner])
    gate = up = 0.0
    chosen = chosen_ref[...]
    pieces = []
    for side, ref in ((half, own_ref), (1 - half, got_ref)):
        rows = dot(chosen, ref[...])
        for core in range(2):
            piece = rows[:, core * quarter : (core + 1) * quarter]
            pieces.append((piece, pl.multiple_of(core * span + side * quarter, quarter)))
    square = sum(jnp.sum(piece * piece, axis=-1, keepdims=True) for piece, _ in pieces)
    scale = lax.rsqrt(square / width + EPS)
    for piece, start in pieces:
        normed = (piece * scale * gain_ref[:, pl.ds(start, quarter)]).astype(BF16)
        gate = gate + dot(normed, wg_ref[pl.ds(start, quarter), :])
        up = up + dot(normed, wu_ref[pl.ds(start, quarter), :])
    act = (jax.nn.silu(gate) * up).astype(BF16)
    result = (dot(act, wd_ref[...]) * share_ref[:, 0:1]).astype(BF16)
    part = keep_ref.shape[0]
    low, high = result[:part], result[part:]
    keep_ref[...] = jnp.where(half == 0, low, high)
    send_ref[...] = jnp.where(half == 0, high, low)


def spread_kernel(own_ref, got_ref, out_ref):
    total = (own_ref[...].astype(F32) + got_ref[...].astype(F32)).astype(BF16)
    owners, copies, _, cols = out_ref.shape
    for owner in range(owners):
        piece = total[:, owner * cols : (owner + 1) * cols]
        for copy in range(copies):
            out_ref[owner, copy] = piece


def mix_kernel(middle_ref, pick_ref, got_ref, out_ref):
    total = middle_ref[...].astype(F32) + dot(pick_ref[...], got_ref[...])
    out_ref[...] = total.astype(BF16)


def long_mix_kernel(middle_ref, route_ref, got_ref, out_ref, *, experts, sources, part):
    slots = slot_table(route_ref[...], experts)

    def add(step, total):
        start = step * CHUNK_ROWS
        pick = pick_matrix(slots, start, CHUNK_ROWS, sources, part)
        return total + dot(pick, got_ref[pl.ds(start, CHUNK_ROWS), :])

    steps = got_ref.shape[0] // CHUNK_ROWS
    total = lax.fori_loop(0, steps, add, middle_ref[...].astype(F32))
    out_ref[...] = total.astype(BF16)


def paired(values):
    heads = lax.axis_size("tp")
    return lax.ppermute(values, "tp", [(i, i ^ 1) for i in range(heads)])


def near(values):
    return pltpu.with_memory_space_constraint(values, pltpu.VMEM)


def far(values):
    return pltpu.with_memory_space_constraint(values, pltpu.HBM)


def call(kernel, out_shape, in_specs, name, out_specs=None, **kw):
    if out_specs is None:
        vmem = pl.BlockSpec(memory_space=pltpu.VMEM)
        out_specs = [vmem] * len(out_shape) if isinstance(out_shape, tuple) else vmem
    return pl.pallas_call(
        kernel,
        out_shape=out_shape,
        in_specs=in_specs,
        out_specs=out_specs,
        name=name,
        compiler_params=pltpu.CompilerParams(vmem_limit_bytes=VMEM_LIMIT),
        **kw,
    )


def shards(
    tokens, mix_gain, w_query, w_key, w_value, w_ogate, w_igate, w_fgate, forget_bias, head_gain,
    w_out, memory, normalizer, running_max, ffn_gain, route, route_weight, w_gate, w_up, w_down,
):
    vmem = pl.BlockSpec(memory_space=pltpu.VMEM)
    hbm = pl.BlockSpec(memory_space=pl.ANY)
    owners, heads = lax.axis_size("ep"), lax.axis_size("tp")
    chips = heads // 2
    rows, width = tokens.shape
    span = width // 2
    cols = width // owners
    count = route.shape[0]
    qk_dim, dv = w_query.shape[1], w_value.shape[1]
    part = EXPERT_CAPACITY // 2
    got_rows = owners * heads * part
    short = got_rows <= CHUNK_ROWS
    aligned = cols % LANES == 0
    sizes = dict(experts=owners, sources=heads, part=part)
    spec = jax.ShapeDtypeStruct
    memory_rows = memory.reshape(rows, qk_dim, dv)
    cell_inputs = dict(
        tokens=tokens,
        mix=mix_gain.reshape(1, -1),
        wi=w_igate.T,
        wf=w_fgate.T,
        bias=forget_bias.reshape(1, -1),
        max=running_max.T,
        route=route.T,
        share=route_weight.T,
        fgain=ffn_gain.reshape(1, -1),
        wq=w_query,
        wk=w_key,
        norm=normalizer.reshape(rows, qk_dim),
        mem=memory_rows,
        wv=w_value,
        wo=w_ogate,
        hgain=head_gain.reshape(1, -1),
        wout=w_out,
    )
    cell_inputs = [cell_inputs[name] for name in CELL_INPUTS]
    scratch = [
        (8, LANES) if name in CELL_PASSED else x.shape for name, x in zip(CELL_INPUTS, cell_inputs)
    ]
    own, send, norm_state, new_max, *state_parts, gain, near_route, near_weight = call(
        cell_kernel,
        (
            pltpu.VMEM((rows, span), F32),
            pltpu.VMEM((rows, span), BF16),
            pltpu.HBM((rows, qk_dim), F32),
            pltpu.HBM((1, rows), F32),
            pltpu.VMEM((rows, dv), F32),
            pltpu.VMEM((rows, qk_dim), F32),
            pltpu.VMEM((rows, dv), F32),
            pltpu.VMEM((rows, qk_dim, dv), F32),
            pltpu.VMEM((1, width), F32),
            pltpu.VMEM((route.shape[1], count), jnp.int32),
            pltpu.VMEM((route.shape[1], count), F32),
        ),
        [hbm] * len(cell_inputs),
        "cell",
        out_specs=[vmem, vmem, hbm, hbm] + [vmem] * 7,
        scratch_shapes=[pltpu.VMEM(shape, x.dtype) for shape, x in zip(scratch, cell_inputs)]
        + [
            pltpu.VMEM((rows, qk_dim), F32),
            pltpu.VMEM((1, rows), F32),
            pltpu.SemaphoreType.DMA((len(cell_inputs),)),
            pltpu.SemaphoreType.DMA((2,)),
        ],
    )(*map(far, cell_inputs))

    chosen, share, *pick = call(
        functools.partial(plan_kernel, **sizes),
        (
            pltpu.VMEM((EXPERT_CAPACITY, count), BF16),
            pltpu.VMEM((EXPERT_CAPACITY, LANES), F32),
        )
        + ((pltpu.VMEM((count, got_rows), BF16),) if short else ()),
        [vmem] * 2,
        "plan",
        cost_estimate=pl.CostEstimate(flops=1 << 22, bytes_accessed=1 << 16, transcendentals=0),
    )(near(near_route), near(near_weight))
    got, chosen, share, pick = lax.optimization_barrier((paired(send), chosen, share, pick))
    chunks = call(
        pair_kernel, pltpu.VMEM((owners * chips, 2, rows, span // 2), BF16), [vmem] * 2, "pair"
    )(near(own), near(got))
    chunks = chunks.reshape(owners * heads, rows, span // 2)
    chunks = lax.all_to_all(chunks, ("ep", "tp"), split_axis=0, concat_axis=0, tiled=True)
    own = call(join_kernel, pltpu.VMEM((count, span), BF16), [vmem], "join")(
        near(chunks.reshape(owners, chips, 2, rows, span // 2))
    )
    got = paired(own)
    kept, send, *own_middle = call(
        expert_kernel,
        (pltpu.VMEM((part, width), BF16), pltpu.VMEM((part, width), BF16))
        + ((pltpu.VMEM((count, cols), BF16),) if aligned else ()),
        [vmem] * 8,
        "expert",
    )(
        near(own),
        near(got),
        near(gain),
        near(chosen),
        near(share),
        near(w_gate[0]),
        near(w_up[0]),
        near(w_down[0]),
    )
    send, state_parts = lax.optimization_barrier((send, state_parts))
    handed = paired(send)
    state = call(
        state_kernel,
        pltpu.HBM((rows, qk_dim, dv), F32),
        [vmem] * 4,
        "state",
        out_specs=hbm,
        scratch_shapes=[pltpu.VMEM((rows, qk_dim, dv), F32), pltpu.SemaphoreType.DMA((rows,))],
        cost_estimate=pl.CostEstimate(flops=1 << 20, bytes_accessed=1 << 21, transcendentals=0),
    )(*map(near, state_parts))
    handed, state = lax.optimization_barrier((handed, state))
    if aligned:
        pieces = call(
            spread_kernel, pltpu.VMEM((owners, heads, part, cols), BF16), [vmem, vmem], "spread"
        )(near(kept), near(handed))
    else:
        first = lax.axis_index("tp") % 2 == 0
        sides = jnp.stack([jnp.where(first, own, got), jnp.where(first, got, own)], axis=1)
        middle = sides.reshape(count, 2, 2, span // 2).swapaxes(1, 2).reshape(count, width)
        start = lax.axis_index("ep") * cols
        own_middle = [lax.dynamic_slice_in_dim(middle, start, cols, axis=1)]
        total = (kept.astype(F32) + handed.astype(F32)).astype(BF16)
        total = total.reshape(part, owners, cols).transpose(1, 0, 2)
        pieces = jnp.broadcast_to(total[:, None], (owners, heads, part, cols))
    pieces = pieces.reshape(owners * heads, part, cols)
    results = lax.all_to_all(pieces, ("ep", "tp"), split_axis=0, concat_axis=0, tiled=True)
    results = near(results.reshape(got_rows, cols))
    if short:
        mixed = call(mix_kernel, spec((count, cols), BF16), [vmem] * 3, "mix")(
            near(own_middle[0]), near(pick[0]), results
        )
    else:
        mixed = call(
            functools.partial(long_mix_kernel, **sizes),
            spec((count, cols), BF16),
            [vmem] * 3,
            "mix",
        )(own_middle[0], route.T, results)
    return (
        mixed,
        state.reshape(memory.shape),
        norm_state.reshape(normalizer.shape),
        new_max.T,
    )


def solution(mesh):
    return jax.shard_map(
        shards,
        mesh=mesh,
        in_specs=(
            P("ep", None),
            P(),
            P(None, "tp"),
            P(None, "tp"),
            P(None, "tp"),
            P(None, "tp"),
            P(),
            P(),
            P(),
            P("tp"),
            P("tp", None),
            P("ep", "tp", None, None),
            P("ep", "tp", None),
            P("ep", "tp"),
            P(),
            P(),
            P(),
            P("ep", None, "tp"),
            P("ep", None, "tp"),
            P("ep", "tp", None),
        ),
        out_specs=(P(None, "ep"), P("ep", "tp", None, None), P("ep", "tp", None), P("ep", "tp")),
        check_vma=False,
    )
```

```python
import functools

import jax
import jax.numpy as jnp
from jax import lax
from jax.experimental import pallas as pl
from jax.experimental.pallas import tpu as pltpu
from jax.sharding import PartitionSpec as P

EXPERT_CAPACITY = 32
EPS = 1e-06
LANES = 128
CHUNK_ROWS = 512
VMEM_LIMIT = 32 << 20
CELL_INPUTS = (
    "tokens", "mix", "wq", "wi", "wf", "bias", "max", "wk", "norm", "mem", "hgain", "fgain", "route",
    "share", "wv", "wo", "wout",
)
CELL_PASSED = ("mem", "fgain", "route", "share")

F32 = jnp.float32
BF16 = jnp.bfloat16


def ranked(count):
    return [i // 2 if i % 2 == 0 else count - 1 - i // 2 for i in range(count)]


def ranked_at(index, count):
    return jnp.where(index % 2 == 0, index // 2, count - 1 - index // 2)


def iota(shape, dim):
    return lax.broadcasted_iota(jnp.int32, shape, dim)


def dot(a, b):
    return jnp.dot(a, b, preferred_element_type=F32)


def rounded(a, b):
    return dot(a, b).astype(BF16).astype(F32)


def norm_rows(floats, gain):
    scale = lax.rsqrt(jnp.mean(floats * floats, axis=-1, keepdims=True) + EPS)
    return (floats * scale * gain).astype(BF16)


def column_of(row, eye):
    return jnp.sum(jnp.where(eye, row, 0.0), axis=1, keepdims=True)


def row_of(column, eye):
    return jnp.sum(jnp.where(eye, column, 0.0), axis=0, keepdims=True)


def cell_kernel(*refs):
    count = len(CELL_INPUTS)
    far_refs, outs, scratch = refs[:count], refs[count : -count - 4], refs[-count - 4 :]
    near_refs, (nstate_near, nmax_near), (sems, out_sems) = scratch[:count], scratch[count:-2], scratch[-2:]
    (
        own_ref, send_ref, nstate_ref, nmax_ref, keep_ref, adk_ref, value_ref, mem_ref, gain_ref,
        route_ref, share_ref,
    ) = outs
    direct = dict(zip(CELL_PASSED, (mem_ref, gain_ref, route_ref, share_ref)))
    copies, local = {}, {}
    for i, name in enumerate(CELL_INPUTS):
        local[name] = direct.get(name, near_refs[i])
        copies[name] = pltpu.make_async_copy(far_refs[i], local[name], sems.at[i])
        copies[name].start()

    def ready(*names):
        for name in names:
            copies[name].wait()
        return local[names[-1]]

    head = lax.axis_index("tp")
    tokens = ready("tokens")[...].astype(F32)
    rows = tokens.shape[0]
    normed = norm_rows(tokens, ready("mix")[...])
    contract_last = (((1,), (1,)), ((), ()))
    wi_ref, wf_ref = ready("wi"), ready("wf")
    bias, old_max = ready("bias")[...], ready("max")[...]
    heads = bias.shape[1]
    pick = iota((rows, heads), 1) == head
    gate_in = lax.dot_general(normed, wi_ref[...], contract_last, preferred_element_type=F32)
    gate_forget = lax.dot_general(normed, wf_ref[...], contract_last, preferred_element_type=F32)
    log_in = jnp.sum(jnp.where(pick, gate_in, 0.0), axis=1, keepdims=True)
    forget_pre = jnp.sum(jnp.where(pick, gate_forget + bias, 0.0), axis=1, keepdims=True)
    log_forget = jnp.minimum(forget_pre, 0.0) - jnp.log1p(jnp.exp(-jnp.abs(forget_pre)))
    eye = iota((rows, rows), 0) == iota((rows, rows), 1)
    carried = log_forget + column_of(old_max, eye)
    new_max = jnp.maximum(carried, log_in)
    keep = jnp.exp(carried - new_max)
    admit = jnp.exp(log_in - new_max)
    nmax_near[...] = row_of(new_max, eye)
    nmax_copy = pltpu.make_async_copy(nmax_near, nmax_ref, out_sems.at[0])
    nmax_copy.start()
    ready("norm", "hgain", "fgain", "route", "share", "wq", "wk")
    query = rounded(normed, local["wq"][...])
    scaled_key = rounded(normed, local["wk"][...]) * query.shape[1] ** (-0.5)
    admitted = admit * scaled_key
    norm_state = keep * local["norm"][...] + admitted
    nstate_near[...] = norm_state
    nstate_copy = pltpu.make_async_copy(nstate_near, nstate_ref, out_sems.at[1])
    nstate_copy.start()
    adk_ref[...] = admitted
    keep_ref[...] = jnp.broadcast_to(keep, keep_ref.shape)
    denom = jnp.sum(query * norm_state, axis=1, keepdims=True)
    overlap = jnp.sum(query * admitted, axis=1, keepdims=True)
    query_cols = jnp.transpose(query)
    mem = ready("mem")
    reads = [
        jnp.sum(query_cols[:, t : t + 1] * mem[t], axis=0, keepdims=True) for t in range(rows)
    ]
    ready("wv", "wo")
    value = rounded(normed, local["wv"][...])
    ogate = rounded(normed, local["wo"][...])
    value_ref[...] = value
    numer = keep * jnp.concatenate(reads, axis=0) + overlap * value
    read = numer / jnp.maximum(jnp.abs(denom), jnp.exp(-new_max))
    scale = lax.rsqrt(jnp.mean(read * read, axis=-1, keepdims=True) + EPS)
    gated = (jax.nn.sigmoid(ogate) * read * scale * local["hgain"][...]).astype(BF16)
    partial = dot(gated, ready("wout")[...])
    span = own_ref.shape[1]
    low, high = partial[:, :span], partial[:, span:]
    first = head % 2 == 0
    residual = jnp.where(first, tokens[:, :span], tokens[:, span:]) * 0.5
    own_ref[...] = jnp.where(first, low, high) + residual
    send_ref[...] = jnp.where(first, high, low).astype(BF16)
    nmax_copy.wait()
    nstate_copy.wait()


def state_kernel(keep_ref, adk_ref, value_ref, mem_ref, _, *refs, first, last):
    *_, out_ref, made, sems = refs
    adk_cols = jnp.transpose(adk_ref[...])
    copies = []
    for t in range(first, last):
        old = keep_ref[t : t + 1, :] * mem_ref[t]
        i = t - first
        made[i] = old + adk_cols[:, t : t + 1] * value_ref[t : t + 1, :]
        copies.append(pltpu.make_async_copy(made.at[i], out_ref.at[t], sems.at[i]))
        copies[-1].start()
    for copy in copies:
        copy.wait()


def pair_kernel(own_ref, got_ref, out_ref):
    total = (own_ref[...] + got_ref[...].astype(F32)).astype(BF16)
    devices, _, span = out_ref.shape
    for rank, device in enumerate(ranked(devices)):
        core = device % 2
        out_ref[rank] = total[:, core * span : (core + 1) * span]


def join_kernel(got_ref, *refs, heads):
    out_ref = refs[-1]
    devices, rows, span = got_ref.shape
    rank_of = {device: rank for rank, device in enumerate(ranked(devices))}
    for owner in range(devices // heads):
        for core in range(2):
            total = 0.0
            for chip in range(heads // 2):
                total = total + got_ref[rank_of[owner * heads + 2 * chip + core]].astype(F32)
            place = slice(owner * rows, (owner + 1) * rows), slice(core * span, (core + 1) * span)
            out_ref[place] = total.astype(BF16)


def earlier_matrix(count):
    return (iota((count, count), 0) < iota((count, count), 1)).astype(BF16)


def plan_kernel(
    route_ref, weight_ref, chosen_ref, share_ref, *pick_refs, experts, sources, part
):
    route, weight = route_ref[...], weight_ref[...]
    count = route.shape[1]
    named = route == lax.axis_index("ep")
    share = jnp.where(named, weight, 0.0) / jnp.sum(weight, axis=0, keepdims=True)
    share = jnp.sum(share, axis=0, keepdims=True)
    member = jnp.sum(named.astype(F32), axis=0, keepdims=True)
    slot = dot(jnp.broadcast_to(member, (8, count)).astype(BF16), earlier_matrix(count))[0:1]
    shape = (EXPERT_CAPACITY, count)
    chosen = (iota(shape, 0).astype(F32) == slot) & (member > 0.5)
    chosen_ref[...] = chosen.astype(BF16)
    slot_share = jnp.sum(jnp.where(chosen, share, 0.0), axis=1, keepdims=True)
    share_ref[...] = jnp.broadcast_to(slot_share, share_ref.shape)
    for pick_ref in pick_refs:
        slots = slot_table(route, experts)
        pick_ref[...] = pick_matrix(slots, 0, pick_ref.shape[1], sources, part)


def slot_table(route, experts):
    count = route.shape[1]
    shape = (experts, count)
    member = jnp.zeros(shape, jnp.bool_)
    for choice in range(route.shape[0]):
        member = member | (iota(shape, 0) == route[choice : choice + 1])
    slots = dot(member.astype(BF16), earlier_matrix(count))
    return jnp.where(member, slots, -1.0).astype(BF16)


def pick_matrix(slots, start, size, sources, part):
    experts = slots.shape[0]

    def device(shape):
        return ranked_at((iota(shape, len(shape) - 1) + start) // part, experts * sources)

    shape = (experts, size)
    expand = (device(shape) // sources == iota(shape, 0)).astype(BF16)
    expanded = lax.dot_general(
        slots, expand, (((0,), (0,)), ((), ())), preferred_element_type=F32
    )
    column = iota((1, size), 1) + start
    groups = EXPERT_CAPACITY // part
    slot = (device((1, size)) % sources % groups) * part + column % part
    return (expanded == slot.astype(F32)).astype(BF16)


def expert_kernel(
    own_ref, got_ref, gain_ref, chosen_ref, share_ref, wg_ref, wu_ref, wd_ref, _,
    keep_ref, send_ref, *block_refs,
):
    expert, half = lax.axis_index("ep"), lax.axis_index("tp") % 2
    span = own_ref.shape[1]
    width = 2 * span
    quarter = span // 2
    for block_ref in block_refs:
        cols = block_ref.shape[1]
        start = expert * cols
        inner = pl.ds(pl.multiple_of(start // span * quarter + start % quarter, cols), cols)
        mine = start % span // quarter == half
        block_ref[...] = jnp.where(mine, own_ref[:, inner], got_ref[:, inner])
    gate = up = 0.0
    chosen = chosen_ref[...]
    pieces = []
    for side, ref in ((half, own_ref), (1 - half, got_ref)):
        rows = dot(chosen, ref[...])
        for core in range(2):
            piece = rows[:, core * quarter : (core + 1) * quarter]
            pieces.append((piece, pl.multiple_of(core * span + side * quarter, quarter)))
    square = sum(jnp.sum(piece * piece, axis=-1, keepdims=True) for piece, _ in pieces)
    scale = lax.rsqrt(square / width + EPS)
    for piece, start in pieces:
        normed = (piece * scale * gain_ref[:, pl.ds(start, quarter)]).astype(BF16)
        gate = gate + dot(normed, wg_ref[pl.ds(start, quarter), :])
        up = up + dot(normed, wu_ref[pl.ds(start, quarter), :])
    act = (jax.nn.silu(gate) * up).astype(BF16)
    result = (dot(act, wd_ref[...]) * share_ref[:, 0:1]).astype(BF16)
    part = keep_ref.shape[0]
    low, high = result[:part], result[part:]
    keep_ref[...] = jnp.where(half == 0, low, high)
    send_ref[...] = jnp.where(half == 0, high, low)


def spread_kernel(own_ref, got_ref, _, out_ref, *, heads):
    total = (own_ref[...].astype(F32) + got_ref[...].astype(F32)).astype(BF16)
    devices, _, cols = out_ref.shape
    for rank, device in enumerate(ranked(devices)):
        owner = device // heads
        out_ref[rank] = total[:, owner * cols : (owner + 1) * cols]


def mix_kernel(middle_ref, pick_ref, got_ref, out_ref):
    total = middle_ref[...].astype(F32) + dot(pick_ref[...], got_ref[...])
    out_ref[...] = total.astype(BF16)


def long_mix_kernel(middle_ref, route_ref, got_ref, out_ref, *, experts, sources, part):
    slots = slot_table(route_ref[...], experts)

    def add(step, total):
        start = step * CHUNK_ROWS
        pick = pick_matrix(slots, start, CHUNK_ROWS, sources, part)
        return total + dot(pick, got_ref[pl.ds(start, CHUNK_ROWS), :])

    steps = got_ref.shape[0] // CHUNK_ROWS
    total = lax.fori_loop(0, steps, add, middle_ref[...].astype(F32))
    out_ref[...] = total.astype(BF16)


def paired(values):
    heads = lax.axis_size("tp")
    return lax.ppermute(values, "tp", [(i, i ^ 1) for i in range(heads)])


def update(parts, first, last, after, *begun):
    hbm = pl.BlockSpec(memory_space=pl.ANY)
    shape = parts[-1].shape
    begun = [far(part) for part in begun]
    return call(
        functools.partial(state_kernel, first=first, last=last),
        pltpu.HBM(shape, F32),
        [pl.BlockSpec(memory_space=pltpu.VMEM)] * 5 + [hbm] * len(begun),
        "state",
        out_specs=hbm,
        scratch_shapes=[
            pltpu.VMEM((last - first,) + shape[1:], F32),
            pltpu.SemaphoreType.DMA((last - first,)),
        ],
        input_output_aliases={5: 0} if begun else {},
        cost_estimate=pl.CostEstimate(flops=1 << 20, bytes_accessed=1 << 20, transcendentals=0),
    )(*map(near, parts), near(after), *begun)


def near(values):
    return pltpu.with_memory_space_constraint(values, pltpu.VMEM)


def far(values):
    return pltpu.with_memory_space_constraint(values, pltpu.HBM)


def call(kernel, out_shape, in_specs, name, out_specs=None, **kw):
    if out_specs is None:
        vmem = pl.BlockSpec(memory_space=pltpu.VMEM)
        out_specs = [vmem] * len(out_shape) if isinstance(out_shape, tuple) else vmem
    return pl.pallas_call(
        kernel,
        out_shape=out_shape,
        in_specs=in_specs,
        out_specs=out_specs,
        name=name,
        compiler_params=pltpu.CompilerParams(vmem_limit_bytes=VMEM_LIMIT),
        **kw,
    )


def shards(
    tokens, mix_gain, w_query, w_key, w_value, w_ogate, w_igate, w_fgate, forget_bias, head_gain,
    w_out, memory, normalizer, running_max, ffn_gain, route, route_weight, w_gate, w_up, w_down,
):
    vmem = pl.BlockSpec(memory_space=pltpu.VMEM)
    hbm = pl.BlockSpec(memory_space=pl.ANY)
    owners, heads = lax.axis_size("ep"), lax.axis_size("tp")
    chips = heads // 2
    rows, width = tokens.shape
    span = width // 2
    cols = width // owners
    count = route.shape[0]
    qk_dim, dv = w_query.shape[1], w_value.shape[1]
    part = EXPERT_CAPACITY // 2
    got_rows = owners * heads * part
    short = got_rows <= CHUNK_ROWS
    aligned = cols % LANES == 0
    sizes = dict(experts=owners, sources=heads, part=part)
    spec = jax.ShapeDtypeStruct
    memory_rows = memory.reshape(rows, qk_dim, dv)
    cell_inputs = dict(
        tokens=tokens,
        mix=mix_gain.reshape(1, -1),
        wi=w_igate.T,
        wf=w_fgate.T,
        bias=forget_bias.reshape(1, -1),
        max=running_max.T,
        route=route.T,
        share=route_weight.T,
        fgain=ffn_gain.reshape(1, -1),
        wq=w_query,
        wk=w_key,
        norm=normalizer.reshape(rows, qk_dim),
        mem=memory_rows,
        wv=w_value,
        wo=w_ogate,
        hgain=head_gain.reshape(1, -1),
        wout=w_out,
    )
    cell_inputs = [cell_inputs[name] for name in CELL_INPUTS]
    scratch = [
        (8, LANES) if name in CELL_PASSED else x.shape for name, x in zip(CELL_INPUTS, cell_inputs)
    ]
    own, send, norm_state, new_max, *state_parts, gain, near_route, near_weight = call(
        cell_kernel,
        (
            pltpu.VMEM((rows, span), F32),
            pltpu.VMEM((rows, span), BF16),
            pltpu.HBM((rows, qk_dim), F32),
            pltpu.HBM((1, rows), F32),
            pltpu.VMEM((rows, dv), F32),
            pltpu.VMEM((rows, qk_dim), F32),
            pltpu.VMEM((rows, dv), F32),
            pltpu.VMEM((rows, qk_dim, dv), F32),
            pltpu.VMEM((1, width), F32),
            pltpu.VMEM((route.shape[1], count), jnp.int32),
            pltpu.VMEM((route.shape[1], count), F32),
        ),
        [hbm] * len(cell_inputs),
        "cell",
        out_specs=[vmem, vmem, hbm, hbm] + [vmem] * 7,
        scratch_shapes=[pltpu.VMEM(shape, x.dtype) for shape, x in zip(scratch, cell_inputs)]
        + [
            pltpu.VMEM((rows, qk_dim), F32),
            pltpu.VMEM((1, rows), F32),
            pltpu.SemaphoreType.DMA((len(cell_inputs),)),
            pltpu.SemaphoreType.DMA((2,)),
        ],
    )(*map(far, cell_inputs))

    chosen, share, *pick = call(
        functools.partial(plan_kernel, **sizes),
        (
            pltpu.VMEM((EXPERT_CAPACITY, count), BF16),
            pltpu.VMEM((EXPERT_CAPACITY, LANES), F32),
        )
        + ((pltpu.VMEM((count, got_rows), BF16),) if short else ()),
        [vmem] * 2,
        "plan",
        cost_estimate=pl.CostEstimate(flops=1 << 22, bytes_accessed=1 << 16, transcendentals=0),
    )(near(near_route), near(near_weight))
    got, chosen, share, pick = lax.optimization_barrier((paired(send), chosen, share, pick))
    devices = owners * heads
    order = [ranked(devices)]
    weights = [near(w_gate[0]), near(w_up[0]), near(w_down[0])]
    chunks = call(
        pair_kernel, pltpu.VMEM((devices, rows, span // 2), BF16), [vmem] * 2, "pair"
    )(near(own), near(got))
    chunks = lax.all_to_all(
        chunks, ("ep", "tp"), split_axis=0, concat_axis=0, tiled=True, axis_index_groups=order
    )
    own = call(
        functools.partial(join_kernel, heads=heads),
        pltpu.VMEM((count, span), BF16),
        [vmem] * 4,
        "join",
    )(near(chunks), *weights)
    got = paired(own)
    state = update(state_parts, 0, rows // 2, own)
    kept, send, *own_middle = call(
        expert_kernel,
        (pltpu.VMEM((part, width), BF16), pltpu.VMEM((part, width), BF16))
        + ((pltpu.VMEM((count, cols), BF16),) if aligned else ()),
        [vmem] * 8 + [hbm],
        "expert",
    )(
        near(own),
        near(got),
        near(gain),
        near(chosen),
        near(share),
        *weights,
        far(state),
    )
    handed = paired(send)
    state = update(state_parts, rows // 2, rows, send, state)
    if aligned:
        pieces = call(
            functools.partial(spread_kernel, heads=heads),
            pltpu.VMEM((devices, part, cols), BF16),
            [vmem, vmem, hbm],
            "spread",
        )(near(kept), near(handed), far(state))
    else:
        first = lax.axis_index("tp") % 2 == 0
        sides = jnp.stack([jnp.where(first, own, got), jnp.where(first, got, own)], axis=1)
        middle = sides.reshape(count, 2, 2, span // 2).swapaxes(1, 2).reshape(count, width)
        start = lax.axis_index("ep") * cols
        own_middle = [lax.dynamic_slice_in_dim(middle, start, cols, axis=1)]
        total = (kept.astype(F32) + handed.astype(F32)).astype(BF16)
        total = total.reshape(part, owners, cols).transpose(1, 0, 2)
        pieces = total[jnp.asarray(order[0]) // heads]
    results = lax.all_to_all(
        pieces, ("ep", "tp"), split_axis=0, concat_axis=0, tiled=True, axis_index_groups=order
    )
    results = near(results.reshape(got_rows, cols))
    if short:
        mixed = call(mix_kernel, spec((count, cols), BF16), [vmem] * 3, "mix")(
            near(own_middle[0]), near(pick[0]), results
        )
    else:
        mixed = call(
            functools.partial(long_mix_kernel, **sizes),
            spec((count, cols), BF16),
            [vmem] * 3,
            "mix",
        )(own_middle[0], route.T, results)
    return (
        mixed,
        state.reshape(memory.shape),
        norm_state.reshape(normalizer.shape),
        new_max.T,
    )


def solution(mesh):
    return jax.shard_map(
        shards,
        mesh=mesh,
        in_specs=(
            P("ep", None),
            P(),
            P(None, "tp"),
            P(None, "tp"),
            P(None, "tp"),
            P(None, "tp"),
            P(),
            P(),
            P(),
            P("tp"),
            P("tp", None),
            P("ep", "tp", None, None),
            P("ep", "tp", None),
            P("ep", "tp"),
            P(),
            P(),
            P(),
            P("ep", None, "tp"),
            P("ep", None, "tp"),
            P("ep", "tp", None),
        ),
        out_specs=(P(None, "ep"), P("ep", "tp", None, None), P("ep", "tp", None), P("ep", "tp")),
        check_vma=False,
    )
```

```python
import functools

import jax
import jax.numpy as jnp
import numpy as np
from jax import lax
from jax.experimental import pallas as pl
from jax.experimental.pallas import tpu as pltpu
from jax.sharding import PartitionSpec as P

EXPERT_CAPACITY = 32
EPS = 1e-06
LANES = 128
CHUNK_ROWS = 512
VMEM_LIMIT = 32 << 20
CELL_INPUTS = (
    "tokens", "mix", "wq", "wi", "wf", "bias", "max", "wk", "norm", "mem", "hgain", "fgain", "route",
    "share", "source", "wv", "wo", "wout",
)
CELL_PASSED = ("mem", "fgain", "route", "share", "source")

F32 = jnp.float32
BF16 = jnp.bfloat16


def ranked(count):
    return [i // 2 if i % 2 == 0 else count - 1 - i // 2 for i in range(count)]


def led_by(leader, ranks):
    return [leader] + [rank for rank in ranks if rank != leader]


def iota(shape, dim):
    return lax.broadcasted_iota(jnp.int32, shape, dim)


def dot(a, b):
    return jnp.dot(a, b, preferred_element_type=F32)


def rounded(a, b):
    return dot(a, b).astype(BF16).astype(F32)


def norm_rows(floats, gain):
    scale = lax.rsqrt(jnp.mean(floats * floats, axis=-1, keepdims=True) + EPS)
    return (floats * scale * gain).astype(BF16)


def column_of(row, eye):
    return jnp.sum(jnp.where(eye, row, 0.0), axis=1, keepdims=True)


def row_of(column, eye):
    return jnp.sum(jnp.where(eye, column, 0.0), axis=0, keepdims=True)


def cell_kernel(*refs):
    count = len(CELL_INPUTS)
    far_refs, outs, scratch = refs[:count], refs[count : -count - 4], refs[-count - 4 :]
    near_refs, (nstate_near, nmax_near), (sems, out_sems) = scratch[:count], scratch[count:-2], scratch[-2:]
    (
        own_ref, send_ref, nstate_ref, nmax_ref, keep_ref, adk_ref, value_ref, mem_ref, gain_ref,
        route_ref, share_ref, source_ref,
    ) = outs
    direct = dict(zip(CELL_PASSED, (mem_ref, gain_ref, route_ref, share_ref, source_ref)))
    copies, local = {}, {}
    for i, name in enumerate(CELL_INPUTS):
        local[name] = direct.get(name, near_refs[i])
        copies[name] = pltpu.make_async_copy(far_refs[i], local[name], sems.at[i])
        copies[name].start()

    def ready(*names):
        for name in names:
            copies[name].wait()
        return local[names[-1]]

    head = lax.axis_index("tp")
    tokens = ready("tokens")[...].astype(F32)
    rows = tokens.shape[0]
    normed = norm_rows(tokens, ready("mix")[...])
    contract_last = (((1,), (1,)), ((), ()))
    wi_ref, wf_ref = ready("wi"), ready("wf")
    bias, old_max = ready("bias")[...], ready("max")[...]
    heads = bias.shape[1]
    pick = iota((rows, heads), 1) == head
    gate_in = lax.dot_general(normed, wi_ref[...], contract_last, preferred_element_type=F32)
    gate_forget = lax.dot_general(normed, wf_ref[...], contract_last, preferred_element_type=F32)
    log_in = jnp.sum(jnp.where(pick, gate_in, 0.0), axis=1, keepdims=True)
    forget_pre = jnp.sum(jnp.where(pick, gate_forget + bias, 0.0), axis=1, keepdims=True)
    log_forget = jnp.minimum(forget_pre, 0.0) - jnp.log1p(jnp.exp(-jnp.abs(forget_pre)))
    eye = iota((rows, rows), 0) == iota((rows, rows), 1)
    carried = log_forget + column_of(old_max, eye)
    new_max = jnp.maximum(carried, log_in)
    keep = jnp.exp(carried - new_max)
    admit = jnp.exp(log_in - new_max)
    nmax_near[...] = row_of(new_max, eye)
    nmax_copy = pltpu.make_async_copy(nmax_near, nmax_ref, out_sems.at[0])
    nmax_copy.start()
    ready("norm", "hgain", "fgain", "route", "share", "source", "wq", "wk")
    query = rounded(normed, local["wq"][...])
    scaled_key = rounded(normed, local["wk"][...]) * query.shape[1] ** (-0.5)
    admitted = admit * scaled_key
    norm_state = keep * local["norm"][...] + admitted
    nstate_near[...] = norm_state
    nstate_copy = pltpu.make_async_copy(nstate_near, nstate_ref, out_sems.at[1])
    nstate_copy.start()
    adk_ref[...] = admitted
    keep_ref[...] = jnp.broadcast_to(keep, keep_ref.shape)
    denom = jnp.sum(query * norm_state, axis=1, keepdims=True)
    overlap = jnp.sum(query * admitted, axis=1, keepdims=True)
    query_cols = jnp.transpose(query)
    mem = ready("mem")
    reads = [
        jnp.sum(query_cols[:, t : t + 1] * mem[t], axis=0, keepdims=True) for t in range(rows)
    ]
    ready("wv", "wo")
    value = rounded(normed, local["wv"][...])
    ogate = rounded(normed, local["wo"][...])
    value_ref[...] = value
    numer = keep * jnp.concatenate(reads, axis=0) + overlap * value
    read = numer / jnp.maximum(jnp.abs(denom), jnp.exp(-new_max))
    scale = lax.rsqrt(jnp.mean(read * read, axis=-1, keepdims=True) + EPS)
    gated = (jax.nn.sigmoid(ogate) * read * scale * local["hgain"][...]).astype(BF16)
    partial = dot(gated, ready("wout")[...])
    span = own_ref.shape[1]
    low, high = partial[:, :span], partial[:, span:]
    first = head % 2 == 0
    residual = jnp.where(first, tokens[:, :span], tokens[:, span:]) * 0.5
    own_ref[...] = jnp.where(first, low, high) + residual
    send_ref[...] = jnp.where(first, high, low).astype(BF16)
    nmax_copy.wait()
    nstate_copy.wait()


def state_kernel(keep_ref, adk_ref, value_ref, mem_ref, _, *refs, early):
    *_, out_ref, made, sems = refs

    @pl.when((lax.axis_index("ep") < lax.axis_size("ep") * 3 // 4) == early)
    def write():
        adk_cols = jnp.transpose(adk_ref[...])
        copies = []
        for t in range(mem_ref.shape[0]):
            old = keep_ref[t : t + 1, :] * mem_ref[t]
            made[t] = old + adk_cols[:, t : t + 1] * value_ref[t : t + 1, :]
            copies.append(pltpu.make_async_copy(made.at[t], out_ref.at[t], sems.at[t]))
            copies[-1].start()
        for copy in copies:
            copy.wait()


def pair_kernel(own_ref, got_ref, _, out_ref):
    total = (own_ref[...] + got_ref[...].astype(F32)).astype(BF16)
    for rank in range(out_ref.shape[0]):
        out_ref[rank] = total


def join_kernel(got_ref, *refs, order, chips):
    out_ref = refs[-1]
    rows = got_ref.shape[1]
    rank_of = {place: rank for rank, place in enumerate(order)}
    for owner in range(len(order) // chips):
        total = 0.0
        for chip in range(chips):
            total = total + got_ref[rank_of[owner * chips + chip]].astype(F32)
        out_ref[owner * rows : (owner + 1) * rows] = total.astype(BF16)


def earlier_matrix(count):
    return (iota((count, count), 0) < iota((count, count), 1)).astype(BF16)


def plan_kernel(route_ref, weight_ref, source_ref, chosen_ref, share_ref, *pick_refs, experts):
    route, weight = route_ref[...], weight_ref[...]
    count = route.shape[1]
    named = route == lax.axis_index("ep")
    share = jnp.where(named, weight, 0.0) / jnp.sum(weight, axis=0, keepdims=True)
    share = jnp.sum(share, axis=0, keepdims=True)
    member = jnp.sum(named.astype(F32), axis=0, keepdims=True)
    slot = dot(jnp.broadcast_to(member, (8, count)).astype(BF16), earlier_matrix(count))[0:1]
    shape = (EXPERT_CAPACITY, count)
    chosen = (iota(shape, 0).astype(F32) == slot) & (member > 0.5)
    chosen_ref[...] = chosen.astype(BF16)
    slot_share = jnp.sum(jnp.where(chosen, share, 0.0), axis=1, keepdims=True)
    share_ref[...] = jnp.broadcast_to(slot_share, share_ref.shape)
    for pick_ref in pick_refs:
        slots = slot_table(route, experts)
        pick_ref[...] = pick_matrix(slots, source_ref[...])


def slot_table(route, experts):
    count = route.shape[1]
    shape = (experts, count)
    member = jnp.zeros(shape, jnp.bool_)
    for choice in range(route.shape[0]):
        member = member | (iota(shape, 0) == route[choice : choice + 1])
    slots = dot(member.astype(BF16), earlier_matrix(count))
    return jnp.where(member, slots, -1.0).astype(BF16)


def pick_matrix(slots, source):
    shape = (slots.shape[0], source.shape[1])
    expand = (source == iota(shape, 0)).astype(BF16)
    expanded = lax.dot_general(
        slots, expand, (((0,), (0,)), ((), ())), preferred_element_type=F32
    )
    slot = iota((1, shape[1]), 1) % EXPERT_CAPACITY
    return (expanded == slot.astype(F32)).astype(BF16)


def expert_kernel(
    own_ref, got_ref, gain_ref, chosen_ref, share_ref, wg_ref, wu_ref, wd_ref, _,
    out_ref, *block_refs, order, chips,
):
    expert, half = lax.axis_index("ep"), lax.axis_index("tp") % 2
    span = own_ref.shape[1]
    width = 2 * span
    for block_ref in block_refs:
        cols = block_ref.shape[1]
        start = expert * cols
        inner = pl.ds(pl.multiple_of(start % span, cols), cols)
        mine = start // span == half
        block_ref[...] = jnp.where(mine, own_ref[:, inner], got_ref[:, inner])
    gate = up = 0.0
    chosen = chosen_ref[...]
    sides = []
    for side, ref in ((half, own_ref), (1 - half, got_ref)):
        rows = dot(chosen, ref[...])
        sides.append((rows, pl.multiple_of(side * span, span)))
    square = sum(jnp.sum(rows * rows, axis=-1, keepdims=True) for rows, _ in sides)
    scale = lax.rsqrt(square / width + EPS)
    for rows, start in sides:
        normed = (rows * scale * gain_ref[:, pl.ds(start, span)]).astype(BF16)
        gate = gate + dot(normed, wg_ref[pl.ds(start, span), :])
        up = up + dot(normed, wu_ref[pl.ds(start, span), :])
    act = (jax.nn.silu(gate) * up).astype(BF16)
    result = (dot(act, wd_ref[...]) * share_ref[:, 0:1]).astype(BF16)
    if not block_refs:
        out_ref[...] = result
        return
    for rank, place in enumerate(order):
        owner = place // chips
        out_ref[rank] = result[:, owner * cols : (owner + 1) * cols]


def mix_kernel(pick_ref, got_ref, own_ref, send_ref):
    total = dot(pick_ref[...], got_ref[...])
    own_ref[...] = total
    send_ref[...] = total.astype(BF16)


def long_mix_kernel(route_ref, source_ref, got_ref, own_ref, send_ref, *, experts):
    slots = slot_table(route_ref[...], experts)

    def add(step, total):
        rows = pl.ds(pl.multiple_of(step * CHUNK_ROWS, CHUNK_ROWS), CHUNK_ROWS)
        return total + dot(pick_matrix(slots, source_ref[:, rows]), got_ref[rows, :])

    steps = got_ref.shape[0] // CHUNK_ROWS
    total = lax.fori_loop(0, steps, add, jnp.zeros(own_ref.shape, F32))
    own_ref[...] = total
    send_ref[...] = total.astype(BF16)


def final_kernel(middle_ref, own_ref, got_ref, out_ref):
    total = middle_ref[...].astype(F32) + (own_ref[...] + got_ref[...].astype(F32))
    out_ref[...] = total.astype(BF16)


def paired(values):
    heads = lax.axis_size("tp")
    return lax.ppermute(values, "tp", [(i, i ^ 1) for i in range(heads)])


def update(parts, early, after, *begun):
    hbm = pl.BlockSpec(memory_space=pl.ANY)
    shape = parts[-1].shape
    begun = [far(part) for part in begun]
    return call(
        functools.partial(state_kernel, early=early),
        pltpu.HBM(shape, F32),
        [pl.BlockSpec(memory_space=pltpu.VMEM)] * 5 + [hbm] * len(begun),
        "state",
        out_specs=hbm,
        scratch_shapes=[pltpu.VMEM(shape, F32), pltpu.SemaphoreType.DMA(shape[:1])],
        input_output_aliases={5: 0} if begun else {},
        cost_estimate=pl.CostEstimate(flops=1 << 20, bytes_accessed=1 << 20, transcendentals=0),
    )(*map(near, parts), near(after), *begun)


def near(values):
    return pltpu.with_memory_space_constraint(values, pltpu.VMEM)


def far(values):
    return pltpu.with_memory_space_constraint(values, pltpu.HBM)


def call(kernel, out_shape, in_specs, name, out_specs=None, **kw):
    if out_specs is None:
        vmem = pl.BlockSpec(memory_space=pltpu.VMEM)
        out_specs = [vmem] * len(out_shape) if isinstance(out_shape, tuple) else vmem
    return pl.pallas_call(
        kernel,
        out_shape=out_shape,
        in_specs=in_specs,
        out_specs=out_specs,
        name=name,
        compiler_params=pltpu.CompilerParams(vmem_limit_bytes=VMEM_LIMIT),
        **kw,
    )


def shards(
    tokens, mix_gain, w_query, w_key, w_value, w_ogate, w_igate, w_fgate, forget_bias, head_gain,
    w_out, memory, normalizer, running_max, ffn_gain, route, route_weight, w_gate, w_up, w_down,
):
    vmem = pl.BlockSpec(memory_space=pltpu.VMEM)
    hbm = pl.BlockSpec(memory_space=pl.ANY)
    owners, heads = lax.axis_size("ep"), lax.axis_size("tp")
    chips = heads // 2
    rows, width = tokens.shape
    span = width // 2
    cols = width // owners
    count = route.shape[0]
    qk_dim, dv = w_query.shape[1], w_value.shape[1]
    places = owners * chips
    got_rows = places * EXPERT_CAPACITY
    short = got_rows <= CHUNK_ROWS
    aligned = cols % LANES == 0
    first_order = led_by(places // 2 - 1, range(places))
    second_order = led_by(3 * places // 4 - 1, ranked(places)[::-1])
    groups = [
        [[2 * place + core for place in order] for core in range(2)]
        for order in (first_order, second_order)
    ]
    source = np.repeat(np.array(second_order, np.int32) // chips, EXPERT_CAPACITY)
    spec = jax.ShapeDtypeStruct
    memory_rows = memory.reshape(rows, qk_dim, dv)
    cell_inputs = dict(
        tokens=tokens,
        mix=mix_gain.reshape(1, -1),
        wi=w_igate.T,
        wf=w_fgate.T,
        bias=forget_bias.reshape(1, -1),
        max=running_max.T,
        route=route.T,
        share=route_weight.T,
        source=jnp.asarray(source).reshape(1, -1),
        fgain=ffn_gain.reshape(1, -1),
        wq=w_query,
        wk=w_key,
        norm=normalizer.reshape(rows, qk_dim),
        mem=memory_rows,
        wv=w_value,
        wo=w_ogate,
        hgain=head_gain.reshape(1, -1),
        wout=w_out,
    )
    cell_inputs = [cell_inputs[name] for name in CELL_INPUTS]
    scratch = [
        (8, LANES) if name in CELL_PASSED else x.shape for name, x in zip(CELL_INPUTS, cell_inputs)
    ]
    own, send, norm_state, new_max, *state_parts, gain, near_route, near_weight, near_source = call(
        cell_kernel,
        (
            pltpu.VMEM((rows, span), F32),
            pltpu.VMEM((rows, span), BF16),
            pltpu.HBM((rows, qk_dim), F32),
            pltpu.HBM((1, rows), F32),
            pltpu.VMEM((rows, dv), F32),
            pltpu.VMEM((rows, qk_dim), F32),
            pltpu.VMEM((rows, dv), F32),
            pltpu.VMEM((rows, qk_dim, dv), F32),
            pltpu.VMEM((1, width), F32),
            pltpu.VMEM((route.shape[1], count), jnp.int32),
            pltpu.VMEM((route.shape[1], count), F32),
            pltpu.VMEM((1, got_rows), jnp.int32),
        ),
        [hbm] * len(cell_inputs),
        "cell",
        out_specs=[vmem, vmem, hbm, hbm] + [vmem] * 8,
        scratch_shapes=[pltpu.VMEM(shape, x.dtype) for shape, x in zip(scratch, cell_inputs)]
        + [
            pltpu.VMEM((rows, qk_dim), F32),
            pltpu.VMEM((1, rows), F32),
            pltpu.SemaphoreType.DMA((len(cell_inputs),)),
            pltpu.SemaphoreType.DMA((2,)),
        ],
    )(*map(far, cell_inputs))

    chosen, share, *pick = call(
        functools.partial(plan_kernel, experts=owners),
        (
            pltpu.VMEM((EXPERT_CAPACITY, count), BF16),
            pltpu.VMEM((EXPERT_CAPACITY, LANES), F32),
        )
        + ((pltpu.VMEM((count, got_rows), BF16),) if short else ()),
        [vmem] * 3,
        "plan",
        cost_estimate=pl.CostEstimate(flops=1 << 22, bytes_accessed=1 << 16, transcendentals=0),
    )(near(near_route), near(near_weight), near(near_source))
    got, chosen, share, pick = lax.optimization_barrier((paired(send), chosen, share, pick))
    state = update(state_parts, True, send)
    weights = [near(w_gate[0]), near(w_up[0]), near(w_down[0])]
    chunks = call(
        pair_kernel, pltpu.VMEM((places, rows, span), BF16), [vmem] * 2 + [hbm], "pair"
    )(near(own), near(got), far(state))
    chunks = lax.all_to_all(
        chunks, ("ep", "tp"), split_axis=0, concat_axis=0, tiled=True, axis_index_groups=groups[0]
    )
    own = call(
        functools.partial(join_kernel, order=first_order, chips=chips),
        pltpu.VMEM((count, span), BF16),
        [vmem] * 4,
        "join",
    )(near(chunks), *weights)
    got = paired(own)
    state = update(state_parts, False, own, state)
    shape = (places, EXPERT_CAPACITY, cols) if aligned else (EXPERT_CAPACITY, width)
    pieces, *own_middle = call(
        functools.partial(expert_kernel, order=second_order, chips=chips),
        (pltpu.VMEM(shape, BF16),) + ((pltpu.VMEM((count, cols), BF16),) if aligned else ()),
        [vmem] * 8 + [hbm],
        "expert",
    )(
        near(own),
        near(got),
        near(gain),
        near(chosen),
        near(share),
        *weights,
        far(state),
    )
    if not aligned:
        first = lax.axis_index("tp") % 2 == 0
        middle = jnp.concatenate([jnp.where(first, own, got), jnp.where(first, got, own)], axis=1)
        start = lax.axis_index("ep") * cols
        own_middle = [lax.dynamic_slice_in_dim(middle, start, cols, axis=1)]
        pieces = pieces.reshape(EXPERT_CAPACITY, owners, cols).transpose(1, 0, 2)
        pieces = pieces[np.array(second_order) // chips]
    results = lax.all_to_all(
        pieces, ("ep", "tp"), split_axis=0, concat_axis=0, tiled=True, axis_index_groups=groups[1]
    )
    results = near(results.reshape(got_rows, cols))
    shapes = (pltpu.VMEM((count, cols), F32), pltpu.VMEM((count, cols), BF16))
    if short:
        own, send = call(mix_kernel, shapes, [vmem] * 2, "mix")(near(pick[0]), results)
    else:
        own, send = call(
            functools.partial(long_mix_kernel, experts=owners), shapes, [vmem] * 3, "mix"
        )(near(near_route), near(near_source), results)
    mixed = call(final_kernel, spec((count, cols), BF16), [vmem] * 3, "final")(
        near(own_middle[0]), near(own), near(paired(send))
    )
    return (
        mixed,
        state.reshape(memory.shape),
        norm_state.reshape(normalizer.shape),
        new_max.T,
    )


def solution(mesh):
    return jax.shard_map(
        shards,
        mesh=mesh,
        in_specs=(
            P("ep", None),
            P(),
            P(None, "tp"),
            P(None, "tp"),
            P(None, "tp"),
            P(None, "tp"),
            P(),
            P(),
            P(),
            P("tp"),
            P("tp", None),
            P("ep", "tp", None, None),
            P("ep", "tp", None),
            P("ep", "tp"),
            P(),
            P(),
            P(),
            P("ep", None, "tp"),
            P("ep", None, "tp"),
            P("ep", "tp", None),
        ),
        out_specs=(P(None, "ep"), P("ep", "tp", None, None), P("ep", "tp", None), P("ep", "tp")),
        check_vma=False,
    )
```

```python
import functools

import jax
import jax.numpy as jnp
import numpy as np
from jax import lax
from jax.experimental import pallas as pl
from jax.experimental.pallas import tpu as pltpu
from jax.sharding import PartitionSpec as P

EXPERT_CAPACITY = 32
EPS = 1e-06
LANES = 128
CHUNK_ROWS = 512
VMEM_LIMIT = 32 << 20
CELL_INPUTS = (
    "tokens", "mix", "wq", "wi", "wf", "bias", "max", "wk", "norm", "mem", "hgain", "fgain", "route",
    "share", "source", "wv", "wo", "wout",
)
CELL_PASSED = ("mem", "fgain", "route", "share", "source")

F32 = jnp.float32
BF16 = jnp.bfloat16


def ranked(count):
    return [i // 2 if i % 2 == 0 else count - 1 - i // 2 for i in range(count)]


def led_by(leader, ranks):
    return [leader] + [rank for rank in ranks if rank != leader]


def iota(shape, dim):
    return lax.broadcasted_iota(jnp.int32, shape, dim)


def dot(a, b):
    return jnp.dot(a, b, preferred_element_type=F32)


def rounded(a, b):
    return dot(a, b).astype(BF16).astype(F32)


def norm_rows(floats, gain):
    scale = lax.rsqrt(jnp.mean(floats * floats, axis=-1, keepdims=True) + EPS)
    return (floats * scale * gain).astype(BF16)


def column_of(row, eye):
    return jnp.sum(jnp.where(eye, row, 0.0), axis=1, keepdims=True)


def row_of(column, eye):
    return jnp.sum(jnp.where(eye, column, 0.0), axis=0, keepdims=True)


def cell_kernel(*refs):
    count = len(CELL_INPUTS)
    far_refs, outs, scratch = refs[:count], refs[count : -count - 4], refs[-count - 4 :]
    near_refs, (nstate_near, nmax_near), (sems, out_sems) = scratch[:count], scratch[count:-2], scratch[-2:]
    (
        own_ref, send_ref, nstate_ref, nmax_ref, keep_ref, adk_ref, value_ref, mem_ref, gain_ref,
        route_ref, share_ref, source_ref,
    ) = outs
    direct = dict(zip(CELL_PASSED, (mem_ref, gain_ref, route_ref, share_ref, source_ref)))
    copies, local = {}, {}
    for i, name in enumerate(CELL_INPUTS):
        local[name] = direct.get(name, near_refs[i])
        copies[name] = pltpu.make_async_copy(far_refs[i], local[name], sems.at[i])
        copies[name].start()

    def ready(*names):
        for name in names:
            copies[name].wait()
        return local[names[-1]]

    head = lax.axis_index("tp")
    tokens = ready("tokens")[...].astype(F32)
    rows = tokens.shape[0]
    normed = norm_rows(tokens, ready("mix")[...])
    contract_last = (((1,), (1,)), ((), ()))
    wi_ref, wf_ref = ready("wi"), ready("wf")
    bias, old_max = ready("bias")[...], ready("max")[...]
    heads = bias.shape[1]
    pick = iota((rows, heads), 1) == head
    gate_in = lax.dot_general(normed, wi_ref[...], contract_last, preferred_element_type=F32)
    gate_forget = lax.dot_general(normed, wf_ref[...], contract_last, preferred_element_type=F32)
    log_in = jnp.sum(jnp.where(pick, gate_in, 0.0), axis=1, keepdims=True)
    forget_pre = jnp.sum(jnp.where(pick, gate_forget + bias, 0.0), axis=1, keepdims=True)
    log_forget = jnp.minimum(forget_pre, 0.0) - jnp.log1p(jnp.exp(-jnp.abs(forget_pre)))
    eye = iota((rows, rows), 0) == iota((rows, rows), 1)
    carried = log_forget + column_of(old_max, eye)
    new_max = jnp.maximum(carried, log_in)
    keep = jnp.exp(carried - new_max)
    admit = jnp.exp(log_in - new_max)
    nmax_near[...] = row_of(new_max, eye)
    nmax_copy = pltpu.make_async_copy(nmax_near, nmax_ref, out_sems.at[0])
    nmax_copy.start()
    ready("norm", "hgain", "fgain", "route", "share", "source", "wq", "wk")
    query = rounded(normed, local["wq"][...])
    scaled_key = rounded(normed, local["wk"][...]) * query.shape[1] ** (-0.5)
    admitted = admit * scaled_key
    norm_state = keep * local["norm"][...] + admitted
    nstate_near[...] = norm_state
    nstate_copy = pltpu.make_async_copy(nstate_near, nstate_ref, out_sems.at[1])
    nstate_copy.start()
    adk_ref[...] = admitted
    keep_ref[...] = jnp.broadcast_to(keep, keep_ref.shape)
    denom = jnp.sum(query * norm_state, axis=1, keepdims=True)
    overlap = jnp.sum(query * admitted, axis=1, keepdims=True)
    query_cols = jnp.transpose(query)
    mem = ready("mem")
    reads = [
        jnp.sum(query_cols[:, t : t + 1] * mem[t], axis=0, keepdims=True) for t in range(rows)
    ]
    ready("wv", "wo")
    value = rounded(normed, local["wv"][...])
    ogate = rounded(normed, local["wo"][...])
    value_ref[...] = value
    numer = keep * jnp.concatenate(reads, axis=0) + overlap * value
    read = numer / jnp.maximum(jnp.abs(denom), jnp.exp(-new_max))
    scale = lax.rsqrt(jnp.mean(read * read, axis=-1, keepdims=True) + EPS)
    gated = (jax.nn.sigmoid(ogate) * read * scale * local["hgain"][...]).astype(BF16)
    partial = dot(gated, ready("wout")[...])
    span = own_ref.shape[1]
    low, high = partial[:, :span], partial[:, span:]
    first = head % 2 == 0
    residual = jnp.where(first, tokens[:, :span], tokens[:, span:]) * 0.5
    own_ref[...] = jnp.where(first, low, high) + residual
    send_ref[...] = jnp.where(first, high, low).astype(BF16)
    nmax_copy.wait()
    nstate_copy.wait()


def state_kernel(keep_ref, adk_ref, value_ref, mem_ref, _, *refs, early):
    *_, out_ref, made, sems = refs

    @pl.when((lax.axis_index("ep") < lax.axis_size("ep") // 2) == early)
    def write():
        adk_cols = jnp.transpose(adk_ref[...])
        copies = []
        for t in range(mem_ref.shape[0]):
            old = keep_ref[t : t + 1, :] * mem_ref[t]
            made[t] = old + adk_cols[:, t : t + 1] * value_ref[t : t + 1, :]
            copies.append(pltpu.make_async_copy(made.at[t], out_ref.at[t], sems.at[t]))
            copies[-1].start()
        for copy in copies:
            copy.wait()


def pair_kernel(own_ref, got_ref, _, out_ref):
    total = (own_ref[...] + got_ref[...].astype(F32)).astype(BF16)
    for rank in range(out_ref.shape[0]):
        out_ref[rank] = total


def join_kernel(got_ref, *refs, order, chips):
    out_ref = refs[-1]
    rows = got_ref.shape[1]
    rank_of = {place: rank for rank, place in enumerate(order)}
    for owner in range(len(order) // chips):
        total = 0.0
        for chip in range(chips):
            total = total + got_ref[rank_of[owner * chips + chip]].astype(F32)
        out_ref[owner * rows : (owner + 1) * rows] = total.astype(BF16)


def earlier_matrix(count):
    return (iota((count, count), 0) < iota((count, count), 1)).astype(BF16)


def plan_kernel(route_ref, weight_ref, source_ref, chosen_ref, share_ref, *pick_refs, experts):
    route, weight = route_ref[...], weight_ref[...]
    count = route.shape[1]
    named = route == lax.axis_index("ep")
    share = jnp.where(named, weight, 0.0) / jnp.sum(weight, axis=0, keepdims=True)
    share = jnp.sum(share, axis=0, keepdims=True)
    member = jnp.sum(named.astype(F32), axis=0, keepdims=True)
    slot = dot(jnp.broadcast_to(member, (8, count)).astype(BF16), earlier_matrix(count))[0:1]
    shape = (EXPERT_CAPACITY, count)
    chosen = (iota(shape, 0).astype(F32) == slot) & (member > 0.5)
    chosen_ref[...] = chosen.astype(BF16)
    slot_share = jnp.sum(jnp.where(chosen, share, 0.0), axis=1, keepdims=True)
    share_ref[...] = jnp.broadcast_to(slot_share, share_ref.shape)
    for pick_ref in pick_refs:
        slots = slot_table(route, experts)
        pick_ref[...] = pick_matrix(slots, source_ref[...])


def slot_table(route, experts):
    count = route.shape[1]
    shape = (experts, count)
    member = jnp.zeros(shape, jnp.bool_)
    for choice in range(route.shape[0]):
        member = member | (iota(shape, 0) == route[choice : choice + 1])
    slots = dot(member.astype(BF16), earlier_matrix(count))
    return jnp.where(member, slots, -1.0).astype(BF16)


def pick_matrix(slots, source):
    shape = (slots.shape[0], source.shape[1])
    expand = (source == iota(shape, 0)).astype(BF16)
    expanded = lax.dot_general(
        slots, expand, (((0,), (0,)), ((), ())), preferred_element_type=F32
    )
    slot = iota((1, shape[1]), 1) % EXPERT_CAPACITY
    return (expanded == slot.astype(F32)).astype(BF16)


def expert_kernel(
    own_ref, got_ref, gain_ref, chosen_ref, share_ref, wg_ref, wu_ref, wd_ref,
    out_ref, *block_refs, order, chips,
):
    expert, half = lax.axis_index("ep"), lax.axis_index("tp") % 2
    span = own_ref.shape[1]
    width = 2 * span
    for block_ref in block_refs:
        cols = block_ref.shape[1]
        start = expert * cols
        inner = pl.ds(pl.multiple_of(start % span, cols), cols)
        mine = start // span == half
        block_ref[...] = jnp.where(mine, own_ref[:, inner], got_ref[:, inner])
    gate = up = 0.0
    chosen = chosen_ref[...]
    sides = []
    for side, ref in ((half, own_ref), (1 - half, got_ref)):
        rows = dot(chosen, ref[...])
        sides.append((rows, pl.multiple_of(side * span, span)))
    square = sum(jnp.sum(rows * rows, axis=-1, keepdims=True) for rows, _ in sides)
    scale = lax.rsqrt(square / width + EPS)
    for rows, start in sides:
        normed = (rows * scale * gain_ref[:, pl.ds(start, span)]).astype(BF16)
        gate = gate + dot(normed, wg_ref[pl.ds(start, span), :])
        up = up + dot(normed, wu_ref[pl.ds(start, span), :])
    act = (jax.nn.silu(gate) * up).astype(BF16)
    result = (dot(act, wd_ref[...]) * share_ref[:, 0:1]).astype(BF16)
    if not block_refs:
        out_ref[...] = result
        return
    for rank, place in enumerate(order):
        owner = place // chips
        out_ref[rank] = result[:, owner * cols : (owner + 1) * cols]


def mix_kernel(pick_ref, got_ref, own_ref, send_ref):
    total = dot(pick_ref[...], got_ref[...])
    own_ref[...] = total
    send_ref[...] = total.astype(BF16)


def long_mix_kernel(route_ref, source_ref, got_ref, own_ref, send_ref, *, experts):
    slots = slot_table(route_ref[...], experts)

    def add(step, total):
        rows = pl.ds(pl.multiple_of(step * CHUNK_ROWS, CHUNK_ROWS), CHUNK_ROWS)
        return total + dot(pick_matrix(slots, source_ref[:, rows]), got_ref[rows, :])

    steps = got_ref.shape[0] // CHUNK_ROWS
    total = lax.fori_loop(0, steps, add, jnp.zeros(own_ref.shape, F32))
    own_ref[...] = total
    send_ref[...] = total.astype(BF16)


def final_kernel(middle_ref, own_ref, got_ref, _, out_ref):
    total = middle_ref[...].astype(F32) + (own_ref[...] + got_ref[...].astype(F32))
    out_ref[...] = total.astype(BF16)


def paired(values):
    heads = lax.axis_size("tp")
    return lax.ppermute(values, "tp", [(i, i ^ 1) for i in range(heads)])


def update(parts, early, after, *begun):
    hbm = pl.BlockSpec(memory_space=pl.ANY)
    shape = parts[-1].shape
    begun = [far(part) for part in begun]
    return call(
        functools.partial(state_kernel, early=early),
        pltpu.HBM(shape, F32),
        [pl.BlockSpec(memory_space=pltpu.VMEM)] * 5 + [hbm] * len(begun),
        "state",
        out_specs=hbm,
        scratch_shapes=[pltpu.VMEM(shape, F32), pltpu.SemaphoreType.DMA(shape[:1])],
        input_output_aliases={5: 0} if begun else {},
        cost_estimate=pl.CostEstimate(flops=1 << 20, bytes_accessed=1 << 20, transcendentals=0),
    )(*map(near, parts), near(after), *begun)


def near(values):
    return pltpu.with_memory_space_constraint(values, pltpu.VMEM)


def far(values):
    return pltpu.with_memory_space_constraint(values, pltpu.HBM)


def call(kernel, out_shape, in_specs, name, out_specs=None, **kw):
    if out_specs is None:
        vmem = pl.BlockSpec(memory_space=pltpu.VMEM)
        out_specs = [vmem] * len(out_shape) if isinstance(out_shape, tuple) else vmem
    return pl.pallas_call(
        kernel,
        out_shape=out_shape,
        in_specs=in_specs,
        out_specs=out_specs,
        name=name,
        compiler_params=pltpu.CompilerParams(vmem_limit_bytes=VMEM_LIMIT),
        **kw,
    )


def shards(
    tokens, mix_gain, w_query, w_key, w_value, w_ogate, w_igate, w_fgate, forget_bias, head_gain,
    w_out, memory, normalizer, running_max, ffn_gain, route, route_weight, w_gate, w_up, w_down,
):
    vmem = pl.BlockSpec(memory_space=pltpu.VMEM)
    hbm = pl.BlockSpec(memory_space=pl.ANY)
    owners, heads = lax.axis_size("ep"), lax.axis_size("tp")
    chips = heads // 2
    rows, width = tokens.shape
    span = width // 2
    cols = width // owners
    count = route.shape[0]
    qk_dim, dv = w_query.shape[1], w_value.shape[1]
    places = owners * chips
    got_rows = places * EXPERT_CAPACITY
    short = got_rows <= CHUNK_ROWS
    aligned = cols % LANES == 0
    first_order = led_by(3 * places // 4 - 1, range(places))
    second_order = led_by(3 * places // 4 - 1, ranked(places)[::-1])
    groups = [
        [[2 * place + core for place in first_order] for core in range(2)],
        [
            [2 * place + (core + (place >= places // 2)) % 2 for place in second_order]
            for core in range(2)
        ],
    ]
    source = np.repeat(np.array(second_order, np.int32) // chips, EXPERT_CAPACITY)
    spec = jax.ShapeDtypeStruct
    memory_rows = memory.reshape(rows, qk_dim, dv)
    cell_inputs = dict(
        tokens=tokens,
        mix=mix_gain.reshape(1, -1),
        wi=w_igate.T,
        wf=w_fgate.T,
        bias=forget_bias.reshape(1, -1),
        max=running_max.T,
        route=route.T,
        share=route_weight.T,
        source=jnp.asarray(source).reshape(1, -1),
        fgain=ffn_gain.reshape(1, -1),
        wq=w_query,
        wk=w_key,
        norm=normalizer.reshape(rows, qk_dim),
        mem=memory_rows,
        wv=w_value,
        wo=w_ogate,
        hgain=head_gain.reshape(1, -1),
        wout=w_out,
    )
    cell_inputs = [cell_inputs[name] for name in CELL_INPUTS]
    scratch = [
        (8, LANES) if name in CELL_PASSED else x.shape for name, x in zip(CELL_INPUTS, cell_inputs)
    ]
    own, send, norm_state, new_max, *state_parts, gain, near_route, near_weight, near_source = call(
        cell_kernel,
        (
            pltpu.VMEM((rows, span), F32),
            pltpu.VMEM((rows, span), BF16),
            pltpu.HBM((rows, qk_dim), F32),
            pltpu.HBM((1, rows), F32),
            pltpu.VMEM((rows, dv), F32),
            pltpu.VMEM((rows, qk_dim), F32),
            pltpu.VMEM((rows, dv), F32),
            pltpu.VMEM((rows, qk_dim, dv), F32),
            pltpu.VMEM((1, width), F32),
            pltpu.VMEM((route.shape[1], count), jnp.int32),
            pltpu.VMEM((route.shape[1], count), F32),
            pltpu.VMEM((1, got_rows), jnp.int32),
        ),
        [hbm] * len(cell_inputs),
        "cell",
        out_specs=[vmem, vmem, hbm, hbm] + [vmem] * 8,
        scratch_shapes=[pltpu.VMEM(shape, x.dtype) for shape, x in zip(scratch, cell_inputs)]
        + [
            pltpu.VMEM((rows, qk_dim), F32),
            pltpu.VMEM((1, rows), F32),
            pltpu.SemaphoreType.DMA((len(cell_inputs),)),
            pltpu.SemaphoreType.DMA((2,)),
        ],
    )(*map(far, cell_inputs))

    chosen, share, *pick = call(
        functools.partial(plan_kernel, experts=owners),
        (
            pltpu.VMEM((EXPERT_CAPACITY, count), BF16),
            pltpu.VMEM((EXPERT_CAPACITY, LANES), F32),
        )
        + ((pltpu.VMEM((count, got_rows), BF16),) if short else ()),
        [vmem] * 3,
        "plan",
        cost_estimate=pl.CostEstimate(flops=1 << 22, bytes_accessed=1 << 16, transcendentals=0),
    )(near(near_route), near(near_weight), near(near_source))
    got, chosen, share, pick = lax.optimization_barrier((paired(send), chosen, share, pick))
    state = update(state_parts, True, send)
    weights = [near(w_gate[0]), near(w_up[0]), near(w_down[0])]
    chunks = call(
        pair_kernel, pltpu.VMEM((places, rows, span), BF16), [vmem] * 2 + [hbm], "pair"
    )(near(own), near(got), far(state))
    chunks = lax.all_to_all(
        chunks, ("ep", "tp"), split_axis=0, concat_axis=0, tiled=True, axis_index_groups=groups[0]
    )
    own = call(
        functools.partial(join_kernel, order=first_order, chips=chips),
        pltpu.VMEM((count, span), BF16),
        [vmem] * 4,
        "join",
    )(near(chunks), *weights)
    got = paired(own)
    shape = (places, EXPERT_CAPACITY, cols) if aligned else (EXPERT_CAPACITY, width)
    pieces, *own_middle = call(
        functools.partial(expert_kernel, order=second_order, chips=chips),
        (pltpu.VMEM(shape, BF16),) + ((pltpu.VMEM((count, cols), BF16),) if aligned else ()),
        [vmem] * 8,
        "expert",
    )(
        near(own),
        near(got),
        near(gain),
        near(chosen),
        near(share),
        *weights,
    )
    if not aligned:
        first = lax.axis_index("tp") % 2 == 0
        middle = jnp.concatenate([jnp.where(first, own, got), jnp.where(first, got, own)], axis=1)
        start = lax.axis_index("ep") * cols
        own_middle = [lax.dynamic_slice_in_dim(middle, start, cols, axis=1)]
        pieces = pieces.reshape(EXPERT_CAPACITY, owners, cols).transpose(1, 0, 2)
        pieces = pieces[np.array(second_order) // chips]
    results = lax.all_to_all(
        pieces, ("ep", "tp"), split_axis=0, concat_axis=0, tiled=True, axis_index_groups=groups[1]
    )
    results = near(results.reshape(got_rows, cols))
    shapes = (pltpu.VMEM((count, cols), F32), pltpu.VMEM((count, cols), BF16))
    if short:
        own, send = call(mix_kernel, shapes, [vmem] * 2, "mix")(near(pick[0]), results)
    else:
        own, send = call(
            functools.partial(long_mix_kernel, experts=owners), shapes, [vmem] * 3, "mix"
        )(near(near_route), near(near_source), results)
    got = paired(send)
    state = update(state_parts, False, send, state)
    mixed = call(final_kernel, spec((count, cols), BF16), [vmem] * 3 + [hbm], "final")(
        near(own_middle[0]), near(own), near(got), far(state)
    )
    return (
        mixed,
        state.reshape(memory.shape),
        norm_state.reshape(normalizer.shape),
        new_max.T,
    )


def solution(mesh):
    return jax.shard_map(
        shards,
        mesh=mesh,
        in_specs=(
            P("ep", None),
            P(),
            P(None, "tp"),
            P(None, "tp"),
            P(None, "tp"),
            P(None, "tp"),
            P(),
            P(),
            P(),
            P("tp"),
            P("tp", None),
            P("ep", "tp", None, None),
            P("ep", "tp", None),
            P("ep", "tp"),
            P(),
            P(),
            P(),
            P("ep", None, "tp"),
            P("ep", None, "tp"),
            P("ep", "tp", None),
        ),
        out_specs=(P(None, "ep"), P("ep", "tp", None, None), P("ep", "tp", None), P("ep", "tp")),
        check_vma=False,
    )
```

```python
import functools

import jax
import jax.numpy as jnp
import numpy as np
from jax import lax
from jax.experimental import pallas as pl
from jax.experimental.pallas import tpu as pltpu
from jax.sharding import PartitionSpec as P

EXPERT_CAPACITY = 32
EPS = 1e-06
LANES = 128
CHUNK_ROWS = 512
VMEM_LIMIT = 32 << 20
CELL_INPUTS = (
    "tokens", "mix", "wq", "wi", "wf", "bias", "max", "wk", "norm", "mem", "hgain", "fgain", "route",
    "share", "source", "wv", "wo", "wout",
)
CELL_PASSED = ("mem", "fgain", "route", "share", "source")

F32 = jnp.float32
BF16 = jnp.bfloat16


def ranked(count):
    return [i // 2 if i % 2 == 0 else count - 1 - i // 2 for i in range(count)]


def led_by(leader, ranks):
    return [leader] + [rank for rank in ranks if rank != leader]


def iota(shape, dim):
    return lax.broadcasted_iota(jnp.int32, shape, dim)


def dot(a, b):
    return jnp.dot(a, b, preferred_element_type=F32)


def rounded(a, b):
    return dot(a, b).astype(BF16).astype(F32)


def norm_rows(floats, gain):
    scale = lax.rsqrt(jnp.mean(floats * floats, axis=-1, keepdims=True) + EPS)
    return (floats * scale * gain).astype(BF16)


def column_of(row, eye):
    return jnp.sum(jnp.where(eye, row, 0.0), axis=1, keepdims=True)


def row_of(column, eye):
    return jnp.sum(jnp.where(eye, column, 0.0), axis=0, keepdims=True)


def cell_kernel(*refs):
    count = len(CELL_INPUTS)
    far_refs, outs, scratch = refs[:count], refs[count : -count - 4], refs[-count - 4 :]
    near_refs, (nstate_near, nmax_near), (sems, out_sems) = scratch[:count], scratch[count:-2], scratch[-2:]
    (
        own_ref, send_ref, nstate_ref, nmax_ref, keep_ref, adk_ref, value_ref, mem_ref, gain_ref,
        route_ref, share_ref, source_ref,
    ) = outs
    direct = dict(zip(CELL_PASSED, (mem_ref, gain_ref, route_ref, share_ref, source_ref)))
    copies, local = {}, {}
    for i, name in enumerate(CELL_INPUTS):
        local[name] = direct.get(name, near_refs[i])
        copies[name] = pltpu.make_async_copy(far_refs[i], local[name], sems.at[i])
        copies[name].start()

    def ready(*names):
        for name in names:
            copies[name].wait()
        return local[names[-1]]

    head = lax.axis_index("tp")
    tokens = ready("tokens")[...].astype(F32)
    rows = tokens.shape[0]
    normed = norm_rows(tokens, ready("mix")[...])
    contract_last = (((1,), (1,)), ((), ()))
    wi_ref, wf_ref = ready("wi"), ready("wf")
    bias, old_max = ready("bias")[...], ready("max")[...]
    heads = bias.shape[1]
    pick = iota((rows, heads), 1) == head
    gate_in = lax.dot_general(normed, wi_ref[...], contract_last, preferred_element_type=F32)
    gate_forget = lax.dot_general(normed, wf_ref[...], contract_last, preferred_element_type=F32)
    log_in = jnp.sum(jnp.where(pick, gate_in, 0.0), axis=1, keepdims=True)
    forget_pre = jnp.sum(jnp.where(pick, gate_forget + bias, 0.0), axis=1, keepdims=True)
    log_forget = jnp.minimum(forget_pre, 0.0) - jnp.log1p(jnp.exp(-jnp.abs(forget_pre)))
    eye = iota((rows, rows), 0) == iota((rows, rows), 1)
    carried = log_forget + column_of(old_max, eye)
    new_max = jnp.maximum(carried, log_in)
    keep = jnp.exp(carried - new_max)
    admit = jnp.exp(log_in - new_max)
    nmax_near[...] = row_of(new_max, eye)
    nmax_copy = pltpu.make_async_copy(nmax_near, nmax_ref, out_sems.at[0])
    nmax_copy.start()
    ready("norm", "hgain", "fgain", "route", "share", "source", "wq", "wk")
    query = rounded(normed, local["wq"][...])
    scaled_key = rounded(normed, local["wk"][...]) * query.shape[1] ** (-0.5)
    admitted = admit * scaled_key
    norm_state = keep * local["norm"][...] + admitted
    nstate_near[...] = norm_state
    nstate_copy = pltpu.make_async_copy(nstate_near, nstate_ref, out_sems.at[1])
    nstate_copy.start()
    adk_ref[...] = admitted
    keep_ref[...] = jnp.broadcast_to(keep, keep_ref.shape)
    denom = jnp.sum(query * norm_state, axis=1, keepdims=True)
    overlap = jnp.sum(query * admitted, axis=1, keepdims=True)
    query_cols = jnp.transpose(query)
    mem = ready("mem")
    reads = [
        jnp.sum(query_cols[:, t : t + 1] * mem[t], axis=0, keepdims=True) for t in range(rows)
    ]
    ready("wv", "wo")
    value = rounded(normed, local["wv"][...])
    ogate = rounded(normed, local["wo"][...])
    value_ref[...] = value
    numer = keep * jnp.concatenate(reads, axis=0) + overlap * value
    read = numer / jnp.maximum(jnp.abs(denom), jnp.exp(-new_max))
    scale = lax.rsqrt(jnp.mean(read * read, axis=-1, keepdims=True) + EPS)
    gated = (jax.nn.sigmoid(ogate) * read * scale * local["hgain"][...]).astype(BF16)
    partial = dot(gated, ready("wout")[...])
    span = own_ref.shape[1]
    low, high = partial[:, :span], partial[:, span:]
    first = head % 2 == 0
    residual = jnp.where(first, tokens[:, :span], tokens[:, span:]) * 0.5
    own_ref[...] = jnp.where(first, low, high) + residual
    send_ref[...] = jnp.where(first, high, low).astype(BF16)
    nmax_copy.wait()
    nstate_copy.wait()


def state_kernel(keep_ref, adk_ref, value_ref, mem_ref, _, *refs, early):
    *_, out_ref, made, sems = refs

    @pl.when((lax.axis_index("ep") < lax.axis_size("ep") // 2) == early)
    def write():
        adk_cols = jnp.transpose(adk_ref[...])
        copies = []
        for t in range(mem_ref.shape[0]):
            old = keep_ref[t : t + 1, :] * mem_ref[t]
            made[t] = old + adk_cols[:, t : t + 1] * value_ref[t : t + 1, :]
            copies.append(pltpu.make_async_copy(made.at[t], out_ref.at[t], sems.at[t]))
            copies[-1].start()
        for copy in copies:
            copy.wait()


def pair_kernel(own_ref, got_ref, _, out_ref):
    total = (own_ref[...] + got_ref[...].astype(F32)).astype(BF16)
    for rank in range(out_ref.shape[0]):
        out_ref[rank] = total


def join_kernel(got_ref, *refs, order, chips):
    out_ref = refs[-1]
    rows = got_ref.shape[1]
    rank_of = {place: rank for rank, place in enumerate(order)}
    for owner in range(len(order) // chips):
        total = 0.0
        for chip in range(chips):
            total = total + got_ref[rank_of[owner * chips + chip]].astype(F32)
        out_ref[owner * rows : (owner + 1) * rows] = total.astype(BF16)


def earlier_matrix(count):
    return (iota((count, count), 0) < iota((count, count), 1)).astype(BF16)


def plan_kernel(route_ref, weight_ref, source_ref, chosen_ref, share_ref, *pick_refs, experts):
    route, weight = route_ref[...], weight_ref[...]
    count = route.shape[1]
    named = route == lax.axis_index("ep")
    share = jnp.where(named, weight, 0.0) / jnp.sum(weight, axis=0, keepdims=True)
    share = jnp.sum(share, axis=0, keepdims=True)
    member = jnp.sum(named.astype(F32), axis=0, keepdims=True)
    slot = dot(jnp.broadcast_to(member, (8, count)).astype(BF16), earlier_matrix(count))[0:1]
    shape = (EXPERT_CAPACITY, count)
    chosen = (iota(shape, 0).astype(F32) == slot) & (member > 0.5)
    chosen_ref[...] = chosen.astype(BF16)
    slot_share = jnp.sum(jnp.where(chosen, share, 0.0), axis=1, keepdims=True)
    share_ref[...] = jnp.broadcast_to(slot_share, share_ref.shape)
    for pick_ref in pick_refs:
        slots = slot_table(route, experts)
        pick_ref[...] = pick_matrix(slots, source_ref[...])


def slot_table(route, experts):
    count = route.shape[1]
    shape = (experts, count)
    member = jnp.zeros(shape, jnp.bool_)
    for choice in range(route.shape[0]):
        member = member | (iota(shape, 0) == route[choice : choice + 1])
    slots = dot(member.astype(BF16), earlier_matrix(count))
    return jnp.where(member, slots, -1.0).astype(BF16)


def pick_matrix(slots, source):
    shape = (slots.shape[0], source.shape[1])
    expand = (source == iota(shape, 0)).astype(BF16)
    expanded = lax.dot_general(
        slots, expand, (((0,), (0,)), ((), ())), preferred_element_type=F32
    )
    slot = iota((1, shape[1]), 1) % EXPERT_CAPACITY
    return (expanded == slot.astype(F32)).astype(BF16)


def expert_kernel(
    own_ref, got_ref, gain_ref, chosen_ref, share_ref, wg_ref, wu_ref, wd_ref,
    out_ref, *block_refs, order, chips,
):
    expert, half = lax.axis_index("ep"), lax.axis_index("tp") % 2
    span = own_ref.shape[1]
    width = 2 * span
    for block_ref in block_refs:
        cols = block_ref.shape[1]
        start = expert * cols
        inner = pl.ds(pl.multiple_of(start % span, cols), cols)
        mine = start // span == half
        block_ref[...] = jnp.where(mine, own_ref[:, inner], got_ref[:, inner])
    gate = up = 0.0
    chosen = chosen_ref[...]
    sides = []
    for side, ref in ((half, own_ref), (1 - half, got_ref)):
        rows = dot(chosen, ref[...])
        sides.append((rows, pl.multiple_of(side * span, span)))
    square = sum(jnp.sum(rows * rows, axis=-1, keepdims=True) for rows, _ in sides)
    scale = lax.rsqrt(square / width + EPS)
    for rows, start in sides:
        normed = (rows * scale * gain_ref[:, pl.ds(start, span)]).astype(BF16)
        gate = gate + dot(normed, wg_ref[pl.ds(start, span), :])
        up = up + dot(normed, wu_ref[pl.ds(start, span), :])
    act = (jax.nn.silu(gate) * up).astype(BF16)
    result = (dot(act, wd_ref[...]) * share_ref[:, 0:1]).astype(BF16)
    if not block_refs:
        out_ref[...] = result
        return
    for rank, place in enumerate(order):
        owner = place // chips
        out_ref[rank] = result[:, owner * cols : (owner + 1) * cols]


def mix_kernel(pick_ref, got_ref, own_ref, send_ref):
    total = dot(pick_ref[...], got_ref[...])
    own_ref[...] = total
    send_ref[...] = total.astype(BF16)


def long_mix_kernel(route_ref, source_ref, got_ref, own_ref, send_ref, *, experts):
    slots = slot_table(route_ref[...], experts)

    def add(step, total):
        rows = pl.ds(pl.multiple_of(step * CHUNK_ROWS, CHUNK_ROWS), CHUNK_ROWS)
        return total + dot(pick_matrix(slots, source_ref[:, rows]), got_ref[rows, :])

    steps = got_ref.shape[0] // CHUNK_ROWS
    total = lax.fori_loop(0, steps, add, jnp.zeros(own_ref.shape, F32))
    own_ref[...] = total
    send_ref[...] = total.astype(BF16)


def final_kernel(middle_ref, own_ref, got_ref, _, out_ref):
    total = middle_ref[...].astype(F32) + (own_ref[...] + got_ref[...].astype(F32))
    out_ref[...] = total.astype(BF16)


def paired(values):
    heads = lax.axis_size("tp")
    return lax.ppermute(values, "tp", [(i, i ^ 1) for i in range(heads)])


def update(parts, early, after, *begun):
    hbm = pl.BlockSpec(memory_space=pl.ANY)
    shape = parts[-1].shape
    begun = [far(part) for part in begun]
    return call(
        functools.partial(state_kernel, early=early),
        pltpu.HBM(shape, F32),
        [pl.BlockSpec(memory_space=pltpu.VMEM)] * 5 + [hbm] * len(begun),
        "state",
        out_specs=hbm,
        scratch_shapes=[pltpu.VMEM(shape, F32), pltpu.SemaphoreType.DMA(shape[:1])],
        input_output_aliases={5: 0} if begun else {},
        cost_estimate=pl.CostEstimate(flops=1 << 20, bytes_accessed=1 << 20, transcendentals=0),
    )(*map(near, parts), near(after), *begun)


def near(values):
    return pltpu.with_memory_space_constraint(values, pltpu.VMEM)


def far(values):
    return pltpu.with_memory_space_constraint(values, pltpu.HBM)


def call(kernel, out_shape, in_specs, name, out_specs=None, **kw):
    if out_specs is None:
        vmem = pl.BlockSpec(memory_space=pltpu.VMEM)
        out_specs = [vmem] * len(out_shape) if isinstance(out_shape, tuple) else vmem
    return pl.pallas_call(
        kernel,
        out_shape=out_shape,
        in_specs=in_specs,
        out_specs=out_specs,
        name=name,
        compiler_params=pltpu.CompilerParams(vmem_limit_bytes=VMEM_LIMIT),
        **kw,
    )


def shards(
    tokens, mix_gain, w_query, w_key, w_value, w_ogate, w_igate, w_fgate, forget_bias, head_gain,
    w_out, memory, normalizer, running_max, ffn_gain, route, route_weight, w_gate, w_up, w_down,
):
    vmem = pl.BlockSpec(memory_space=pltpu.VMEM)
    hbm = pl.BlockSpec(memory_space=pl.ANY)
    owners, heads = lax.axis_size("ep"), lax.axis_size("tp")
    chips = heads // 2
    rows, width = tokens.shape
    span = width // 2
    cols = width // owners
    count = route.shape[0]
    qk_dim, dv = w_query.shape[1], w_value.shape[1]
    places = owners * chips
    got_rows = places * EXPERT_CAPACITY
    short = got_rows <= CHUNK_ROWS
    aligned = cols % LANES == 0
    first_order = led_by(3 * places // 4 - 1, ranked(places)[::-1])
    second_order = led_by(3 * places // 4 - 1, ranked(places)[::-1])
    groups = [
        [[2 * place + core for place in first_order] for core in range(2)],
        [
            [2 * place + (core + (place >= places // 2)) % 2 for place in second_order]
            for core in range(2)
        ],
    ]
    source = np.repeat(np.array(second_order, np.int32) // chips, EXPERT_CAPACITY)
    spec = jax.ShapeDtypeStruct
    memory_rows = memory.reshape(rows, qk_dim, dv)
    cell_inputs = dict(
        tokens=tokens,
        mix=mix_gain.reshape(1, -1),
        wi=w_igate.T,
        wf=w_fgate.T,
        bias=forget_bias.reshape(1, -1),
        max=running_max.T,
        route=route.T,
        share=route_weight.T,
        source=jnp.asarray(source).reshape(1, -1),
        fgain=ffn_gain.reshape(1, -1),
        wq=w_query,
        wk=w_key,
        norm=normalizer.reshape(rows, qk_dim),
        mem=memory_rows,
        wv=w_value,
        wo=w_ogate,
        hgain=head_gain.reshape(1, -1),
        wout=w_out,
    )
    cell_inputs = [cell_inputs[name] for name in CELL_INPUTS]
    scratch = [
        (8, LANES) if name in CELL_PASSED else x.shape for name, x in zip(CELL_INPUTS, cell_inputs)
    ]
    own, send, norm_state, new_max, *state_parts, gain, near_route, near_weight, near_source = call(
        cell_kernel,
        (
            pltpu.VMEM((rows, span), F32),
            pltpu.VMEM((rows, span), BF16),
            pltpu.HBM((rows, qk_dim), F32),
            pltpu.HBM((1, rows), F32),
            pltpu.VMEM((rows, dv), F32),
            pltpu.VMEM((rows, qk_dim), F32),
            pltpu.VMEM((rows, dv), F32),
            pltpu.VMEM((rows, qk_dim, dv), F32),
            pltpu.VMEM((1, width), F32),
            pltpu.VMEM((route.shape[1], count), jnp.int32),
            pltpu.VMEM((route.shape[1], count), F32),
            pltpu.VMEM((1, got_rows), jnp.int32),
        ),
        [hbm] * len(cell_inputs),
        "cell",
        out_specs=[vmem, vmem, hbm, hbm] + [vmem] * 8,
        scratch_shapes=[pltpu.VMEM(shape, x.dtype) for shape, x in zip(scratch, cell_inputs)]
        + [
            pltpu.VMEM((rows, qk_dim), F32),
            pltpu.VMEM((1, rows), F32),
            pltpu.SemaphoreType.DMA((len(cell_inputs),)),
            pltpu.SemaphoreType.DMA((2,)),
        ],
    )(*map(far, cell_inputs))

    chosen, share, *pick = call(
        functools.partial(plan_kernel, experts=owners),
        (
            pltpu.VMEM((EXPERT_CAPACITY, count), BF16),
            pltpu.VMEM((EXPERT_CAPACITY, LANES), F32),
        )
        + ((pltpu.VMEM((count, got_rows), BF16),) if short else ()),
        [vmem] * 3,
        "plan",
        cost_estimate=pl.CostEstimate(flops=1 << 22, bytes_accessed=1 << 16, transcendentals=0),
    )(near(near_route), near(near_weight), near(near_source))
    got, chosen, share, pick = lax.optimization_barrier((paired(send), chosen, share, pick))
    state = update(state_parts, True, send)
    weights = [near(w_gate[0]), near(w_up[0]), near(w_down[0])]
    chunks = call(
        pair_kernel, pltpu.VMEM((places, rows, span), BF16), [vmem] * 2 + [hbm], "pair"
    )(near(own), near(got), far(state))
    chunks = lax.all_to_all(
        chunks, ("ep", "tp"), split_axis=0, concat_axis=0, tiled=True, axis_index_groups=groups[0]
    )
    own = call(
        functools.partial(join_kernel, order=first_order, chips=chips),
        pltpu.VMEM((count, span), BF16),
        [vmem] * 4,
        "join",
    )(near(chunks), *weights)
    got = paired(own)
    shape = (places, EXPERT_CAPACITY, cols) if aligned else (EXPERT_CAPACITY, width)
    pieces, *own_middle = call(
        functools.partial(expert_kernel, order=second_order, chips=chips),
        (pltpu.VMEM(shape, BF16),) + ((pltpu.VMEM((count, cols), BF16),) if aligned else ()),
        [vmem] * 8,
        "expert",
    )(
        near(own),
        near(got),
        near(gain),
        near(chosen),
        near(share),
        *weights,
    )
    if not aligned:
        first = lax.axis_index("tp") % 2 == 0
        middle = jnp.concatenate([jnp.where(first, own, got), jnp.where(first, got, own)], axis=1)
        start = lax.axis_index("ep") * cols
        own_middle = [lax.dynamic_slice_in_dim(middle, start, cols, axis=1)]
        pieces = pieces.reshape(EXPERT_CAPACITY, owners, cols).transpose(1, 0, 2)
        pieces = pieces[np.array(second_order) // chips]
    results = lax.all_to_all(
        pieces, ("ep", "tp"), split_axis=0, concat_axis=0, tiled=True, axis_index_groups=groups[1]
    )
    results = near(results.reshape(got_rows, cols))
    shapes = (pltpu.VMEM((count, cols), F32), pltpu.VMEM((count, cols), BF16))
    if short:
        own, send = call(mix_kernel, shapes, [vmem] * 2, "mix")(near(pick[0]), results)
    else:
        own, send = call(
            functools.partial(long_mix_kernel, experts=owners), shapes, [vmem] * 3, "mix"
        )(near(near_route), near(near_source), results)
    got = paired(send)
    state = update(state_parts, False, send, state)
    mixed = call(final_kernel, spec((count, cols), BF16), [vmem] * 3 + [hbm], "final")(
        near(own_middle[0]), near(own), near(got), far(state)
    )
    return (
        mixed,
        state.reshape(memory.shape),
        norm_state.reshape(normalizer.shape),
        new_max.T,
    )


def solution(mesh):
    return jax.shard_map(
        shards,
        mesh=mesh,
        in_specs=(
            P("ep", None),
            P(),
            P(None, "tp"),
            P(None, "tp"),
            P(None, "tp"),
            P(None, "tp"),
            P(),
            P(),
            P(),
            P("tp"),
            P("tp", None),
            P("ep", "tp", None, None),
            P("ep", "tp", None),
            P("ep", "tp"),
            P(),
            P(),
            P(),
            P("ep", None, "tp"),
            P("ep", None, "tp"),
            P("ep", "tp", None),
        ),
        out_specs=(P(None, "ep"), P("ep", "tp", None, None), P("ep", "tp", None), P("ep", "tp")),
        check_vma=False,
    )
```
